512 devices in a mesh: grp: 2 (over y), sp: 32 (over z), tp: 8 (over x, core).
Axes of the slice: x: 4, y: 2, z: 32, core: 2. Of those that a mesh axis runs over, the one named last changes fastest.
The devices are a block of a 4x8x32 slice.
Arguments:
- inputs: bfloat16 [16384, 2048], P(('grp', 'sp'), 'tp'), parts along dimension 0, may hold values from -20 to 20
- norm_gain: bfloat16 [2048], replicated, may hold values from 0.099609375 to 1.8984375
- w_conv_in: bfloat16 [1024, 2048], P('tp'), may hold values from -0.125 to 0.125
- w_conv_gate: bfloat16 [1024, 2048], P('tp'), may hold values from -0.125 to 0.125
- conv_kernel: bfloat16 [31, 1024], P(None, 'tp'), may hold values from -4.3105272 to 4.3105272
- ln_gain: bfloat16 [1024], P('tp'), may hold values from 0.099609375 to 1.8984375
- w_query: bfloat16 [1024, 2048], P('tp'), may hold values from -0.53033009 to 0.53033009
- w_key: bfloat16 [1024, 2048], P('tp'), may hold values from -0.53033009 to 0.53033009
- w_value: bfloat16 [1024, 2048], P('tp'), may hold values from -0.125 to 0.125
- cum_gate: float32 [16, 16384], P('tp', ('grp', 'sp')), parts along dimension 1, may hold values from -8192 to 0, as said below
- w_conv_out: bfloat16 [1024, 2048], P('tp'), may hold values from -0.125 to 0.125
- w_attn_out: bfloat16 [1024, 2048], P('tp'), may hold values from -0.125 to 0.125
Outputs:
- mixed: bfloat16 [16384, 2048], P(('grp', 'sp', 'tp')), parts along dimension 0
- log_total: float32 [16, 16384], P('tp', ('grp', 'sp')), parts along dimension 1
The draws below stay inside these ranges and needn't reach their ends.
There are 2 independent parts, one for each index of `grp`. The reference program is written for one: setup_inputs(seed, part) draws one part's arguments, and reference() takes and returns one part's arrays. A program takes and returns all parts, laid end to end along the dimension named above; an argument that names none is the same for every part. Nothing has to cross between parts.
Inputs may be any that keep to these rules, and one draw needn't show every extreme that they name: cum_gate never rises along positions: entry t is the sum of the head's log forget gates at positions 0 to t.
All inputs are finite; a program needn't handle non-finite values.
Results may differ from the reference program's by a relative error of at most 0.0144.
Values may be sent and summed in bfloat16 or wider, within the bound.
A program may use at most 64 MiB of HBM per device.

```python
import math
import jax
import jax.numpy as jnp
from jax import lax

D = 2048
CONV_CH = 1024
ATTENDER_TOTAL = 16
HEAD_DIM = 64
CONV_WIDTH = 31
TOK_DEV = 256
ATT_W = 1024
SEQUENCE_SPAN = 8192
N_SP = 32
N_TP = 8


def draw_inputs(key, part):
    key_one = jax.random.fold_in(key, 0)
    columns = jnp.exp(jnp.linspace(math.log(0.5), math.log(3.0), D)).astype(jnp.float32)
    raw_draw = jnp.clip(jax.random.normal(key_one, (SEQUENCE_SPAN, D), jnp.float32), -6.0, 6.0)
    return (raw_draw * columns[None, :]).astype(jnp.bfloat16)


def query_key_pair(key):
    query_draw = jnp.clip(jax.random.normal(jax.random.fold_in(key, 11), (ATT_W, D), jnp.float32), -6.0, 6.0) * D ** (-0.5)
    key_draw = 2.0 * jnp.clip(jax.random.normal(jax.random.fold_in(key, 13), (ATT_W, D), jnp.float32), -6.0, 6.0) * D ** (-0.5)
    query_draw = 2.0 * query_draw
    return (query_draw, key_draw)


def draw_w_query(key, part):
    return query_key_pair(key)[0].astype(jnp.bfloat16)


def draw_w_key(key, part):
    return query_key_pair(key)[1].astype(jnp.bfloat16)


def draw_conv_kernel(key, part):
    channels = jnp.exp(jnp.linspace(math.log(0.4), math.log(4.0), CONV_CH)).astype(jnp.float32)
    raw_draw = jnp.clip(jax.random.normal(key, (CONV_WIDTH, CONV_CH), jnp.float32), -6.0, 6.0)
    return (raw_draw * CONV_WIDTH ** (-0.5) * channels[None, :]).astype(jnp.bfloat16)


def draw_cum_gate(key, part):
    derived_seeds = jax.random.split(key, 6)
    head_order = jax.random.permutation(derived_seeds[0], ATTENDER_TOTAL)
    longest_memory_channel = head_order < ATTENDER_TOTAL // 2
    head_rate = jnp.exp(jax.random.uniform(derived_seeds[1], (ATTENDER_TOTAL,), jnp.float32, math.log(0.8), math.log(1.25)))
    base_rate = jnp.where(longest_memory_channel, 0.5 / SEQUENCE_SPAN, 1.0 / 25.0) * head_rate
    block_rate = jnp.exp(jax.random.uniform(derived_seeds[2], (ATTENDER_TOTAL, SEQUENCE_SPAN // TOK_DEV), jnp.float32, math.log(0.5), math.log(2.0)))
    block_rate = jnp.repeat(block_rate, TOK_DEV, axis=1)
    position_rate = jax.random.uniform(derived_seeds[3], (ATTENDER_TOTAL, SEQUENCE_SPAN), jnp.float32, 0.5, 1.5)
    decay_exponent = -base_rate[:, None] * block_rate * position_rate
    contiguous_offset = jax.random.randint(derived_seeds[4], (ATTENDER_TOTAL, 2, 1), 0, SEQUENCE_SPAN)
    contiguous_extent = jax.random.uniform(derived_seeds[5], (ATTENDER_TOTAL, 2, 1), jnp.float32, 0.22, 0.69)
    location_numbers = jnp.arange(SEQUENCE_SPAN, dtype=jnp.int32)
    contiguous_batches = jnp.sum(jnp.where(location_numbers[None, None, :] == contiguous_offset, contiguous_extent, 0.0), axis=1)
    decay_exponent = decay_exponent - jnp.where(longest_memory_channel[:, None], contiguous_batches, 0.0)
    return jnp.cumsum(decay_exponent, axis=1)


def levels(own_key, shape, pieces, least, top_value):
    def one(position, blocks):
        steps = jax.random.uniform(jax.random.fold_in(jax.random.fold_in(own_key, 6), position), (blocks,), jnp.float32, least / len(pieces), top_value / len(pieces))
        return jnp.repeat(jnp.exp(steps), shape[position] // blocks).reshape((-1,) + (1,) * (len(shape) - position - 1))

    level = one(*pieces[0])
    for cut in pieces[1:]:
        level = level * one(*cut)
    return level


def noise(key, shape, spread, most, pieces=(), kind=jnp.bfloat16):
    array = spread * jax.random.normal(key, shape, jnp.float32)
    if pieces:
        array = array * levels(key, shape, pieces, -0.22, 0.18)
    return jnp.clip(array, -most, most).astype(kind)


def setup_inputs(seed: int = 0, part: int = 0) -> dict:
    key_list = jax.random.split(jax.random.key(seed), 13)
    part_splits = jax.random.split(jax.random.fold_in(key_list[12], part), 13)
    return {
        "inputs": draw_inputs(jax.random.fold_in(jax.random.fold_in(key_list[12], part), 71), part),
        "norm_gain": jnp.clip(1.0 + 0.18 * jax.random.normal(key_list[1], (D,), jnp.float32), 0.099609375, 1.8984375).astype(jnp.bfloat16),
        "w_conv_in": noise(key_list[2], (CONV_CH, D), D ** -0.5, 0.125, ((0, 8),)),
        "w_conv_gate": noise(key_list[3], (CONV_CH, D), D ** -0.5, 0.125, ((0, 8),)),
        "conv_kernel": draw_conv_kernel(jax.random.fold_in(key_list[12], 71), part),
        "ln_gain": jnp.clip(1.0 + 0.18 * jax.random.normal(key_list[5], (CONV_CH,), jnp.float32), 0.099609375, 1.8984375).astype(jnp.bfloat16),
        "w_query": draw_w_query(jax.random.fold_in(key_list[12], 71), part),
        "w_key": draw_w_key(jax.random.fold_in(key_list[12], 71), part),
        "w_value": noise(key_list[8], (ATT_W, D), D ** -0.5, 0.125, ((0, 8),)),
        "cum_gate": draw_cum_gate(jax.random.fold_in(jax.random.fold_in(key_list[12], part), 71), part),
        "w_conv_out": noise(key_list[10], (CONV_CH, D), (CONV_CH + ATT_W) ** -0.5, 0.125, ((0, 8),)),
        "w_attn_out": noise(key_list[11], (ATT_W, D), (CONV_CH + ATT_W) ** -0.5, 0.125, ((0, 8),)),
    }


neg_large = -1e+30

def block_terms(q_blk, q_cum, k_blk, v_blk, k_cum, q_first, k_first):
    score_scale = q_blk.shape[2] ** (-0.5)
    scores = jnp.einsum('qhd,khd->hqk', q_blk.astype(jnp.float32), k_blk.astype(jnp.float32)) * score_scale
    scores = scores + q_cum[:, :, None] - k_cum[:, None, :]
    q_pos = q_first + jnp.arange(q_blk.shape[0], dtype=jnp.int32)
    k_pos = k_first + jnp.arange(k_blk.shape[0], dtype=jnp.int32)
    allowed = k_pos[None, :] <= q_pos[:, None]
    scores = jnp.where(allowed[None], scores, -jnp.inf)
    block_top = lax.optimization_barrier(jnp.max(scores, axis=-1))
    weights = jnp.exp(scores - block_top[..., None])
    block_total = lax.optimization_barrier(jnp.sum(weights, axis=-1))
    rounded = lax.optimization_barrier(weights.astype(jnp.bfloat16))
    block_out = jnp.einsum('hqk,khd->hqd', rounded.astype(jnp.float32), v_blk.astype(jnp.float32)).astype(jnp.bfloat16)
    return (block_top, block_total, block_out)

def merge_terms(state, terms):
    top_now, total_now, acc_now = state
    block_top, block_total, block_out = terms
    top_new = jnp.maximum(top_now, block_top)
    keep_old = jnp.exp(top_now - top_new)
    keep_new = jnp.exp(block_top - top_new)
    return (top_new, total_now * keep_old + block_total * keep_new, acc_now * keep_old[..., None] + block_out.astype(jnp.float32) * keep_new[..., None])

def reference(inputs, norm_gain, w_conv_in, w_conv_gate, conv_kernel, ln_gain, w_query, w_key, w_value, cum_gate, w_conv_out, w_attn_out):
    rows_f = inputs.astype(jnp.float32)
    rms = lax.rsqrt(lax.optimization_barrier(jnp.mean(rows_f * rows_f, axis=1, keepdims=True)) + 1e-06)
    scaled = (rows_f * norm_gain.astype(jnp.float32)[None, :]).astype(jnp.bfloat16)

    def project(weight):
        return lax.dot_general(scaled, weight, (((1,), (1,)), ((), ())), preferred_element_type=jnp.float32) * rms
    conv_in = project(w_conv_in)
    conv_gate = project(w_conv_gate)
    glu = (conv_in * jax.nn.sigmoid(conv_gate)).astype(jnp.bfloat16)
    padded = jnp.concatenate([jnp.zeros((CONV_WIDTH - 1, CONV_CH), jnp.bfloat16), glu], axis=0)
    kernel = conv_kernel.astype(jnp.float32)
    conv_sum = jnp.zeros((SEQUENCE_SPAN, CONV_CH), jnp.float32)
    for tap_idx in range(CONV_WIDTH):
        conv_sum = conv_sum + padded[tap_idx:tap_idx + SEQUENCE_SPAN].astype(jnp.float32) * kernel[tap_idx][None, :]
    chan_mean = lax.optimization_barrier(jnp.mean(conv_sum, axis=1, keepdims=True))
    chan_var = lax.optimization_barrier(jnp.mean(conv_sum * conv_sum, axis=1, keepdims=True)) - chan_mean * chan_mean
    normed = (conv_sum - chan_mean) * lax.rsqrt(chan_var + 1e-05) * ln_gain.astype(jnp.float32)[None, :]
    conv_out = jax.nn.silu(normed).astype(jnp.bfloat16)
    query = project(w_query).astype(jnp.bfloat16).reshape(N_SP, TOK_DEV, ATTENDER_TOTAL, HEAD_DIM)
    key_rows = project(w_key).astype(jnp.bfloat16).reshape(N_SP, TOK_DEV, ATTENDER_TOTAL, HEAD_DIM)
    value = project(w_value).astype(jnp.bfloat16).reshape(N_SP, TOK_DEV, ATTENDER_TOTAL, HEAD_DIM)
    cum_blocks = cum_gate.reshape(ATTENDER_TOTAL, N_SP, TOK_DEV).transpose(1, 0, 2)

    def one_query_block(query_idx):
        q_blk = query[query_idx]
        q_cum = cum_blocks[query_idx]

        def visit(key_idx, state):
            terms = block_terms(q_blk, q_cum, key_rows[key_idx], value[key_idx], cum_blocks[key_idx], query_idx * TOK_DEV, key_idx * TOK_DEV)
            return merge_terms(state, terms)
        start_state = (jnp.full((ATTENDER_TOTAL, TOK_DEV), neg_large, jnp.float32), jnp.zeros((ATTENDER_TOTAL, TOK_DEV), jnp.float32), jnp.zeros((ATTENDER_TOTAL, TOK_DEV, HEAD_DIM), jnp.float32))
        top_all, total_all, acc_all = lax.fori_loop(0, query_idx + 1, visit, start_state)
        result = (acc_all / total_all[..., None]).transpose(1, 0, 2).reshape(TOK_DEV, ATT_W).astype(jnp.bfloat16)
        return (result, top_all + jnp.log(total_all))
    attn_blocks, log_blocks = lax.map(one_query_block, jnp.arange(N_SP, dtype=jnp.int32))
    attn_out = attn_blocks.reshape(SEQUENCE_SPAN, ATT_W)
    log_total = log_blocks.transpose(1, 0, 2).reshape(ATTENDER_TOTAL, SEQUENCE_SPAN)
    chan_group = CONV_CH // N_TP
    head_group = ATT_W // N_TP
    mixed = jnp.zeros((SEQUENCE_SPAN, D), jnp.float32)
    for group_idx in range(N_TP):
        part = jnp.dot(conv_out[:, group_idx * chan_group:(group_idx + 1) * chan_group], w_conv_out[group_idx * chan_group:(group_idx + 1) * chan_group], preferred_element_type=jnp.float32)
        part = part + jnp.dot(attn_out[:, group_idx * head_group:(group_idx + 1) * head_group], w_attn_out[group_idx * head_group:(group_idx + 1) * head_group], preferred_element_type=jnp.float32)
        part_round = lax.optimization_barrier(part.astype(jnp.bfloat16))
        mixed = mixed + part_round.astype(jnp.float32)
    return (mixed.astype(jnp.bfloat16), log_total)
```

```python
import functools

import jax
import jax.numpy as jnp
from jax import lax
from jax.experimental import pallas as pl
from jax.experimental.pallas import tpu as pltpu
from jax.sharding import PartitionSpec as P

MESH = pl.DeviceIdType.MESH
F32 = jnp.float32
BF16 = jnp.bfloat16
CHUNKS = 4
OUT_CUTS = 2
NT = (((1,), (1,)), ((), ()))
NN = (((1,), (0,)), ((), ()))


def dot(a, b, dims):
    return lax.dot_general(a, b, dims, preferred_element_type=F32)


def layer(
    n,
    n_tp,
    x_hbm,
    gain_hbm,
    wci_hbm,
    wcg_hbm,
    taps_hbm,
    lng_hbm,
    wq_hbm,
    wk_hbm,
    wv_hbm,
    cum_hbm,
    wco_hbm,
    wao_hbm,
    mixed_ref,
    log_ref,
    xg,
    xs,
    gain,
    taps,
    lng,
    wkv,
    w3,
    wo,
    kv,
    cum,
    kvacc,
    sq,
    qs,
    m_ref,
    l_ref,
    acc,
    ext,
    glu_tail,
    halo,
    ctr,
    stats,
    comb,
    pair_out,
    pair_in,
    xout,
    xin,
    ld_sem,
    in_send,
    in_recv,
    kv_send,
    kv_recv,
    cum_send,
    cum_recv,
    halo_sem,
    st_send,
    st_recv,
    pair_send,
    pair_recv,
    x_send,
    x_recv,
):
    z = lax.axis_index("sp")
    t = lax.axis_index("tp")
    rows, feat = x_hbm.shape
    width = wk_hbm.shape[0]
    heads = cum_hbm.shape[0]
    hd = width // heads
    n_taps = taps_hbm.shape[0]
    half_n = n // 2
    nx = n_tp // 2
    x = t // 2
    c = t % 2

    def at(dx, core):
        return 2 * ((x + dx + nx) % nx) + core

    right, left, far, mate = at(1, c), at(-1, c), at(2, c), at(0, 1 - c)
    up, down = (z + 1) % n, (z + n - 1) % n

    def rdma(src, dst, send, recv, **device):
        return pltpu.make_async_remote_copy(
            src_ref=src, dst_ref=dst, send_sem=send, recv_sem=recv, device_id=device, device_id_type=MESH
        )

    loads = [
        (x_hbm, xg.at[t]),
        (wk_hbm, wkv.at[pl.ds(0, width)]),
        (wv_hbm, wkv.at[pl.ds(width, width)]),
        (gain_hbm, gain),
        (cum_hbm, cum.at[z]),
        (wci_hbm, w3.at[pl.ds(0, width)]),
        (wcg_hbm, w3.at[pl.ds(width, width)]),
        (wq_hbm, w3.at[pl.ds(2 * width, width)]),
        (taps_hbm, taps),
        (lng_hbm, lng),
        (wco_hbm, wo.at[pl.ds(0, width)]),
        (wao_hbm, wo.at[pl.ds(width, width)]),
    ]
    loads = [pltpu.make_async_copy(a, b, ld_sem.at[i]) for i, (a, b) in enumerate(loads)]
    for copy in loads:
        copy.start()

    barrier = pltpu.get_barrier_semaphore()
    for k in range(1, n_tp):
        pl.semaphore_signal(barrier, inc=1, device_id={"tp": (t + k) % n_tp}, device_id_type=MESH)
    pl.semaphore_signal(barrier, inc=1, device_id={"sp": up}, device_id_type=MESH)
    pl.semaphore_signal(barrier, inc=1, device_id={"sp": down}, device_id_type=MESH)
    pl.semaphore_wait(barrier, n_tp + 1)

    half = rows // 2
    pending = []

    def part(slot, h):
        return xg.at[slot, pl.ds(h * half, half)]

    def send_in(slot, h, to):
        k = len(pending)
        copy = rdma(part(slot, h), part(slot, h), in_send.at[k], in_recv.at[slot, h], tp=to)
        copy.start()
        pending.append(copy)

    def got(slot, h):
        rdma(part(slot, h), part(slot, h), in_send.at[0], in_recv.at[slot, h], tp=mate).wait_recv()

    loads[0].wait()
    send_in(t, 0, right)
    send_in(t, 1, left)
    send_in(t, 1, right)
    send_in(t, 0, left)
    send_in(t, 0, mate)
    send_in(t, 1, mate)
    for copy in loads[1:4]:
        copy.wait()
    kvacc[...] = jnp.zeros_like(kvacc)
    sq[...] = jnp.zeros_like(sq)

    def process(slot):
        xf = xg[slot].astype(F32)
        lanes = pl.ds(pl.multiple_of(slot * feat, feat), feat)
        s2 = xf * xf
        sq[...] += s2[:, :128] + s2[:, 128:]
        sc = (xf * gain[:, lanes].astype(F32)).astype(BF16)
        xs[slot] = sc
        kvacc[...] += dot(sc, wkv[:, lanes], NT)

    process(t)
    got(mate, 0)
    got(mate, 1)
    process(mate)
    got(left, 0)
    send_in(left, 0, right)
    send_in(left, 0, mate)
    got(right, 1)
    send_in(right, 1, left)
    send_in(right, 1, mate)
    got(left, 1)
    send_in(left, 1, mate)
    got(right, 0)
    send_in(right, 0, mate)
    process(left)
    process(right)
    for slot in (at(-1, 1 - c), at(1, 1 - c)):
        got(slot, 0)
        got(slot, 1)
        process(slot)
    got(far, 0)
    send_in(far, 0, mate)
    got(far, 1)
    send_in(far, 1, mate)
    process(far)
    got(at(2, 1 - c), 0)
    got(at(2, 1 - c), 1)
    process(at(2, 1 - c))

    rms = lax.rsqrt(jnp.sum(sq[...], axis=1, keepdims=True) / (feat * n_tp) + 1e-06)
    kv[z] = (kvacc[...] * rms).astype(BF16)
    loads[4].wait()

    chunk = rows // CHUNKS

    def kv_copy(way, blk, q, k, to):
        ref = kv.at[blk, pl.ds(q * chunk, chunk)]
        return rdma(ref, ref, kv_send.at[way, k, q], kv_recv.at[blk, q], sp=to)

    def cum_copy(way, blk, k, to):
        return rdma(cum.at[blk], cum.at[blk], cum_send.at[way, k], cum_recv.at[blk], sp=to)

    first_up = z < n - 1
    first_down = z <= half_n - 2
    for way, cond, to in ((0, first_up, up), (1, first_down, down)):

        @pl.when(cond)
        def _(way=way, to=to):
            cum_copy(way, z, 0, to).start()
            for q in range(CHUNKS):
                kv_copy(way, z, q, 0, to).start()

    for copy in loads[5:8]:
        copy.wait()
    r3 = dot(xs[0], w3[:, :feat], NT)
    for p in range(1, n_tp):
        r3 += dot(xs[p], w3[:, p * feat : (p + 1) * feat], NT)
    r3 = r3 * rms
    glu = (r3[:, :width] * jax.nn.sigmoid(r3[:, width : 2 * width])).astype(BF16)
    pad = glu_tail.shape[0]
    glu_tail[...] = glu[rows - pad :]
    ext[pl.ds(pad, rows)] = glu.astype(F32)
    ext[pl.ds(pad + rows, 8)] = jnp.zeros((8, width), F32)
    query = (r3[:, 2 * width :]).astype(BF16) * jnp.asarray(hd ** (-0.5), BF16)
    lane = lax.broadcasted_iota(jnp.int32, (rows, width), 1)
    for h in range(heads):
        mine = (lane >= h * hd) & (lane < (h + 1) * hd)
        qs[pl.ds(h * rows, rows)] = jnp.where(mine, query.astype(F32), 0.0).astype(BF16)
    m_ref[...] = jnp.full_like(m_ref, -1e30)
    l_ref[...] = jnp.zeros_like(l_ref)
    acc[...] = jnp.zeros_like(acc)
    halo_copy = rdma(glu_tail, halo, halo_sem.at[0], halo_sem.at[1], sp=up)

    @pl.when(first_up)
    def _():
        halo_copy.start()

    piece = heads * rows // CHUNKS
    per_head = rows // piece

    def attend(q, blk, offset):
        h = q // per_head
        here = pl.ds(q * piece, piece)
        s = dot(qs[here], kv[blk, :, :width], NT)
        s = s + (cum[z, h : h + 1, 0:1] - cum[blk, h : h + 1, :])
        q_pos = lax.broadcasted_iota(jnp.int32, s.shape, 0) + (q % per_head) * piece + offset
        k_pos = lax.broadcasted_iota(jnp.int32, s.shape, 1)
        s = jnp.where(k_pos <= q_pos, s, -1e30)
        m_old = m_ref[here]
        m_new = jnp.maximum(m_old, jnp.max(s, axis=1, keepdims=True))
        fade = jnp.exp(m_old - m_new)
        p = jnp.exp(s - m_new[:, :1])
        l_ref[here] = l_ref[here] * fade + jnp.sum(p, axis=1, keepdims=True)
        m_ref[here] = m_new
        acc[here] = acc[here] * fade + dot(p.astype(BF16), kv[blk, :, width:], NN)

    def convolve():
        loads[8].wait()

        @pl.when(z > 0)
        def _():
            halo_copy.wait_recv()
            ext[pl.ds(0, pad)] = halo[...].astype(F32)

        @pl.when(z == 0)
        def _():
            ext[pl.ds(0, pad)] = jnp.zeros((pad, width), F32)

        weight = taps[...].astype(F32)
        shift = pad - (n_taps - 1)
        long = rows + 8
        total = jnp.zeros((rows, width), F32)
        for r in range(8):
            sub = None
            for j in range(n_taps):
                if (shift + j) % 8 == r:
                    base = shift + j - r
                    if r == 0:
                        term = ext[pl.ds(base, rows)] * weight[j : j + 1]
                    else:
                        term = ext[pl.ds(base, long)] * weight[j : j + 1]
                    sub = term if sub is None else sub + term
            if r == 0:
                total = total + sub
            else:
                total = total + pltpu.roll(sub, long - r, 0)[:rows]
        turned = total.T
        ctr[...] = turned
        stats[t, 0:1] = jnp.sum(turned, axis=0, keepdims=True)
        stats[t, 1:2] = jnp.sum(turned * turned, axis=0, keepdims=True)

    def stat_copy(k):
        return rdma(stats.at[t], stats.at[t], st_send.at[k], st_recv.at[t], tp=(t + k) % n_tp)

    def send_stats():
        for k in range(1, n_tp):
            stat_copy(k).start()

    def finish_conv():
        for k in range(1, n_tp):
            src = (t + k) % n_tp
            rdma(stats.at[src], stats.at[src], st_send.at[0], st_recv.at[src], tp=src).wait_recv()
        loads[9].wait()
        tot = stats[0]
        for p in range(1, n_tp):
            tot = tot + stats[p]
        mean = tot[0:1] / (width * n_tp)
        var = tot[1:2] / (width * n_tp) - mean * mean
        y = ((ctr[...] - mean) * lax.rsqrt(var + 1e-05)).T
        y = y * lng[...].astype(F32)
        y = (y * jax.nn.sigmoid(y)).astype(BF16)
        each = rows // n_tp
        for d in range(n_tp):
            comb[d // 2, d % 2, :, :width] = y[d * each : (d + 1) * each]

    conv_at = 2
    stats_at = min(5, half_n + 1)

    def flows(s):
        cw_in = (z >= s) & (s <= half_n)
        cw_on = cw_in & (z < n - 1) & (s < half_n)
        reach = (z + s <= half_n - 2) | (z + s >= n)
        cc_in = reach & (s <= half_n - 1)
        cc_on = cc_in & (s < half_n - 1)
        return cw_in, cw_on, cc_in, cc_on

    def step(s, carry):
        cw_in, cw_on, cc_in, cc_on = flows(s)
        j_cw, j_cc = (z + n - s) % n, (z + s) % n
        b_cw, b_cc = (z + n - s + 1) % n, (z + s - 1) % n
        use_cw = z >= s - 1
        use_cc = (z + s - 1 >= n) & (s <= half_n)
        for q in range(CHUNKS):
            for way, arrives, goes, blk, to in (
                (0, cw_in, cw_on, j_cw, up),
                (1, cc_in, cc_on, j_cc, down),
            ):

                @pl.when(arrives)
                def _(way=way, blk=blk, to=to):
                    if q == 0:
                        cum_copy(way, blk, 0, to).wait_recv()
                    kv_copy(way, blk, q, 0, to).wait_recv()

                @pl.when(goes)
                def _(way=way, blk=blk, to=to):
                    if q == 0:
                        cum_copy(way, blk, s, to).start()
                    kv_copy(way, blk, q, s, to).start()

            @pl.when(use_cw)
            def _():
                attend(q, b_cw, (s - 1) * rows)

            @pl.when(use_cc)
            def _():
                attend(q, b_cc, n * rows)

        @pl.when(s == conv_at)
        def _():
            convolve()
            send_stats()

        @pl.when(s == stats_at)
        def _():
            finish_conv()

        return carry

    lax.fori_loop(1, half_n + 2, step, 0)

    tops, sums = m_ref[...], l_ref[...]
    logs = tops + jnp.log(sums)
    attn = acc[...] / sums
    log_row = logs[:rows]
    attn_row = attn[:rows]
    for h in range(1, heads):
        attn_row = jnp.where(lane >= h * hd, attn[h * rows : (h + 1) * rows], attn_row)
        log_row = jnp.where(lane >= h, logs[h * rows : (h + 1) * rows], log_row)
    each = rows // n_tp
    attn_row = attn_row.astype(BF16)
    for d in range(n_tp):
        comb[d // 2, d % 2, :, width:] = attn_row[d * each : (d + 1) * each]

    for copy in loads[10:12]:
        copy.wait()
    cut = wo.shape[1] // OUT_CUTS

    def product(core, i):
        lhs = comb[:, core].reshape(nx * each, 2 * width)
        return dot(lhs, wo[:, i * cut : (i + 1) * cut], NN).reshape(nx, each, cut)

    pairs = []
    for i in range(OUT_CUTS):
        pair_out[i] = product(1 - c, i).astype(BF16)
        copy = rdma(pair_out.at[i], pair_in.at[i], pair_send.at[i], pair_recv.at[i], tp=mate)
        copy.start()
        pairs.append(copy)
    outs = []
    for i in range(OUT_CUTS):
        own = product(c, i)
        pairs[i].wait_recv()
        xout[i] = (own + pair_in[i].astype(F32)).astype(BF16)
        for dx in (2, 1, 3):
            dst = at(dx - nx, c)
            copy = rdma(
                xout.at[i, (x + dx) % nx], xin.at[i, dx - 1], x_send.at[i, dx - 1], x_recv.at[i, dx - 1], tp=dst
            )
            copy.start()
            outs.append((i, copy))
    log_ref[...] = log_row.T[:heads] + (cum[z] - cum[z][:, 0:1])
    for i in range(OUT_CUTS):
        total = xout[i, x].astype(F32)
        for k, copy in outs:
            if k == i:
                copy.wait_recv()
        for dx in range(nx - 1):
            total = total + xin[i, dx].astype(F32)
        mixed_ref[:, i * cut : (i + 1) * cut] = total.astype(BF16)

    for copy in pending:
        copy.wait_send()
    for way, cond, to in ((0, first_up, up), (1, first_down, down)):

        @pl.when(cond)
        def _(way=way, to=to):
            cum_copy(way, z, 0, to).wait_send()
            for q in range(CHUNKS):
                kv_copy(way, z, q, 0, to).wait_send()

    @pl.when(first_up)
    def _():
        halo_copy.wait_send()

    for k in range(1, n_tp):
        stat_copy(k).wait_send()

    def drain(s, carry):
        cw_in, cw_on, cc_in, cc_on = flows(s)
        for way, goes, blk, to in ((0, cw_on, (z + n - s) % n, up), (1, cc_on, (z + s) % n, down)):

            @pl.when(goes)
            def _(way=way, blk=blk, to=to):
                cum_copy(way, blk, s, to).wait_send()
                for q in range(CHUNKS):
                    kv_copy(way, blk, q, s, to).wait_send()

        return carry

    lax.fori_loop(1, half_n, drain, 0)
    for copy in pairs:
        copy.wait_send()
    for k, copy in outs:
        copy.wait_send()


def solution(mesh):
    n, n_tp = mesh.shape["sp"], mesh.shape["tp"]

    def local(
        inputs,
        norm_gain,
        w_conv_in,
        w_conv_gate,
        conv_kernel,
        ln_gain,
        w_query,
        w_key,
        w_value,
        cum_gate,
        w_conv_out,
        w_attn_out,
    ):
        rows, feat = inputs.shape
        width, full = w_key.shape
        heads = cum_gate.shape[0]
        n_taps = conv_kernel.shape[0]
        each = rows // n_tp
        nx = n_tp // 2
        pad = 32
        cut = full // OUT_CUTS
        half_n = n // 2
        dma = pltpu.SemaphoreType.DMA
        vmem = pltpu.VMEM
        scratch = [
            vmem((n_tp, rows, feat), BF16),
            vmem((n_tp, rows, feat), BF16),
            vmem((1, full), BF16),
            vmem((n_taps, width), BF16),
            vmem((1, width), BF16),
            vmem((2 * width, full), BF16),
            vmem((3 * width, full), BF16),
            vmem((2 * width, full), BF16),
            vmem((n, rows, 2 * width), BF16),
            vmem((n, heads, rows), F32),
            vmem((rows, 2 * width), F32),
            vmem((rows, 128), F32),
            vmem((heads * rows, width), BF16),
            vmem((heads * rows, width), F32),
            vmem((heads * rows, width), F32),
            vmem((heads * rows, width), F32),
            vmem((pad + rows + 8, width), F32),
            vmem((pad, width), BF16),
            vmem((pad, width), BF16),
            vmem((width, rows), F32),
            vmem((n_tp, 2, rows), F32),
            vmem((nx, 2, each, 2 * width), BF16),
            vmem((OUT_CUTS, nx, each, cut), BF16),
            vmem((OUT_CUTS, nx, each, cut), BF16),
            vmem((OUT_CUTS, nx, each, cut), BF16),
            vmem((OUT_CUTS, nx - 1, each, cut), BF16),
            dma((12,)),
            dma((14,)),
            dma((n_tp, 2)),
            dma((2, half_n, CHUNKS)),
            dma((n, CHUNKS)),
            dma((2, half_n)),
            dma((n,)),
            dma((2,)),
            dma((n_tp,)),
            dma((n_tp,)),
            dma((OUT_CUTS,)),
            dma((OUT_CUTS,)),
            dma((OUT_CUTS, nx - 1)),
            dma((OUT_CUTS, nx - 1)),
        ]
        return pl.pallas_call(
            functools.partial(layer, n, n_tp),
            out_shape=(
                jax.ShapeDtypeStruct((each, full), BF16),
                jax.ShapeDtypeStruct((heads, rows), F32),
            ),
            in_specs=[pl.BlockSpec(memory_space=pl.ANY)] * 12,
            out_specs=(pl.BlockSpec(memory_space=pltpu.VMEM), pl.BlockSpec(memory_space=pltpu.VMEM)),
            scratch_shapes=scratch,
            compiler_params=pltpu.CompilerParams(collective_id=0, has_side_effects=True),
        )(
            inputs,
            norm_gain.reshape(1, full),
            w_conv_in,
            w_conv_gate,
            conv_kernel,
            ln_gain.reshape(1, width),
            w_query,
            w_key,
            w_value,
            cum_gate,
            w_conv_out,
            w_attn_out,
        )

    in_specs = (
        P(("grp", "sp"), "tp"),
        P(),
        P("tp", None),
        P("tp", None),
        P(None, "tp"),
        P("tp"),
        P("tp", None),
        P("tp", None),
        P("tp", None),
        P("tp", ("grp", "sp")),
        P("tp", None),
        P("tp", None),
    )
    out_specs = (P(("grp", "sp", "tp"), None), P("tp", ("grp", "sp")))
    return jax.shard_map(local, mesh=mesh, in_specs=in_specs, out_specs=out_specs, check_vma=False)
```

```python
import functools

import jax
import jax.numpy as jnp
from jax import lax
from jax.experimental import pallas as pl
from jax.experimental.pallas import tpu as pltpu
from jax.sharding import PartitionSpec as P

MESH = pl.DeviceIdType.MESH
F32 = jnp.float32
BF16 = jnp.bfloat16
CHUNKS = 4
OUT_CUTS = 2
NT = (((1,), (1,)), ((), ()))
NN = (((1,), (0,)), ((), ()))


def dot(a, b, dims):
    return lax.dot_general(a, b, dims, preferred_element_type=F32)


def layer(
    n,
    n_tp,
    x_hbm,
    gain_hbm,
    wci_hbm,
    wcg_hbm,
    taps_hbm,
    lng_hbm,
    wq_hbm,
    wk_hbm,
    wv_hbm,
    cum_hbm,
    wco_hbm,
    wao_hbm,
    mixed_ref,
    log_ref,
    xg,
    xs,
    gain,
    taps,
    lng,
    wkv,
    w3,
    wo,
    kv,
    cum,
    kvacc,
    sq,
    qs,
    m_ref,
    l_ref,
    acc,
    ext,
    glu_tail,
    halo,
    ctr,
    stats,
    comb,
    pair_out,
    pair_in,
    xout,
    xin,
    ld_sem,
    in_send,
    in_recv,
    kv_send,
    kv_recv,
    cum_send,
    cum_recv,
    halo_sem,
    up_ready,
    far_ready,
    st_send,
    st_recv,
    pair_send,
    pair_recv,
    x_send,
    x_recv,
):
    z = lax.axis_index("sp")
    t = lax.axis_index("tp")
    rows, feat = x_hbm.shape
    width = wk_hbm.shape[0]
    heads = cum_hbm.shape[0]
    hd = width // heads
    n_taps = taps_hbm.shape[0]
    half_n = n // 2
    nx = n_tp // 2
    x = t // 2
    c = t % 2

    def at(dx, core):
        return 2 * ((x + dx + nx) % nx) + core

    right, left, far, mate = at(1, c), at(-1, c), at(2, c), at(0, 1 - c)
    up, down = (z + 1) % n, (z + n - 1) % n

    def rdma(src, dst, send, recv, **device):
        return pltpu.make_async_remote_copy(
            src_ref=src, dst_ref=dst, send_sem=send, recv_sem=recv, device_id=device, device_id_type=MESH
        )

    loads = [
        (x_hbm, xg.at[t]),
        (wk_hbm, wkv.at[pl.ds(0, width)]),
        (wv_hbm, wkv.at[pl.ds(width, width)]),
        (gain_hbm, gain),
        (cum_hbm, cum.at[z]),
        (wci_hbm, w3.at[pl.ds(0, width)]),
        (wcg_hbm, w3.at[pl.ds(width, width)]),
        (wq_hbm, w3.at[pl.ds(2 * width, width)]),
        (taps_hbm, taps),
        (lng_hbm, lng),
        (wco_hbm, wo.at[pl.ds(0, width)]),
        (wao_hbm, wo.at[pl.ds(width, width)]),
    ]
    loads = [pltpu.make_async_copy(a, b, ld_sem.at[i]) for i, (a, b) in enumerate(loads)]
    for copy in loads:
        copy.start()

    barrier = pltpu.get_barrier_semaphore()
    for k in range(1, n_tp):
        pl.semaphore_signal(barrier, inc=1, device_id={"tp": (t + k) % n_tp}, device_id_type=MESH)
    last = n - 1
    n_low = half_n - 1
    is_low = z < n_low

    @pl.when(z < last)
    def _():
        pl.semaphore_signal(barrier, inc=1, device_id={"sp": up}, device_id_type=MESH)

    @pl.when(is_low)
    def _():
        pl.semaphore_signal(barrier, inc=1, device_id={"sp": last}, device_id_type=MESH)

    pl.semaphore_wait(
        barrier, n_tp - 1 + jnp.where(z > 0, 1, 0) + jnp.where(z == last, n_low, 0)
    )

    @pl.when(z > 0)
    def _():
        pl.semaphore_signal(up_ready, inc=1, device_id={"sp": down}, device_id_type=MESH)

    @pl.when(z == last)
    def _():
        def tell(j, carry):
            pl.semaphore_signal(far_ready, inc=1, device_id={"sp": j}, device_id_type=MESH)
            return carry

        lax.fori_loop(0, n_low, tell, 0)


    half = rows // 2
    pending = []

    def part(slot, h):
        return xg.at[slot, pl.ds(h * half, half)]

    def send_in(slot, h, to):
        k = len(pending)
        copy = rdma(part(slot, h), part(slot, h), in_send.at[k], in_recv.at[slot, h], tp=to)
        copy.start()
        pending.append(copy)

    def got(slot, h):
        rdma(part(slot, h), part(slot, h), in_send.at[0], in_recv.at[slot, h], tp=mate).wait_recv()

    loads[0].wait()
    send_in(t, 0, right)
    send_in(t, 1, left)
    send_in(t, 1, right)
    send_in(t, 0, left)
    send_in(t, 0, mate)
    send_in(t, 1, mate)
    for copy in loads[1:4]:
        copy.wait()
    kvacc[...] = jnp.zeros_like(kvacc)
    sq[...] = jnp.zeros_like(sq)

    def process(slot):
        xf = xg[slot].astype(F32)
        lanes = pl.ds(pl.multiple_of(slot * feat, feat), feat)
        s2 = xf * xf
        sq[...] += s2[:, :128] + s2[:, 128:]
        sc = (xf * gain[:, lanes].astype(F32)).astype(BF16)
        xs[slot] = sc
        kvacc[...] += dot(sc, wkv[:, lanes], NT)

    process(t)
    got(mate, 0)
    got(mate, 1)
    process(mate)
    got(left, 0)
    send_in(left, 0, right)
    send_in(left, 0, mate)
    got(right, 1)
    send_in(right, 1, left)
    send_in(right, 1, mate)
    got(left, 1)
    send_in(left, 1, mate)
    got(right, 0)
    send_in(right, 0, mate)
    process(left)
    process(right)
    for slot in (at(-1, 1 - c), at(1, 1 - c)):
        got(slot, 0)
        got(slot, 1)
        process(slot)
    got(far, 0)
    send_in(far, 0, mate)
    got(far, 1)
    send_in(far, 1, mate)
    process(far)
    got(at(2, 1 - c), 0)
    got(at(2, 1 - c), 1)
    process(at(2, 1 - c))

    rms = lax.rsqrt(jnp.sum(sq[...], axis=1, keepdims=True) / (feat * n_tp) + 1e-06)
    kv[z] = (kvacc[...] * rms).astype(BF16)
    loads[4].wait()

    chunk = rows // CHUNKS

    def kv_copy(way, blk, q, k, to):
        ref = kv.at[blk, pl.ds(q * chunk, chunk)]
        return rdma(ref, ref, kv_send.at[way, k, q], kv_recv.at[blk, q], sp=to)

    def cum_copy(way, blk, k, to):
        return rdma(cum.at[blk], cum.at[blk], cum_send.at[way, k], cum_recv.at[blk], sp=to)

    first_up = z < last

    @pl.when(first_up)
    def _():
        pl.semaphore_wait(up_ready, 1)
        cum_copy(0, z, 0, up).start()
        for q in range(CHUNKS):
            kv_copy(0, z, q, 0, up).start()

    for copy in loads[5:8]:
        copy.wait()
    r3 = dot(xs[0], w3[:, :feat], NT)
    for p in range(1, n_tp):
        r3 += dot(xs[p], w3[:, p * feat : (p + 1) * feat], NT)
    r3 = r3 * rms
    glu = (r3[:, :width] * jax.nn.sigmoid(r3[:, width : 2 * width])).astype(BF16)
    pad = glu_tail.shape[0]
    glu_tail[...] = glu[rows - pad :]
    ext[pl.ds(pad, rows)] = glu.astype(F32)
    ext[pl.ds(pad + rows, 8)] = jnp.zeros((8, width), F32)
    query = (r3[:, 2 * width :]).astype(BF16) * jnp.asarray(hd ** (-0.5), BF16)
    lane = lax.broadcasted_iota(jnp.int32, (rows, width), 1)
    for h in range(heads):
        mine = (lane >= h * hd) & (lane < (h + 1) * hd)
        qs[pl.ds(h * rows, rows)] = jnp.where(mine, query.astype(F32), 0.0).astype(BF16)
    halo_copy = rdma(glu_tail, halo, halo_sem.at[0], halo_sem.at[1], sp=up)

    @pl.when(first_up)
    def _():
        halo_copy.start()

    ones = jnp.ones((rows, width), BF16)

    def attend(h, blocks, diagonal=False):
        here = pl.ds(h * rows, rows)
        q = qs[here]
        scores = []
        for blk in blocks:
            s = dot(q, kv[blk, :, :width], NT)
            s = s + (cum[z, h : h + 1, 0:1] - cum[blk, h : h + 1, :])
            if diagonal:
                q_pos = lax.broadcasted_iota(jnp.int32, s.shape, 0)
                k_pos = lax.broadcasted_iota(jnp.int32, s.shape, 1)
                s = jnp.where(k_pos <= q_pos, s, -1e30)
            scores.append(s)
        best = scores[0]
        for s in scores[1:]:
            best = jnp.maximum(best, s)
        m_new = jnp.broadcast_to(jnp.max(best, axis=1, keepdims=True), (rows, width))
        if not diagonal:
            m_old = m_ref[here]
            m_new = jnp.maximum(m_old, m_new)
        m_ref[here] = m_new
        wide = jnp.concatenate([m_new] * (rows // width), axis=1)
        out = None
        for blk, s in zip(blocks, scores):
            p = jnp.exp(s - wide).astype(BF16)
            o = dot(p, jnp.concatenate([kv[blk, :, width:], ones], axis=1), NN)
            out = o if out is None else out + o
        if diagonal:
            acc[here] = out[:, :width]
            l_ref[here] = out[:, width:]
        else:
            fade = jnp.exp(m_old - m_new)
            acc[here] = acc[here] * fade + out[:, :width]
            l_ref[here] = l_ref[here] * fade + out[:, width:]

    for h in range(heads):
        attend(h, [z], diagonal=True)

    def convolve():
        loads[8].wait()

        @pl.when(z > 0)
        def _():
            halo_copy.wait_recv()
            ext[pl.ds(0, pad)] = halo[...].astype(F32)

        @pl.when(z == 0)
        def _():
            ext[pl.ds(0, pad)] = jnp.zeros((pad, width), F32)

        weight = taps[...].astype(F32)
        shift = pad - (n_taps - 1)
        long = rows + 8
        total = jnp.zeros((rows, width), F32)
        for r in range(8):
            sub = None
            for j in range(n_taps):
                if (shift + j) % 8 == r:
                    base = shift + j - r
                    if r == 0:
                        term = ext[pl.ds(base, rows)] * weight[j : j + 1]
                    else:
                        term = ext[pl.ds(base, long)] * weight[j : j + 1]
                    sub = term if sub is None else sub + term
            if r == 0:
                total = total + sub
            else:
                total = total + pltpu.roll(sub, long - r, 0)[:rows]
        turned = total.T
        ctr[...] = turned
        stats[t, 0:1] = jnp.sum(turned, axis=0, keepdims=True)
        stats[t, 1:2] = jnp.sum(turned * turned, axis=0, keepdims=True)

    def stat_copy(k):
        return rdma(stats.at[t], stats.at[t], st_send.at[k], st_recv.at[t], tp=(t + k) % n_tp)

    def send_stats():
        for k in range(1, n_tp):
            stat_copy(k).start()

    def finish_conv():
        for k in range(1, n_tp):
            src = (t + k) % n_tp
            rdma(stats.at[src], stats.at[src], st_send.at[0], st_recv.at[src], tp=src).wait_recv()
        loads[9].wait()
        tot = stats[0]
        for p in range(1, n_tp):
            tot = tot + stats[p]
        mean = tot[0:1] / (width * n_tp)
        var = tot[1:2] / (width * n_tp) - mean * mean
        y = ((ctr[...] - mean) * lax.rsqrt(var + 1e-05)).T
        y = y * lng[...].astype(F32)
        y = (y * jax.nn.sigmoid(y)).astype(BF16)
        each = rows // n_tp
        for d in range(n_tp):
            comb[d // 2, d % 2, :, :width] = y[d * each : (d + 1) * each]

    conv_at = 2
    stats_at = min(5, half_n + 1)

    def flows(s):
        cw_in = (z >= s) & (s <= half_n)
        cw_on = cw_in & (z < n - 1) & (s < half_n)
        cc_in = (z + s >= n) & (s <= n_low)
        cc_on = cc_in & (s < n_low)
        return cw_in, cw_on, cc_in, cc_on

    def step(s, carry):
        cw_in, cw_on, cc_in, cc_on = flows(s)
        j_cw, j_cc = (z + n - s) % n, (z + s) % n
        b_cw, b_cc = (z + n - s + 1) % n, (z + s - 1) % n
        two = (z + s - 1 >= n) & (s <= half_n) & (s > 1)
        one = (z >= s - 1) & (s > 1) & jnp.logical_not(two)
        every = CHUNKS // heads
        for q in range(CHUNKS):
            for way, arrives, goes, blk, to in (
                (0, cw_in, cw_on, j_cw, up),
                (1, cc_in, cc_on, j_cc, down),
            ):

                @pl.when(arrives)
                def _(way=way, blk=blk, to=to):
                    if q == 0:
                        cum_copy(way, blk, 0, to).wait_recv()
                    kv_copy(way, blk, q, 0, to).wait_recv()

                @pl.when(goes)
                def _(way=way, blk=blk, to=to):
                    if q == 0:
                        cum_copy(way, blk, s, to).start()
                    kv_copy(way, blk, q, s, to).start()

            if q % every == every - 1:

                @pl.when(two)
                def _():
                    attend(q // every, [b_cw, b_cc])

                @pl.when(one)
                def _():
                    attend(q // every, [b_cw])

        @pl.when(s == conv_at)
        def _():
            convolve()
            send_stats()

        @pl.when(s == stats_at)
        def _():
            finish_conv()

        return carry

    lax.fori_loop(1, half_n + 2, step, 0)

    tops, sums = m_ref[...], l_ref[...]
    logs = tops + jnp.log(sums)
    attn = acc[...] / sums
    log_row = logs[:rows]
    attn_row = attn[:rows]
    for h in range(1, heads):
        attn_row = jnp.where(lane >= h * hd, attn[h * rows : (h + 1) * rows], attn_row)
        log_row = jnp.where(lane >= h, logs[h * rows : (h + 1) * rows], log_row)
    each = rows // n_tp
    attn_row = attn_row.astype(BF16)
    for d in range(n_tp):
        comb[d // 2, d % 2, :, width:] = attn_row[d * each : (d + 1) * each]

    for copy in loads[10:12]:
        copy.wait()
    cut = wo.shape[1] // OUT_CUTS

    def product(core, i):
        lhs = comb[:, core].reshape(nx * each, 2 * width)
        return dot(lhs, wo[:, i * cut : (i + 1) * cut], NN).reshape(nx, each, cut)

    pairs = []
    for i in range(OUT_CUTS):
        pair_out[i] = product(1 - c, i).astype(BF16)
        copy = rdma(pair_out.at[i], pair_in.at[i], pair_send.at[i], pair_recv.at[i], tp=mate)
        copy.start()
        pairs.append(copy)
    outs = []
    for i in range(OUT_CUTS):
        own = product(c, i)
        pairs[i].wait_recv()
        xout[i] = (own + pair_in[i].astype(F32)).astype(BF16)
        for dx in (2, 1, 3):
            dst = at(dx - nx, c)
            copy = rdma(
                xout.at[i, (x + dx) % nx], xin.at[i, dx - 1], x_send.at[i, dx - 1], x_recv.at[i, dx - 1], tp=dst
            )
            copy.start()
            outs.append((i, copy))
    @pl.when(is_low)
    def _():
        pl.semaphore_wait(far_ready, 1)
        cum_copy(1, z, 0, last).start()
        for q in range(CHUNKS):
            kv_copy(1, z, q, 0, last).start()

    log_ref[...] = log_row.T[:heads] + (cum[z] - cum[z][:, 0:1])
    for i in range(OUT_CUTS):
        total = xout[i, x].astype(F32)
        for k, copy in outs:
            if k == i:
                copy.wait_recv()
        for dx in range(nx - 1):
            total = total + xin[i, dx].astype(F32)
        mixed_ref[:, i * cut : (i + 1) * cut] = total.astype(BF16)

    for copy in pending:
        copy.wait_send()
    for way, cond, to in ((0, first_up, up), (1, is_low, last)):

        @pl.when(cond)
        def _(way=way, to=to):
            cum_copy(way, z, 0, to).wait_send()
            for q in range(CHUNKS):
                kv_copy(way, z, q, 0, to).wait_send()

    @pl.when(first_up)
    def _():
        halo_copy.wait_send()

    for k in range(1, n_tp):
        stat_copy(k).wait_send()

    def drain(s, carry):
        cw_in, cw_on, cc_in, cc_on = flows(s)
        for way, goes, blk, to in ((0, cw_on, (z + n - s) % n, up), (1, cc_on, (z + s) % n, down)):

            @pl.when(goes)
            def _(way=way, blk=blk, to=to):
                cum_copy(way, blk, s, to).wait_send()
                for q in range(CHUNKS):
                    kv_copy(way, blk, q, s, to).wait_send()

        return carry

    lax.fori_loop(1, half_n, drain, 0)
    for copy in pairs:
        copy.wait_send()
    for k, copy in outs:
        copy.wait_send()


def solution(mesh):
    n, n_tp = mesh.shape["sp"], mesh.shape["tp"]

    def local(
        inputs,
        norm_gain,
        w_conv_in,
        w_conv_gate,
        conv_kernel,
        ln_gain,
        w_query,
        w_key,
        w_value,
        cum_gate,
        w_conv_out,
        w_attn_out,
    ):
        rows, feat = inputs.shape
        width, full = w_key.shape
        heads = cum_gate.shape[0]
        n_taps = conv_kernel.shape[0]
        each = rows // n_tp
        nx = n_tp // 2
        pad = 32
        cut = full // OUT_CUTS
        half_n = n // 2
        dma = pltpu.SemaphoreType.DMA
        vmem = pltpu.VMEM
        scratch = [
            vmem((n_tp, rows, feat), BF16),
            vmem((n_tp, rows, feat), BF16),
            vmem((1, full), BF16),
            vmem((n_taps, width), BF16),
            vmem((1, width), BF16),
            vmem((2 * width, full), BF16),
            vmem((3 * width, full), BF16),
            vmem((2 * width, full), BF16),
            vmem((n, rows, 2 * width), BF16),
            vmem((n, heads, rows), F32),
            vmem((rows, 2 * width), F32),
            vmem((rows, 128), F32),
            vmem((heads * rows, width), BF16),
            vmem((heads * rows, width), F32),
            vmem((heads * rows, width), F32),
            vmem((heads * rows, width), F32),
            vmem((pad + rows + 8, width), F32),
            vmem((pad, width), BF16),
            vmem((pad, width), BF16),
            vmem((width, rows), F32),
            vmem((n_tp, 2, rows), F32),
            vmem((nx, 2, each, 2 * width), BF16),
            vmem((OUT_CUTS, nx, each, cut), BF16),
            vmem((OUT_CUTS, nx, each, cut), BF16),
            vmem((OUT_CUTS, nx, each, cut), BF16),
            vmem((OUT_CUTS, nx - 1, each, cut), BF16),
            dma((12,)),
            dma((14,)),
            dma((n_tp, 2)),
            dma((2, half_n, CHUNKS)),
            dma((n, CHUNKS)),
            dma((2, half_n)),
            dma((n,)),
            dma((2,)),
            pltpu.SemaphoreType.REGULAR,
            pltpu.SemaphoreType.REGULAR,
            dma((n_tp,)),
            dma((n_tp,)),
            dma((OUT_CUTS,)),
            dma((OUT_CUTS,)),
            dma((OUT_CUTS, nx - 1)),
            dma((OUT_CUTS, nx - 1)),
        ]
        return pl.pallas_call(
            functools.partial(layer, n, n_tp),
            out_shape=(
                jax.ShapeDtypeStruct((each, full), BF16),
                jax.ShapeDtypeStruct((heads, rows), F32),
            ),
            in_specs=[pl.BlockSpec(memory_space=pl.ANY)] * 12,
            out_specs=(pl.BlockSpec(memory_space=pltpu.VMEM), pl.BlockSpec(memory_space=pltpu.VMEM)),
            scratch_shapes=scratch,
            compiler_params=pltpu.CompilerParams(collective_id=0, has_side_effects=True),
        )(
            inputs,
            norm_gain.reshape(1, full),
            w_conv_in,
            w_conv_gate,
            conv_kernel,
            ln_gain.reshape(1, width),
            w_query,
            w_key,
            w_value,
            cum_gate,
            w_conv_out,
            w_attn_out,
        )

    in_specs = (
        P(("grp", "sp"), "tp"),
        P(),
        P("tp", None),
        P("tp", None),
        P(None, "tp"),
        P("tp"),
        P("tp", None),
        P("tp", None),
        P("tp", None),
        P("tp", ("grp", "sp")),
        P("tp", None),
        P("tp", None),
    )
    out_specs = (P(("grp", "sp", "tp"), None), P("tp", ("grp", "sp")))
    return jax.shard_map(local, mesh=mesh, in_specs=in_specs, out_specs=out_specs, check_vma=False)
```

```python
import functools

import jax
import jax.numpy as jnp
from jax import lax
from jax.experimental import pallas as pl
from jax.experimental.pallas import tpu as pltpu
from jax.sharding import PartitionSpec as P

MESH = pl.DeviceIdType.MESH
F32 = jnp.float32
BF16 = jnp.bfloat16
CHUNKS = 8
OUT_CUTS = 2
NT = (((1,), (1,)), ((), ()))
NN = (((1,), (0,)), ((), ()))


def dot(a, b, dims):
    return lax.dot_general(a, b, dims, preferred_element_type=F32)


def layer(
    n,
    n_tp,
    x_hbm,
    gain_hbm,
    wci_hbm,
    wcg_hbm,
    taps_hbm,
    lng_hbm,
    wq_hbm,
    wk_hbm,
    wv_hbm,
    cum_hbm,
    wco_hbm,
    wao_hbm,
    mixed_ref,
    log_ref,
    xg,
    xs,
    gain,
    taps,
    lng,
    wkv,
    w3,
    wo,
    kv,
    cum,
    kvacc,
    sq,
    qs,
    m_ref,
    l_ref,
    acc,
    ext,
    glu_tail,
    halo,
    ctr,
    stats,
    comb,
    pair_out,
    pair_in,
    xout,
    xin,
    ld_sem,
    in_send,
    in_recv,
    kv_send,
    kv_recv,
    cum_send,
    cum_recv,
    halo_sem,
    far_ready,
    st_send,
    st_recv,
    pair_send,
    pair_recv,
    x_send,
    x_recv,
):
    z = lax.axis_index("sp")
    t = lax.axis_index("tp")
    rows, feat = x_hbm.shape
    width = wk_hbm.shape[0]
    heads = cum_hbm.shape[0]
    hd = width // heads
    n_taps = taps_hbm.shape[0]
    half_n = n // 2
    nx = n_tp // 2
    x = t // 2
    c = t % 2

    def at(dx, core):
        return 2 * ((x + dx + nx) % nx) + core

    right, left, far, mate = at(1, c), at(-1, c), at(2, c), at(0, 1 - c)
    up, down = (z + 1) % n, (z + n - 1) % n

    def rdma(src, dst, send, recv, **device):
        return pltpu.make_async_remote_copy(
            src_ref=src, dst_ref=dst, send_sem=send, recv_sem=recv, device_id=device, device_id_type=MESH
        )

    loads = [
        (x_hbm, xg.at[t]),
        (wk_hbm, wkv.at[pl.ds(0, width)]),
        (wv_hbm, wkv.at[pl.ds(width, width)]),
        (gain_hbm, gain),
        (cum_hbm, cum.at[z]),
        (wci_hbm, w3.at[pl.ds(0, width)]),
        (wcg_hbm, w3.at[pl.ds(width, width)]),
        (wq_hbm, w3.at[pl.ds(2 * width, width)]),
        (taps_hbm, taps),
        (lng_hbm, lng),
        (wco_hbm, wo.at[pl.ds(0, width)]),
        (wao_hbm, wo.at[pl.ds(width, width)]),
    ]
    loads = [pltpu.make_async_copy(a, b, ld_sem.at[i]) for i, (a, b) in enumerate(loads)]
    for copy in loads:
        copy.start()

    barrier = pltpu.get_barrier_semaphore()
    for k in range(1, n_tp):
        pl.semaphore_signal(barrier, inc=1, device_id={"tp": (t + k) % n_tp}, device_id_type=MESH)
    last = n - 1
    reach = half_n + 1
    n_low = last - reach
    express = n // 4 + 1
    is_low = z < n_low
    relays_down = z >= reach + 2

    @pl.when(z > 0)
    def _():
        pl.semaphore_signal(barrier, inc=1, device_id={"sp": down}, device_id_type=MESH)

    @pl.when((z >= reach + 1) & (z < last))
    def _():
        pl.semaphore_signal(barrier, inc=1, device_id={"sp": up}, device_id_type=MESH)

    @pl.when(z == express)
    def _():
        pl.semaphore_signal(barrier, inc=1, device_id={"sp": 0}, device_id_type=MESH)

    @pl.when(is_low)
    def _():
        pl.semaphore_signal(barrier, inc=1, device_id={"sp": last}, device_id_type=MESH)

    pl.semaphore_wait(
        barrier,
        n_tp
        - 1
        + jnp.where(z < last, 1, 0)
        + jnp.where(relays_down, 1, 0)
        + jnp.where(z == 0, 1, 0)
        + jnp.where(z == last, n_low, 0),
    )

    def tell(j):
        pl.semaphore_signal(far_ready, inc=1, device_id={"sp": j}, device_id_type=MESH)

    @pl.when(z == last)
    def _():
        for j in range(min(4, n_low)):
            tell(j)

    half = rows // 2
    pending = []

    def part(slot, h):
        return xg.at[slot, pl.ds(h * half, half)]

    def send_in(slot, h, to):
        k = len(pending)
        copy = rdma(part(slot, h), part(slot, h), in_send.at[k], in_recv.at[slot, h], tp=to)
        copy.start()
        pending.append(copy)

    def got(slot, h):
        rdma(part(slot, h), part(slot, h), in_send.at[0], in_recv.at[slot, h], tp=mate).wait_recv()

    loads[0].wait()
    send_in(t, 0, right)
    send_in(t, 1, left)
    send_in(t, 1, right)
    send_in(t, 0, left)
    send_in(t, 0, mate)
    send_in(t, 1, mate)
    for copy in loads[1:4]:
        copy.wait()
    kvacc[...] = jnp.zeros_like(kvacc)
    sq[...] = jnp.zeros_like(sq)

    def process(slot):
        xf = xg[slot].astype(F32)
        lanes = pl.ds(pl.multiple_of(slot * feat, feat), feat)
        s2 = xf * xf
        sq[...] += s2[:, :128] + s2[:, 128:]
        sc = (xf * gain[:, lanes].astype(F32)).astype(BF16)
        xs[slot] = sc
        kvacc[...] += dot(sc, wkv[:, lanes], NT)

    process(t)
    got(mate, 0)
    got(mate, 1)
    process(mate)
    got(left, 0)
    send_in(left, 0, right)
    send_in(left, 0, mate)
    got(right, 1)
    send_in(right, 1, left)
    send_in(right, 1, mate)
    got(left, 1)
    send_in(left, 1, mate)
    got(right, 0)
    send_in(right, 0, mate)
    process(left)
    process(right)
    for slot in (at(-1, 1 - c), at(1, 1 - c)):
        got(slot, 0)
        got(slot, 1)
        process(slot)
    got(far, 0)
    send_in(far, 0, mate)
    got(far, 1)
    send_in(far, 1, mate)
    process(far)
    got(at(2, 1 - c), 0)
    got(at(2, 1 - c), 1)
    process(at(2, 1 - c))

    rms = lax.rsqrt(jnp.sum(sq[...], axis=1, keepdims=True) / (feat * n_tp) + 1e-06)
    kv[z] = (kvacc[...] * rms).astype(BF16)
    loads[4].wait()

    chunk = rows // CHUNKS

    def kv_copy(way, blk, q, k, to):
        ref = kv.at[blk, pl.ds(q * chunk, chunk)]
        return rdma(ref, ref, kv_send.at[way, k, q], kv_recv.at[blk, q], sp=to)

    def cum_copy(way, blk, k, to):
        return rdma(cum.at[blk], cum.at[blk], cum_send.at[way, k], cum_recv.at[blk], sp=to)

    first_up = z < last

    @pl.when(first_up)
    def _():
        cum_copy(0, z, 0, up).start()
        for q in range(CHUNKS):
            kv_copy(0, z, q, 0, up).start()

    for copy in loads[5:8]:
        copy.wait()
    r3 = dot(xs[0], w3[:, :feat], NT)
    for p in range(1, n_tp):
        r3 += dot(xs[p], w3[:, p * feat : (p + 1) * feat], NT)
    r3 = r3 * rms
    glu = (r3[:, :width] * jax.nn.sigmoid(r3[:, width : 2 * width])).astype(BF16)
    pad = glu_tail.shape[0]
    glu_tail[...] = glu[rows - pad :]
    ext[pl.ds(pad, rows)] = glu.astype(F32)
    ext[pl.ds(pad + rows, 8)] = jnp.zeros((8, width), F32)
    query = (r3[:, 2 * width :]).astype(BF16) * jnp.asarray(hd ** (-0.5), BF16)
    lane = lax.broadcasted_iota(jnp.int32, (rows, width), 1)
    for h in range(heads):
        mine = (lane >= h * hd) & (lane < (h + 1) * hd)
        qs[pl.ds(h * rows, rows)] = jnp.where(mine, query.astype(F32), 0.0).astype(BF16)
    halo_copy = rdma(glu_tail, halo, halo_sem.at[0], halo_sem.at[1], sp=up)

    @pl.when(first_up)
    def _():
        halo_copy.start()

    ones = jnp.ones((rows, width), BF16)

    def attend(h, blocks, diagonal=False):
        here = pl.ds(h * rows, rows)
        q = qs[here]
        scores = []
        for blk in blocks:
            s = dot(q, kv[blk, :, :width], NT)
            s = s + (cum[z, h : h + 1, 0:1] - cum[blk, h : h + 1, :])
            if diagonal:
                q_pos = lax.broadcasted_iota(jnp.int32, s.shape, 0)
                k_pos = lax.broadcasted_iota(jnp.int32, s.shape, 1)
                s = jnp.where(k_pos <= q_pos, s, -1e30)
            scores.append(s)
        best = scores[0]
        for s in scores[1:]:
            best = jnp.maximum(best, s)
        m_new = jnp.broadcast_to(jnp.max(best, axis=1, keepdims=True), (rows, width))
        if not diagonal:
            m_old = m_ref[here]
            m_new = jnp.maximum(m_old, m_new)
        m_ref[here] = m_new
        wide = jnp.concatenate([m_new] * (rows // width), axis=1)
        out = None
        for blk, s in zip(blocks, scores):
            p = jnp.exp(s - wide).astype(BF16)
            o = dot(p, jnp.concatenate([kv[blk, :, width:], ones], axis=1), NN)
            out = o if out is None else out + o
        if diagonal:
            acc[here] = out[:, :width]
            l_ref[here] = out[:, width:]
        else:
            fade = jnp.exp(m_old - m_new)
            acc[here] = acc[here] * fade + out[:, :width]
            l_ref[here] = l_ref[here] * fade + out[:, width:]

    for h in range(heads):
        attend(h, [z], diagonal=True)

    def convolve():
        loads[8].wait()

        @pl.when(z > 0)
        def _():
            halo_copy.wait_recv()
            ext[pl.ds(0, pad)] = halo[...].astype(F32)

        @pl.when(z == 0)
        def _():
            ext[pl.ds(0, pad)] = jnp.zeros((pad, width), F32)

        weight = taps[...].astype(F32)
        shift = pad - (n_taps - 1)
        long = rows + 8
        total = jnp.zeros((rows, width), F32)
        for r in range(8):
            sub = None
            for j in range(n_taps):
                if (shift + j) % 8 == r:
                    base = shift + j - r
                    if r == 0:
                        term = ext[pl.ds(base, rows)] * weight[j : j + 1]
                    else:
                        term = ext[pl.ds(base, long)] * weight[j : j + 1]
                    sub = term if sub is None else sub + term
            if r == 0:
                total = total + sub
            else:
                total = total + pltpu.roll(sub, long - r, 0)[:rows]
        turned = total.T
        ctr[...] = turned
        stats[t, 0:1] = jnp.sum(turned, axis=0, keepdims=True)
        stats[t, 1:2] = jnp.sum(turned * turned, axis=0, keepdims=True)

    def stat_copy(k):
        return rdma(stats.at[t], stats.at[t], st_send.at[k], st_recv.at[t], tp=(t + k) % n_tp)

    def send_stats():
        for k in range(1, n_tp):
            stat_copy(k).start()

    def finish_conv():
        for k in range(1, n_tp):
            src = (t + k) % n_tp
            rdma(stats.at[src], stats.at[src], st_send.at[0], st_recv.at[src], tp=src).wait_recv()
        loads[9].wait()
        tot = stats[0]
        for p in range(1, n_tp):
            tot = tot + stats[p]
        mean = tot[0:1] / (width * n_tp)
        var = tot[1:2] / (width * n_tp) - mean * mean
        y = ((ctr[...] - mean) * lax.rsqrt(var + 1e-05)).T
        y = y * lng[...].astype(F32)
        y = (y * jax.nn.sigmoid(y)).astype(BF16)
        each = rows // n_tp
        for d in range(n_tp):
            comb[d // 2, d % 2, :, :width] = y[d * each : (d + 1) * each]

    conv_at = 2
    stats_at = min(5, half_n + 1)

    lag = jnp.maximum(last - z, 0) // 2

    def flow_up(s):
        comes = (z >= s) & (s <= reach)
        goes = comes & (z < last) & (s < reach) & jnp.logical_not((z == s) & (z == express - 1))
        return comes, goes

    def flow_down(s):
        comes = (s >= 1) & (z + s >= n) & (s <= n_low)
        goes = comes & (s < n_low) & relays_down
        return comes, goes

    def send_far():
        @pl.when(z == 0)
        def _():
            cum_copy(1, z, 1, express).start()
            for q in range(CHUNKS):
                kv_copy(1, z, q, 1, express).start()

        pl.semaphore_wait(far_ready, 1)
        cum_copy(1, z, 0, last).start()
        for q in range(CHUNKS):
            kv_copy(1, z, q, 0, last).start()

    def step(s, carry):
        d = s - lag
        cw_in, cw_on = flow_up(s)
        cc_in, cc_on = flow_down(d)
        j_cw, j_cc = (z + n - s) % n, (z + n + d) % n
        b_cw, b_cc = (z + n - s + 1) % n, (z + n + d - 1) % n
        has_cw = (z >= s - 1) & (s > 1) & (s - 1 <= reach)
        has_cc, _ = flow_down(d - 1)
        two = has_cw & has_cc
        one = has_cw ^ has_cc
        every = CHUNKS // heads

        @pl.when(is_low & (s == jnp.maximum(z, 1)))
        def _():
            send_far()

        for q in range(CHUNKS):
            for way, arrives, goes, blk, to, k in (
                (0, cw_in, cw_on, j_cw, up, s),
                (1, cc_in, cc_on, j_cc, down, d),
            ):

                @pl.when(arrives)
                def _(way=way, blk=blk, to=to):
                    if q == 0:
                        cum_copy(way, blk, 0, to).wait_recv()
                    kv_copy(way, blk, q, 0, to).wait_recv()

                @pl.when(goes)
                def _(way=way, blk=blk, to=to, k=k):
                    if q == 0:
                        cum_copy(way, blk, k, to).start()
                    kv_copy(way, blk, q, k, to).start()

            if q % every == every - 1:

                @pl.when(two)
                def _():
                    attend(q // every, [b_cw, b_cc])

                @pl.when(one)
                def _():
                    attend(q // every, [jnp.where(has_cw, b_cw, b_cc)])

        @pl.when((z == last) & cc_in)
        def _():
            for j in (2 * s + 2, 2 * s + 3):

                @pl.when(j < n_low)
                def _(j=j):
                    tell(j)

        @pl.when(s == conv_at)
        def _():
            convolve()
            send_stats()

        @pl.when(s == stats_at)
        def _():
            finish_conv()

        return carry

    lax.fori_loop(1, max(reach + 1, n_low + 1 + (n_low - 1) // 2) + 1, step, 0)

    tops, sums = m_ref[...], l_ref[...]
    logs = tops + jnp.log(sums)
    attn = acc[...] / sums
    log_row = logs[:rows]
    attn_row = attn[:rows]
    for h in range(1, heads):
        attn_row = jnp.where(lane >= h * hd, attn[h * rows : (h + 1) * rows], attn_row)
        log_row = jnp.where(lane >= h, logs[h * rows : (h + 1) * rows], log_row)
    each = rows // n_tp
    attn_row = attn_row.astype(BF16)
    for d in range(n_tp):
        comb[d // 2, d % 2, :, width:] = attn_row[d * each : (d + 1) * each]

    for copy in loads[10:12]:
        copy.wait()
    cut = wo.shape[1] // OUT_CUTS

    def product(core, i):
        lhs = comb[:, core].reshape(nx * each, 2 * width)
        return dot(lhs, wo[:, i * cut : (i + 1) * cut], NN).reshape(nx, each, cut)

    pairs = []
    for i in range(OUT_CUTS):
        pair_out[i] = product(1 - c, i).astype(BF16)
        copy = rdma(pair_out.at[i], pair_in.at[i], pair_send.at[i], pair_recv.at[i], tp=mate)
        copy.start()
        pairs.append(copy)
    outs = []
    for i in range(OUT_CUTS):
        own = product(c, i)
        pairs[i].wait_recv()
        xout[i] = (own + pair_in[i].astype(F32)).astype(BF16)
        for dx in (2, 1, 3):
            dst = at(dx - nx, c)
            copy = rdma(
                xout.at[i, (x + dx) % nx], xin.at[i, dx - 1], x_send.at[i, dx - 1], x_recv.at[i, dx - 1], tp=dst
            )
            copy.start()
            outs.append((i, copy))
    log_ref[...] = log_row.T[:heads] + (cum[z] - cum[z][:, 0:1])
    for i in range(OUT_CUTS):
        total = xout[i, x].astype(F32)
        for k, copy in outs:
            if k == i:
                copy.wait_recv()
        for dx in range(nx - 1):
            total = total + xin[i, dx].astype(F32)
        mixed_ref[:, i * cut : (i + 1) * cut] = total.astype(BF16)

    for copy in pending:
        copy.wait_send()
    for way, cond, to in ((0, first_up, up), (1, is_low, last)):

        @pl.when(cond)
        def _(way=way, to=to):
            cum_copy(way, z, 0, to).wait_send()
            for q in range(CHUNKS):
                kv_copy(way, z, q, 0, to).wait_send()

    @pl.when(first_up)
    def _():
        halo_copy.wait_send()

    for k in range(1, n_tp):
        stat_copy(k).wait_send()

    @pl.when(z == 0)
    def _():
        cum_copy(1, z, 1, express).wait_send()
        for q in range(CHUNKS):
            kv_copy(1, z, q, 1, express).wait_send()

    def drain(s, carry):
        for way, goes, blk, to in (
            (0, flow_up(s)[1], (z + n - s) % n, up),
            (1, flow_down(s)[1], (z + s) % n, down),
        ):

            @pl.when(goes)
            def _(way=way, blk=blk, to=to):
                cum_copy(way, blk, s, to).wait_send()
                for q in range(CHUNKS):
                    kv_copy(way, blk, q, s, to).wait_send()

        return carry

    lax.fori_loop(1, reach, drain, 0)
    for copy in pairs:
        copy.wait_send()
    for k, copy in outs:
        copy.wait_send()


def solution(mesh):
    n, n_tp = mesh.shape["sp"], mesh.shape["tp"]

    def local(
        inputs,
        norm_gain,
        w_conv_in,
        w_conv_gate,
        conv_kernel,
        ln_gain,
        w_query,
        w_key,
        w_value,
        cum_gate,
        w_conv_out,
        w_attn_out,
    ):
        rows, feat = inputs.shape
        width, full = w_key.shape
        heads = cum_gate.shape[0]
        n_taps = conv_kernel.shape[0]
        each = rows // n_tp
        nx = n_tp // 2
        pad = 32
        cut = full // OUT_CUTS
        half_n = n // 2
        dma = pltpu.SemaphoreType.DMA
        vmem = pltpu.VMEM
        scratch = [
            vmem((n_tp, rows, feat), BF16),
            vmem((n_tp, rows, feat), BF16),
            vmem((1, full), BF16),
            vmem((n_taps, width), BF16),
            vmem((1, width), BF16),
            vmem((2 * width, full), BF16),
            vmem((3 * width, full), BF16),
            vmem((2 * width, full), BF16),
            vmem((n, rows, 2 * width), BF16),
            vmem((n, heads, rows), F32),
            vmem((rows, 2 * width), F32),
            vmem((rows, 128), F32),
            vmem((heads * rows, width), BF16),
            vmem((heads * rows, width), F32),
            vmem((heads * rows, width), F32),
            vmem((heads * rows, width), F32),
            vmem((pad + rows + 8, width), F32),
            vmem((pad, width), BF16),
            vmem((pad, width), BF16),
            vmem((width, rows), F32),
            vmem((n_tp, 2, rows), F32),
            vmem((nx, 2, each, 2 * width), BF16),
            vmem((OUT_CUTS, nx, each, cut), BF16),
            vmem((OUT_CUTS, nx, each, cut), BF16),
            vmem((OUT_CUTS, nx, each, cut), BF16),
            vmem((OUT_CUTS, nx - 1, each, cut), BF16),
            dma((12,)),
            dma((14,)),
            dma((n_tp, 2)),
            dma((2, half_n + 1, CHUNKS)),
            dma((n, CHUNKS)),
            dma((2, half_n + 1)),
            dma((n,)),
            dma((2,)),
            pltpu.SemaphoreType.REGULAR,
            dma((n_tp,)),
            dma((n_tp,)),
            dma((OUT_CUTS,)),
            dma((OUT_CUTS,)),
            dma((OUT_CUTS, nx - 1)),
            dma((OUT_CUTS, nx - 1)),
        ]
        return pl.pallas_call(
            functools.partial(layer, n, n_tp),
            out_shape=(
                jax.ShapeDtypeStruct((each, full), BF16),
                jax.ShapeDtypeStruct((heads, rows), F32),
            ),
            in_specs=[pl.BlockSpec(memory_space=pl.ANY)] * 12,
            out_specs=(pl.BlockSpec(memory_space=pltpu.VMEM), pl.BlockSpec(memory_space=pltpu.VMEM)),
            scratch_shapes=scratch,
            compiler_params=pltpu.CompilerParams(collective_id=0, has_side_effects=True),
        )(
            inputs,
            norm_gain.reshape(1, full),
            w_conv_in,
            w_conv_gate,
            conv_kernel,
            ln_gain.reshape(1, width),
            w_query,
            w_key,
            w_value,
            cum_gate,
            w_conv_out,
            w_attn_out,
        )

    in_specs = (
        P(("grp", "sp"), "tp"),
        P(),
        P("tp", None),
        P("tp", None),
        P(None, "tp"),
        P("tp"),
        P("tp", None),
        P("tp", None),
        P("tp", None),
        P("tp", ("grp", "sp")),
        P("tp", None),
        P("tp", None),
    )
    out_specs = (P(("grp", "sp", "tp"), None), P("tp", ("grp", "sp")))
    return jax.shard_map(local, mesh=mesh, in_specs=in_specs, out_specs=out_specs, check_vma=False)
```

```python
import functools

import jax
import jax.numpy as jnp
from jax import lax
from jax.experimental import pallas as pl
from jax.experimental.pallas import tpu as pltpu
from jax.sharding import PartitionSpec as P

MESH = pl.DeviceIdType.MESH
F32 = jnp.float32
BF16 = jnp.bfloat16
CHUNKS = 4
OUT_CUTS = 2
NT = (((1,), (1,)), ((), ()))
NN = (((1,), (0,)), ((), ()))


def dot(a, b, dims):
    return lax.dot_general(a, b, dims, preferred_element_type=F32)


def layer(
    n,
    n_tp,
    x_hbm,
    gain_hbm,
    wci_hbm,
    wcg_hbm,
    taps_hbm,
    lng_hbm,
    wq_hbm,
    wk_hbm,
    wv_hbm,
    cum_hbm,
    wco_hbm,
    wao_hbm,
    mixed_ref,
    log_ref,
    xg,
    xs,
    gain,
    gain32,
    taps,
    lng,
    wkv,
    w3,
    wo,
    kv,
    cum,
    kvacc,
    sq,
    qs,
    m_ref,
    l_ref,
    acc,
    ext,
    glu_tail,
    halo,
    ctr,
    stats,
    comb,
    pair_out,
    pair_in,
    xout,
    xin,
    ld_sem,
    in_send,
    in_recv,
    kv_send,
    kv_recv,
    cum_send,
    cum_recv,
    halo_sem,
    far_ready,
    st_send,
    st_recv,
    pair_send,
    pair_recv,
    x_send,
    x_recv,
):
    z = lax.axis_index("sp")
    t = lax.axis_index("tp")
    rows, feat = x_hbm.shape
    width = wk_hbm.shape[0]
    heads = cum_hbm.shape[0]
    hd = width // heads
    n_taps = taps_hbm.shape[0]
    half_n = n // 2
    nx = n_tp // 2
    x = t // 2
    c = t % 2

    def at(dx, core):
        return 2 * ((x + dx + nx) % nx) + core

    right, left, far, mate = at(1, c), at(-1, c), at(2, c), at(0, 1 - c)
    up, down = (z + 1) % n, (z + n - 1) % n

    def rdma(src, dst, send, recv, **device):
        return pltpu.make_async_remote_copy(
            src_ref=src, dst_ref=dst, send_sem=send, recv_sem=recv, device_id=device, device_id_type=MESH
        )

    loads = [
        (x_hbm, xg.at[t]),
        (wk_hbm, wkv.at[pl.ds(0, width)]),
        (wv_hbm, wkv.at[pl.ds(width, width)]),
        (gain_hbm, gain),
        (cum_hbm, cum.at[z]),
        (wci_hbm, w3.at[pl.ds(0, width)]),
        (wcg_hbm, w3.at[pl.ds(width, width)]),
        (wq_hbm, w3.at[pl.ds(2 * width, width)]),
        (taps_hbm, taps),
        (lng_hbm, lng),
        (wco_hbm, wo.at[pl.ds(0, width)]),
        (wao_hbm, wo.at[pl.ds(width, width)]),
    ]
    loads = [pltpu.make_async_copy(a, b, ld_sem.at[i]) for i, (a, b) in enumerate(loads)]
    for copy in loads:
        copy.start()

    barrier = pltpu.get_barrier_semaphore()
    for k in range(1, n_tp):
        pl.semaphore_signal(barrier, inc=1, device_id={"tp": (t + k) % n_tp}, device_id_type=MESH)
    last = n - 1
    reach = half_n + 1
    n_low = last - reach
    express = n // 4 + 1
    first_tells = 4
    is_low = z < n_low
    relays_down = z >= reach + 2

    @pl.when(z > 0)
    def _():
        pl.semaphore_signal(barrier, inc=1, device_id={"sp": down}, device_id_type=MESH)

    @pl.when((z >= reach + 1) & (z < last))
    def _():
        pl.semaphore_signal(barrier, inc=1, device_id={"sp": up}, device_id_type=MESH)

    @pl.when(z == express)
    def _():
        pl.semaphore_signal(barrier, inc=1, device_id={"sp": 0}, device_id_type=MESH)

    @pl.when(is_low)
    def _():
        pl.semaphore_signal(barrier, inc=1, device_id={"sp": last}, device_id_type=MESH)

    pl.semaphore_wait(
        barrier,
        n_tp
        - 1
        + jnp.where(z < last, 1, 0)
        + jnp.where(relays_down, 1, 0)
        + jnp.where(z == 0, 1, 0)
        + jnp.where(z == last, n_low, 0),
    )

    def tell(j):
        pl.semaphore_signal(far_ready, inc=1, device_id={"sp": j}, device_id_type=MESH)

    @pl.when(z == last)
    def _():
        for j in range(min(first_tells, n_low)):
            tell(j)

    half = rows // 2
    pending = []

    def part(slot, h):
        return xg.at[slot, pl.ds(h * half, half)]

    def send_in(slot, h, to):
        k = len(pending)
        copy = rdma(part(slot, h), part(slot, h), in_send.at[k], in_recv.at[slot, h], tp=to)
        copy.start()
        pending.append(copy)

    def got(slot, h):
        rdma(part(slot, h), part(slot, h), in_send.at[0], in_recv.at[slot, h], tp=mate).wait_recv()

    loads[0].wait()
    send_in(t, 0, right)
    send_in(t, 1, left)
    send_in(t, 1, right)
    send_in(t, 0, left)
    send_in(t, 0, mate)
    send_in(t, 1, mate)
    for copy in loads[1:4]:
        copy.wait()
    gain32[...] = gain[...].astype(F32)
    kvacc[...] = jnp.zeros_like(kvacc)
    sq[...] = jnp.zeros_like(sq)

    def process(slot):
        xf = xg[slot].astype(F32)
        lanes = pl.ds(pl.multiple_of(slot * feat, feat), feat)
        s2 = xf * xf
        sq[...] += s2[:, :128] + s2[:, 128:]
        scale = [gain32[pl.ds(slot * (feat // 128) + i, 1)] for i in range(feat // 128)]
        sc = (xf * jnp.concatenate(scale, axis=1)).astype(BF16)
        xs[slot] = sc
        kvacc[...] += dot(sc, wkv[:, lanes], NT)

    process(t)
    got(mate, 0)
    got(mate, 1)
    process(mate)
    got(left, 0)
    send_in(left, 0, right)
    send_in(left, 0, mate)
    got(right, 1)
    send_in(right, 1, left)
    send_in(right, 1, mate)
    got(left, 1)
    send_in(left, 1, mate)
    got(right, 0)
    send_in(right, 0, mate)
    process(left)
    process(right)
    for slot in (at(-1, 1 - c), at(1, 1 - c)):
        got(slot, 0)
        got(slot, 1)
        process(slot)
    got(far, 0)
    send_in(far, 0, mate)
    got(far, 1)
    send_in(far, 1, mate)
    process(far)
    got(at(2, 1 - c), 0)
    got(at(2, 1 - c), 1)
    process(at(2, 1 - c))

    rms = lax.rsqrt(jnp.sum(sq[...], axis=1, keepdims=True) / (feat * n_tp) + 1e-06)
    kv[z] = (kvacc[...] * rms).astype(BF16)
    loads[4].wait()

    chunk = rows // CHUNKS

    def kv_copy(way, blk, q, k, to):
        ref = kv.at[blk, pl.ds(q * chunk, chunk)]
        return rdma(ref, ref, kv_send.at[way, k % 2, q], kv_recv.at[blk, q], sp=to)

    def cum_copy(way, blk, k, to):
        return rdma(cum.at[blk], cum.at[blk], cum_send.at[way, k % 2], cum_recv.at[blk], sp=to)

    first_up = z < last

    @pl.when(z == last)
    def _():
        for j in range(first_tells, min(first_tells + 2, n_low)):
            tell(j)

    @pl.when(first_up)
    def _():
        cum_copy(0, z, 0, up).start()
        for q in range(CHUNKS):
            kv_copy(0, z, q, 0, up).start()

    for copy in loads[5:8]:
        copy.wait()
    r3 = dot(xs[0], w3[:, :feat], NT)
    for p in range(1, n_tp):
        r3 += dot(xs[p], w3[:, p * feat : (p + 1) * feat], NT)
    r3 = r3 * rms
    glu = (r3[:, :width] * jax.nn.sigmoid(r3[:, width : 2 * width])).astype(BF16)
    pad = glu_tail.shape[0]
    glu_tail[...] = glu[rows - pad :]
    ext[pl.ds(pad, rows)] = glu.astype(F32)
    ext[pl.ds(pad + rows, 8)] = jnp.zeros((8, width), F32)
    query = (r3[:, 2 * width :]).astype(BF16) * jnp.asarray(hd ** (-0.5), BF16)
    lane = lax.broadcasted_iota(jnp.int32, (rows, width), 1)
    for h in range(heads):
        mine = (lane >= h * hd) & (lane < (h + 1) * hd)
        qs[pl.ds(h * rows, rows)] = jnp.where(mine, query.astype(F32), 0.0).astype(BF16)
    halo_copy = rdma(glu_tail, halo, halo_sem.at[0], halo_sem.at[1], sp=up)

    @pl.when(first_up)
    def _():
        halo_copy.start()

    ones = jnp.ones((rows, width), BF16)

    def attend(h, blocks, diagonal=False):
        here = pl.ds(h * rows, rows)
        q = qs[here]
        scores = []
        for blk in blocks:
            s = dot(q, kv[blk, :, :width], NT)
            s = s + (cum[z, h : h + 1, 0:1] - cum[blk, h : h + 1, :])
            if diagonal:
                q_pos = lax.broadcasted_iota(jnp.int32, s.shape, 0)
                k_pos = lax.broadcasted_iota(jnp.int32, s.shape, 1)
                s = jnp.where(k_pos <= q_pos, s, -1e30)
            scores.append(s)
        best = scores[0]
        for s in scores[1:]:
            best = jnp.maximum(best, s)
        m_new = jnp.broadcast_to(jnp.max(best, axis=1, keepdims=True), (rows, width))
        if not diagonal:
            m_old = m_ref[here]
            m_new = jnp.maximum(m_old, m_new)
        m_ref[here] = m_new
        wide = jnp.concatenate([m_new] * (rows // width), axis=1)
        out = None
        for blk, s in zip(blocks, scores):
            p = jnp.exp(s - wide).astype(BF16)
            o = dot(p, jnp.concatenate([kv[blk, :, width:], ones], axis=1), NN)
            out = o if out is None else out + o
        if diagonal:
            acc[here] = out[:, :width]
            l_ref[here] = out[:, width:]
        else:
            fade = jnp.exp(m_old - m_new)
            acc[here] = acc[here] * fade + out[:, :width]
            l_ref[here] = l_ref[here] * fade + out[:, width:]

    for h in range(heads):
        attend(h, [z], diagonal=True)

    def convolve():
        loads[8].wait()

        @pl.when(z > 0)
        def _():
            halo_copy.wait_recv()
            ext[pl.ds(0, pad)] = halo[...].astype(F32)

        @pl.when(z == 0)
        def _():
            ext[pl.ds(0, pad)] = jnp.zeros((pad, width), F32)

        weight = taps[...].astype(F32)
        shift = pad - (n_taps - 1)
        long = rows + 8
        total = jnp.zeros((rows, width), F32)
        for r in range(8):
            sub = None
            for j in range(n_taps):
                if (shift + j) % 8 == r:
                    base = shift + j - r
                    if r == 0:
                        term = ext[pl.ds(base, rows)] * weight[j : j + 1]
                    else:
                        term = ext[pl.ds(base, long)] * weight[j : j + 1]
                    sub = term if sub is None else sub + term
            if r == 0:
                total = total + sub
            else:
                total = total + pltpu.roll(sub, long - r, 0)[:rows]
        turned = total.T
        ctr[...] = turned
        stats[t, 0:1] = jnp.sum(turned, axis=0, keepdims=True)
        stats[t, 1:2] = jnp.sum(turned * turned, axis=0, keepdims=True)

    def stat_copy(k):
        return rdma(stats.at[t], stats.at[t], st_send.at[k], st_recv.at[t], tp=(t + k) % n_tp)

    def send_stats():
        for k in range(1, n_tp):
            stat_copy(k).start()

    def finish_conv():
        for k in range(1, n_tp):
            src = (t + k) % n_tp
            rdma(stats.at[src], stats.at[src], st_send.at[0], st_recv.at[src], tp=src).wait_recv()
        loads[9].wait()
        tot = stats[0]
        for p in range(1, n_tp):
            tot = tot + stats[p]
        mean = tot[0:1] / (width * n_tp)
        var = tot[1:2] / (width * n_tp) - mean * mean
        y = ((ctr[...] - mean) * lax.rsqrt(var + 1e-05)).T
        y = y * lng[...].astype(F32)
        y = (y * jax.nn.sigmoid(y)).astype(BF16)
        each = rows // n_tp
        for d in range(n_tp):
            comb[d // 2, d % 2, :, :width] = y[d * each : (d + 1) * each]

    conv_at = 2
    stats_at = min(5, half_n + 1)

    lag = jnp.maximum(last - z, 0) // 2

    def flow_up(s):
        comes = (z >= s) & (s <= reach)
        goes = comes & (z < last) & (s < reach) & jnp.logical_not((z == s) & (z == express - 1))
        return comes, goes

    def flow_down(s):
        comes = (s >= 1) & (z + s >= n) & (s <= n_low)
        goes = comes & (s < n_low) & relays_down
        return comes, goes

    def send_far():
        @pl.when(z == 0)
        def _():
            cum_copy(1, z, 1, express).start()
            for q in range(CHUNKS):
                kv_copy(1, z, q, 1, express).start()

        pl.semaphore_wait(far_ready, 1)
        cum_copy(1, z, 0, last).start()
        for q in range(CHUNKS):
            kv_copy(1, z, q, 0, last).start()

    def step(s, carry):
        d = s - lag
        cw_in, cw_on = flow_up(s)
        cc_in, cc_on = flow_down(d)
        j_cw, j_cc = (z + n - s) % n, (z + n + d) % n
        b_cw, b_cc = (z + n - s + 1) % n, (z + n + d - 1) % n
        has_cw = (z >= s - 1) & (s > 1) & (s - 1 <= reach)
        has_cc, _ = flow_down(d - 1)
        two = has_cw & has_cc
        one = has_cw ^ has_cc
        every = CHUNKS // heads

        @pl.when(is_low & (z < express) & (s == jnp.maximum(z, 1)))
        def _():
            send_far()

        for q in range(CHUNKS):
            for way, arrives, goes, blk, to, k, again in (
                (0, cw_in, cw_on, j_cw, up, s, s >= 2),
                (1, cc_in, cc_on, j_cc, down, d, d - 2 >= n - z),
            ):

                @pl.when(arrives)
                def _(way=way, blk=blk, to=to):
                    if q == 0:
                        cum_copy(way, blk, 0, to).wait_recv()
                    kv_copy(way, blk, q, 0, to).wait_recv()

                @pl.when(goes & again)
                def _(way=way, blk=blk, to=to, k=k):
                    if q == 0:
                        cum_copy(way, blk, k, to).wait_send()
                    kv_copy(way, blk, q, k, to).wait_send()

                @pl.when(goes)
                def _(way=way, blk=blk, to=to, k=k):
                    if q == 0:
                        cum_copy(way, blk, k, to).start()
                    kv_copy(way, blk, q, k, to).start()

            if q % every == every - 1:

                @pl.when(two)
                def _():
                    attend(q // every, [b_cw, b_cc])

                @pl.when(one)
                def _():
                    attend(q // every, [jnp.where(has_cw, b_cw, b_cc)])

        @pl.when((z == last) & (s <= n_low))
        def _():
            first = first_tells + 2 + s + s // 2
            for j, really in ((first - 1, s % 2 < 2), (first, s % 2 == 1)):

                @pl.when(really & (j < n_low))
                def _(j=j):
                    tell(j)

        @pl.when(s == conv_at)
        def _():
            convolve()
            send_stats()

        @pl.when(s == stats_at)
        def _():
            finish_conv()

        return carry

    steps = jnp.where(
        z > reach,
        jnp.maximum(reach + 1, n_low + 1 + lag),
        jnp.maximum(z + 1, stats_at),
    )
    lax.fori_loop(1, steps + 1, step, 0)

    tops, sums = m_ref[...], l_ref[...]
    logs = tops + jnp.log(sums)
    attn = acc[...] / sums
    log_row = logs[:rows]
    attn_row = attn[:rows]
    for h in range(1, heads):
        attn_row = jnp.where(lane >= h * hd, attn[h * rows : (h + 1) * rows], attn_row)
        log_row = jnp.where(lane >= h, logs[h * rows : (h + 1) * rows], log_row)
    each = rows // n_tp
    attn_row = attn_row.astype(BF16)
    for d in range(n_tp):
        comb[d // 2, d % 2, :, width:] = attn_row[d * each : (d + 1) * each]

    for copy in loads[10:12]:
        copy.wait()
    cut = wo.shape[1] // OUT_CUTS

    def product(core, i):
        lhs = comb[:, core].reshape(nx * each, 2 * width)
        return dot(lhs, wo[:, i * cut : (i + 1) * cut], NN).reshape(nx, each, cut)

    pairs = []
    for i in range(OUT_CUTS):
        pair_out[i] = product(1 - c, i).astype(BF16)
        copy = rdma(pair_out.at[i], pair_in.at[i], pair_send.at[i], pair_recv.at[i], tp=mate)
        copy.start()
        pairs.append(copy)
    outs = []
    for i in range(OUT_CUTS):
        own = product(c, i)
        pairs[i].wait_recv()
        xout[i] = (own + pair_in[i].astype(F32)).astype(BF16)
        for dx in (2, 1, 3):
            dst = at(dx - nx, c)
            copy = rdma(
                xout.at[i, (x + dx) % nx], xin.at[i, dx - 1], x_send.at[i, dx - 1], x_recv.at[i, dx - 1], tp=dst
            )
            copy.start()
            outs.append((i, copy))
    @pl.when(is_low & (z >= express))
    def _():
        send_far()

    log_ref[...] = log_row.T[:heads] + (cum[z] - cum[z][:, 0:1])
    for i in range(OUT_CUTS):
        total = xout[i, x].astype(F32)
        for k, copy in outs:
            if k == i:
                copy.wait_recv()
        for dx in range(nx - 1):
            total = total + xin[i, dx].astype(F32)
        mixed_ref[:, i * cut : (i + 1) * cut] = total.astype(BF16)

    for copy in pending:
        copy.wait_send()
    ups = jnp.minimum(z, reach - 1) - jnp.where(z == express - 1, 1, 0) + 1
    downs = z - (reach + 1)
    for way, parity, cond in (
        (0, 0, first_up),
        (0, 1, first_up & (ups > 1)),
        (1, 0, is_low | (downs > 1) | ((downs == 1) & ((n_low - 1) % 2 == 0))),
        (1, 1, (z == 0) | (downs > 1) | ((downs == 1) & ((n_low - 1) % 2 == 1))),
    ):

        @pl.when(cond)
        def _(way=way, parity=parity):
            cum_copy(way, z, parity, up).wait_send()
            for q in range(CHUNKS):
                kv_copy(way, z, q, parity, up).wait_send()

    @pl.when(first_up)
    def _():
        halo_copy.wait_send()

    for k in range(1, n_tp):
        stat_copy(k).wait_send()

    for copy in pairs:
        copy.wait_send()
    for k, copy in outs:
        copy.wait_send()


def solution(mesh):
    n, n_tp = mesh.shape["sp"], mesh.shape["tp"]

    def local(
        inputs,
        norm_gain,
        w_conv_in,
        w_conv_gate,
        conv_kernel,
        ln_gain,
        w_query,
        w_key,
        w_value,
        cum_gate,
        w_conv_out,
        w_attn_out,
    ):
        rows, feat = inputs.shape
        width, full = w_key.shape
        heads = cum_gate.shape[0]
        n_taps = conv_kernel.shape[0]
        each = rows // n_tp
        nx = n_tp // 2
        pad = 32
        cut = full // OUT_CUTS
        half_n = n // 2
        dma = pltpu.SemaphoreType.DMA
        vmem = pltpu.VMEM
        scratch = [
            vmem((n_tp, rows, feat), BF16),
            vmem((n_tp, rows, feat), BF16),
            vmem((full // 128, 128), BF16),
            vmem((full // 128, 128), F32),
            vmem((n_taps, width), BF16),
            vmem((1, width), BF16),
            vmem((2 * width, full), BF16),
            vmem((3 * width, full), BF16),
            vmem((2 * width, full), BF16),
            vmem((n, rows, 2 * width), BF16),
            vmem((n, heads, rows), F32),
            vmem((rows, 2 * width), F32),
            vmem((rows, 128), F32),
            vmem((heads * rows, width), BF16),
            vmem((heads * rows, width), F32),
            vmem((heads * rows, width), F32),
            vmem((heads * rows, width), F32),
            vmem((pad + rows + 8, width), F32),
            vmem((pad, width), BF16),
            vmem((pad, width), BF16),
            vmem((width, rows), F32),
            vmem((n_tp, 2, rows), F32),
            vmem((nx, 2, each, 2 * width), BF16),
            vmem((OUT_CUTS, nx, each, cut), BF16),
            vmem((OUT_CUTS, nx, each, cut), BF16),
            vmem((OUT_CUTS, nx, each, cut), BF16),
            vmem((OUT_CUTS, nx - 1, each, cut), BF16),
            dma((12,)),
            dma((14,)),
            dma((n_tp, 2)),
            dma((2, 2, CHUNKS)),
            dma((n, CHUNKS)),
            dma((2, 2)),
            dma((n,)),
            dma((2,)),
            pltpu.SemaphoreType.REGULAR,
            dma((n_tp,)),
            dma((n_tp,)),
            dma((OUT_CUTS,)),
            dma((OUT_CUTS,)),
            dma((OUT_CUTS, nx - 1)),
            dma((OUT_CUTS, nx - 1)),
        ]
        return pl.pallas_call(
            functools.partial(layer, n, n_tp),
            out_shape=(
                jax.ShapeDtypeStruct((each, full), BF16),
                jax.ShapeDtypeStruct((heads, rows), F32),
            ),
            in_specs=[pl.BlockSpec(memory_space=pl.ANY)] * 12,
            out_specs=(pl.BlockSpec(memory_space=pltpu.VMEM), pl.BlockSpec(memory_space=pltpu.VMEM)),
            scratch_shapes=scratch,
            compiler_params=pltpu.CompilerParams(collective_id=0, has_side_effects=True),
        )(
            inputs,
            norm_gain.reshape(full // 128, 128),
            w_conv_in,
            w_conv_gate,
            conv_kernel,
            ln_gain.reshape(1, width),
            w_query,
            w_key,
            w_value,
            cum_gate,
            w_conv_out,
            w_attn_out,
        )

    in_specs = (
        P(("grp", "sp"), "tp"),
        P(),
        P("tp", None),
        P("tp", None),
        P(None, "tp"),
        P("tp"),
        P("tp", None),
        P("tp", None),
        P("tp", None),
        P("tp", ("grp", "sp")),
        P("tp", None),
        P("tp", None),
    )
    out_specs = (P(("grp", "sp", "tp"), None), P("tp", ("grp", "sp")))
    return jax.shard_map(local, mesh=mesh, in_specs=in_specs, out_specs=out_specs, check_vma=False)
```

```python
import functools

import jax
import jax.numpy as jnp
from jax import lax
from jax.experimental import pallas as pl
from jax.experimental.pallas import tpu as pltpu
from jax.sharding import PartitionSpec as P

MESH = pl.DeviceIdType.MESH
F32 = jnp.float32
BF16 = jnp.bfloat16
CHUNKS = 4
OUT_CUTS = 2
NT = (((1,), (1,)), ((), ()))
NN = (((1,), (0,)), ((), ()))


def dot(a, b, dims):
    return lax.dot_general(a, b, dims, preferred_element_type=F32)


def layer(
    n,
    n_tp,
    x_hbm,
    gain_hbm,
    wci_hbm,
    wcg_hbm,
    taps_hbm,
    lng_hbm,
    wq_hbm,
    wk_hbm,
    wv_hbm,
    cum_hbm,
    wco_hbm,
    wao_hbm,
    mixed_hbm,
    log_hbm,
    mixed_ref,
    log_ref,
    out_sem,
    xg,
    xs,
    gain,
    gain32,
    taps,
    lng,
    wkv,
    w3,
    wo,
    kv,
    cum,
    kvacc,
    sq,
    qs,
    m_ref,
    l_ref,
    acc,
    ext,
    glu_tail,
    halo,
    ctr,
    stats,
    comb,
    pair_out,
    pair_in,
    xout,
    xin,
    ld_sem,
    in_send,
    in_recv,
    kv_send,
    kv_recv,
    cum_send,
    cum_recv,
    halo_sem,
    far_ready,
    st_send,
    st_recv,
    pair_send,
    pair_recv,
    x_send,
    x_recv,
):
    z = lax.axis_index("sp")
    t = lax.axis_index("tp")
    rows, feat = x_hbm.shape
    width = wk_hbm.shape[0]
    heads = cum_hbm.shape[0]
    hd = width // heads
    n_taps = taps_hbm.shape[0]
    half_n = n // 2
    nx = n_tp // 2
    x = t // 2
    c = t % 2

    def at(dx, core):
        return 2 * ((x + dx + nx) % nx) + core

    right, left, far, mate = at(1, c), at(-1, c), at(2, c), at(0, 1 - c)
    up, down = (z + 1) % n, (z + n - 1) % n

    def rdma(src, dst, send, recv, **device):
        return pltpu.make_async_remote_copy(
            src_ref=src, dst_ref=dst, send_sem=send, recv_sem=recv, device_id=device, device_id_type=MESH
        )

    loads = [
        (x_hbm, xg.at[t]),
        (wk_hbm, wkv.at[pl.ds(0, width)]),
        (wv_hbm, wkv.at[pl.ds(width, width)]),
        (gain_hbm, gain),
        (cum_hbm, cum.at[z]),
        (wci_hbm, w3.at[pl.ds(0, width)]),
        (wcg_hbm, w3.at[pl.ds(width, width)]),
        (wq_hbm, w3.at[pl.ds(2 * width, width)]),
        (taps_hbm, taps),
        (lng_hbm, lng),
        (wco_hbm, wo.at[pl.ds(0, width)]),
        (wao_hbm, wo.at[pl.ds(width, width)]),
    ]
    loads = [pltpu.make_async_copy(a, b, ld_sem.at[i]) for i, (a, b) in enumerate(loads)]
    for copy in loads:
        copy.start()

    barrier = pltpu.get_barrier_semaphore()
    for k in range(1, n_tp):
        pl.semaphore_signal(barrier, inc=1, device_id={"tp": (t + k) % n_tp}, device_id_type=MESH)
    last = n - 1
    n_low = last - half_n

    def lowest(p):
        return jnp.where(
            p <= half_n + 2,
            0,
            jnp.where(p <= half_n + 3, 1, p - half_n - jnp.where(p <= half_n + 8, 1, 0)),
        )

    low, low_up, low_down = lowest(z), lowest(z + 1), lowest(z - 1)
    express = n // 4 + 1
    first_tells = 4
    is_low = z < n_low
    relays_down = low_down > 0

    @pl.when(z > 0)
    def _():
        pl.semaphore_signal(barrier, inc=1, device_id={"sp": down}, device_id_type=MESH)

    @pl.when((low > 0) & (z < last))
    def _():
        pl.semaphore_signal(barrier, inc=1, device_id={"sp": up}, device_id_type=MESH)

    @pl.when(z == express)
    def _():
        pl.semaphore_signal(barrier, inc=1, device_id={"sp": 0}, device_id_type=MESH)

    @pl.when(is_low)
    def _():
        pl.semaphore_signal(barrier, inc=1, device_id={"sp": last}, device_id_type=MESH)

    pl.semaphore_wait(
        barrier,
        n_tp
        - 1
        + jnp.where(z < last, 1, 0)
        + jnp.where(relays_down, 1, 0)
        + jnp.where(z == 0, 1, 0)
        + jnp.where(z == last, n_low, 0),
    )

    def tell(j):
        pl.semaphore_signal(far_ready, inc=1, device_id={"sp": j}, device_id_type=MESH)

    @pl.when(z == last)
    def _():
        for j in range(min(first_tells, n_low)):
            tell(j)

    quarter = rows // 4
    pending = []

    def part(slot, h, m=1):
        return xg.at[slot, pl.ds(h * quarter, m * quarter)]

    def send_in(slot, h, to, m=1):
        k = len(pending)
        copy = rdma(part(slot, h, m), part(slot, h, m), in_send.at[k], in_recv.at[slot, h], tp=to)
        copy.start()
        pending.append(copy)

    def got(slot, h, m=1):
        rdma(part(slot, h, m), part(slot, h, m), in_send.at[0], in_recv.at[slot, h], tp=mate).wait_recv()

    loads[0].wait()
    for h in range(4):
        send_in(t, h, right)
        send_in(t, (h + 2) % 4, left)
    send_in(t, 0, mate, 4)
    for copy in loads[1:4]:
        copy.wait()
    gain32[...] = gain[...].astype(F32)
    kvacc[...] = jnp.zeros_like(kvacc)
    sq[...] = jnp.zeros_like(sq)

    def process(slot):
        xf = xg[slot].astype(F32)
        lanes = pl.ds(pl.multiple_of(slot * feat, feat), feat)
        s2 = xf * xf
        sq[...] += s2[:, :128] + s2[:, 128:]
        scale = [gain32[pl.ds(slot * (feat // 128) + i, 1)] for i in range(feat // 128)]
        sc = (xf * jnp.concatenate(scale, axis=1)).astype(BF16)
        xs[slot] = sc
        kvacc[...] += dot(sc, wkv[:, lanes], NT)

    process(t)
    got(mate, 0, 4)
    process(mate)
    for h in range(2):
        got(left, h)
        send_in(left, h, right)
        got(right, 2 + h)
        send_in(right, 2 + h, left)
    send_in(left, 0, mate, 2)
    send_in(right, 2, mate, 2)
    for h in range(2):
        got(left, 2 + h)
        got(right, h)
    send_in(left, 2, mate, 2)
    send_in(right, 0, mate, 2)
    process(left)
    process(right)
    for slot in (at(-1, 1 - c), at(1, 1 - c)):
        got(slot, 0, 2)
        got(slot, 2, 2)
        process(slot)
    for h in (0, 2, 1, 3):
        got(far, h)
        send_in(far, h, mate)
    process(far)
    for h in (0, 2, 1, 3):
        got(at(2, 1 - c), h)
    process(at(2, 1 - c))

    rms = lax.rsqrt(jnp.sum(sq[...], axis=1, keepdims=True) / (feat * n_tp) + 1e-06)
    kv[z] = (kvacc[...] * rms).astype(BF16)
    loads[4].wait()

    chunk = rows // CHUNKS

    def kv_copy(way, blk, q, k, to):
        ref = kv.at[blk, pl.ds(q * chunk, chunk)]
        return rdma(ref, ref, kv_send.at[way, k % 2, q], kv_recv.at[blk, q], sp=to)

    def cum_copy(way, blk, k, to):
        return rdma(cum.at[blk], cum.at[blk], cum_send.at[way, k % 2], cum_recv.at[blk], sp=to)

    first_up = z < last

    @pl.when(z == last)
    def _():
        for j in range(first_tells, min(first_tells + 2, n_low)):
            tell(j)

    @pl.when(first_up)
    def _():
        cum_copy(0, z, 0, up).start()
        for q in range(CHUNKS):
            kv_copy(0, z, q, 0, up).start()

    for copy in loads[5:8]:
        copy.wait()
    r3 = dot(xs[0], w3[:, :feat], NT)
    for p in range(1, n_tp):
        r3 += dot(xs[p], w3[:, p * feat : (p + 1) * feat], NT)
    r3 = r3 * rms
    glu = (r3[:, :width] * jax.nn.sigmoid(r3[:, width : 2 * width])).astype(BF16)
    pad = glu_tail.shape[0]
    glu_tail[...] = glu[rows - pad :]
    ext[pl.ds(pad, rows)] = glu.astype(F32)
    ext[pl.ds(pad + rows, 8)] = jnp.zeros((8, width), F32)
    query = (r3[:, 2 * width :]).astype(BF16) * jnp.asarray(hd ** (-0.5), BF16)
    lane = lax.broadcasted_iota(jnp.int32, (rows, width), 1)
    for h in range(heads):
        mine = (lane >= h * hd) & (lane < (h + 1) * hd)
        qs[pl.ds(h * rows, rows)] = jnp.where(mine, query.astype(F32), 0.0).astype(BF16)
    halo_copy = rdma(glu_tail, halo, halo_sem.at[0], halo_sem.at[1], sp=up)

    @pl.when(first_up)
    def _():
        halo_copy.start()

    ones = jnp.ones((rows, width), BF16)

    def attend(h, blocks, diagonal=False):
        here = pl.ds(h * rows, rows)
        q = qs[here]
        scores = []
        for blk in blocks:
            s = dot(q, kv[blk, :, :width], NT)
            s = s + (cum[z, h : h + 1, 0:1] - cum[blk, h : h + 1, :])
            if diagonal:
                q_pos = lax.broadcasted_iota(jnp.int32, s.shape, 0)
                k_pos = lax.broadcasted_iota(jnp.int32, s.shape, 1)
                s = jnp.where(k_pos <= q_pos, s, -1e30)
            scores.append(s)
        best = scores[0]
        for s in scores[1:]:
            best = jnp.maximum(best, s)
        m_new = jnp.broadcast_to(jnp.max(best, axis=1, keepdims=True), (rows, width))
        if not diagonal:
            m_old = m_ref[here]
            m_new = jnp.maximum(m_old, m_new)
        m_ref[here] = m_new
        wide = jnp.concatenate([m_new] * (rows // width), axis=1)
        out = None
        for blk, s in zip(blocks, scores):
            p = jnp.exp(s - wide).astype(BF16)
            o = dot(p, jnp.concatenate([kv[blk, :, width:], ones], axis=1), NN)
            out = o if out is None else out + o
        if diagonal:
            acc[here] = out[:, :width]
            l_ref[here] = out[:, width:]
        else:
            fade = jnp.exp(m_old - m_new)
            acc[here] = acc[here] * fade + out[:, :width]
            l_ref[here] = l_ref[here] * fade + out[:, width:]

    for h in range(heads):
        attend(h, [z], diagonal=True)

    def convolve():
        loads[8].wait()

        @pl.when(z > 0)
        def _():
            halo_copy.wait_recv()
            ext[pl.ds(0, pad)] = halo[...].astype(F32)

        @pl.when(z == 0)
        def _():
            ext[pl.ds(0, pad)] = jnp.zeros((pad, width), F32)

        weight = taps[...].astype(F32)
        shift = pad - (n_taps - 1)
        long = rows + 8
        total = jnp.zeros((rows, width), F32)
        for r in range(8):
            sub = None
            for j in range(n_taps):
                if (shift + j) % 8 == r:
                    base = shift + j - r
                    if r == 0:
                        term = ext[pl.ds(base, rows)] * weight[j : j + 1]
                    else:
                        term = ext[pl.ds(base, long)] * weight[j : j + 1]
                    sub = term if sub is None else sub + term
            if r == 0:
                total = total + sub
            else:
                total = total + pltpu.roll(sub, long - r, 0)[:rows]
        turned = total.T
        ctr[...] = turned
        stats[t, 0:1] = jnp.sum(turned, axis=0, keepdims=True)
        stats[t, 1:2] = jnp.sum(turned * turned, axis=0, keepdims=True)

    def stat_copy(k):
        return rdma(stats.at[t], stats.at[t], st_send.at[k], st_recv.at[t], tp=(t + k) % n_tp)

    def send_stats():
        for k in range(1, n_tp):
            stat_copy(k).start()

    def finish_conv():
        for k in range(1, n_tp):
            src = (t + k) % n_tp
            rdma(stats.at[src], stats.at[src], st_send.at[0], st_recv.at[src], tp=src).wait_recv()
        loads[9].wait()
        tot = stats[0]
        for p in range(1, n_tp):
            tot = tot + stats[p]
        mean = tot[0:1] / (width * n_tp)
        var = tot[1:2] / (width * n_tp) - mean * mean
        y = ((ctr[...] - mean) * lax.rsqrt(var + 1e-05)).T
        y = y * lng[...].astype(F32)
        y = (y * jax.nn.sigmoid(y)).astype(BF16)
        each = rows // n_tp
        for d in range(n_tp):
            comb[d // 2, d % 2, :, :width] = y[d * each : (d + 1) * each]

    conv_at = 2
    stats_at = min(5, half_n + 1)

    lag = jnp.where(low > 0, (last - z) // 3, 0)

    def flow_up(s):
        blk = z - s
        comes = (s >= 1) & (blk >= low)
        goes = comes & (z < last) & (blk >= low_up) & jnp.logical_not((blk == 0) & (z == express - 1))
        return comes, goes

    def flow_down(d):
        blk = z + d - n
        comes = (d >= 1) & (blk >= 0) & (blk < low)
        goes = comes & (blk < low_down)
        return comes, goes

    def send_far():
        @pl.when(z == 0)
        def _():
            cum_copy(1, z, 1, express).start()
            for q in range(CHUNKS):
                kv_copy(1, z, q, 1, express).start()

        pl.semaphore_wait(far_ready, 1)
        cum_copy(1, z, 0, last).start()
        for q in range(CHUNKS):
            kv_copy(1, z, q, 0, last).start()

    def step(s, carry):
        d = s - lag
        cw_in, cw_on = flow_up(s)
        cc_in, cc_on = flow_down(d)
        j_cw, j_cc = (z + n - s) % n, (z + n + d) % n
        b_cw, b_cc = (z + n - s + 1) % n, (z + n + d - 1) % n
        has_cw, _ = flow_up(s - 1)
        has_cc, _ = flow_down(d - 1)
        two = has_cw & has_cc
        one = has_cw ^ has_cc
        every = CHUNKS // heads

        @pl.when(is_low & (z < express) & (s == jnp.maximum(z, 1)))
        def _():
            send_far()

        for q in range(CHUNKS):
            for way, arrives, goes, blk, to, k, again in (
                (1, cc_in, cc_on, j_cc, down, d, d - 2 >= n - z),
                (0, cw_in, cw_on, j_cw, up, s, s >= 2),
            ):

                @pl.when(arrives)
                def _(way=way, blk=blk, to=to):
                    if q == 0:
                        cum_copy(way, blk, 0, to).wait_recv()
                    kv_copy(way, blk, q, 0, to).wait_recv()

                @pl.when(goes & again)
                def _(way=way, blk=blk, to=to, k=k):
                    if q == 0:
                        cum_copy(way, blk, k, to).wait_send()
                    kv_copy(way, blk, q, k, to).wait_send()

                @pl.when(goes)
                def _(way=way, blk=blk, to=to, k=k):
                    if q == 0:
                        cum_copy(way, blk, k, to).start()
                    kv_copy(way, blk, q, k, to).start()

            if q % every == every - 1:

                @pl.when(two)
                def _():
                    attend(q // every, [b_cw, b_cc])

                @pl.when(one)
                def _():
                    attend(q // every, [jnp.where(has_cw, b_cw, b_cc)])

        @pl.when((z == last) & (s <= n_low))
        def _():
            first = first_tells + 2 + s + s // 2
            for j, really in ((first - 1, s % 2 < 2), (first, s % 2 == 1)):

                @pl.when(really & (j < n_low))
                def _(j=j):
                    tell(j)

        @pl.when(s == conv_at)
        def _():
            convolve()
            send_stats()

        @pl.when(s == stats_at)
        def _():
            finish_conv()

        return carry

    steps = jnp.maximum(
        jnp.maximum(z - low + 1, stats_at), jnp.where(low > 0, n - z + low + lag, 0)
    )
    lax.fori_loop(1, steps + 1, step, 0)

    tops, sums = m_ref[...], l_ref[...]
    logs = tops + jnp.log(sums)
    attn = acc[...] / sums
    log_row = logs[:rows]
    attn_row = attn[:rows]
    for h in range(1, heads):
        attn_row = jnp.where(lane >= h * hd, attn[h * rows : (h + 1) * rows], attn_row)
        log_row = jnp.where(lane >= h, logs[h * rows : (h + 1) * rows], log_row)
    each = rows // n_tp
    attn_row = attn_row.astype(BF16)
    for d in range(n_tp):
        comb[d // 2, d % 2, :, width:] = attn_row[d * each : (d + 1) * each]

    for copy in loads[10:12]:
        copy.wait()
    cut = wo.shape[1] // OUT_CUTS

    def product(core, i):
        lhs = comb[:, core].reshape(nx * each, 2 * width)
        return dot(lhs, wo[:, i * cut : (i + 1) * cut], NN).reshape(nx, each, cut)

    pairs = []
    for i in range(OUT_CUTS):
        pair_out[i] = product(1 - c, i).astype(BF16)
        copy = rdma(pair_out.at[i], pair_in.at[i], pair_send.at[i], pair_recv.at[i], tp=mate)
        copy.start()
        pairs.append(copy)
    outs = []
    for i in range(OUT_CUTS):
        own = product(c, i)
        pairs[i].wait_recv()
        xout[i] = (own + pair_in[i].astype(F32)).astype(BF16)
        for dx in (2, 1, 3):
            dst = at(dx - nx, c)
            copy = rdma(
                xout.at[i, (x + dx) % nx], xin.at[i, dx - 1], x_send.at[i, dx - 1], x_recv.at[i, dx - 1], tp=dst
            )
            copy.start()
            outs.append((i, copy))
    @pl.when(is_low & (z >= express))
    def _():
        send_far()

    log_ref[...] = log_row.T[:heads] + (cum[z] - cum[z][:, 0:1])
    results = [pltpu.make_async_copy(log_ref, log_hbm, out_sem.at[OUT_CUTS])]
    results[0].start()
    for i in range(OUT_CUTS):
        total = xout[i, x].astype(F32)
        for k, copy in outs:
            if k == i:
                copy.wait_recv()
        for dx in range(nx - 1):
            total = total + xin[i, dx].astype(F32)
        columns = pl.ds(i * cut, cut)
        mixed_ref[:, columns] = total.astype(BF16)
        results.append(pltpu.make_async_copy(mixed_ref.at[:, columns], mixed_hbm.at[:, columns], out_sem.at[i]))
        results[-1].start()

    for copy in pending:
        copy.wait_send()
    ups = z - low_up - jnp.where(z == express - 1, 1, 0) + 1
    downs = low_down
    for way, parity, cond in (
        (0, 0, first_up),
        (0, 1, first_up & (ups > 1)),
        (1, 0, is_low | (downs > 1) | ((downs == 1) & ((n - z) % 2 == 0))),
        (1, 1, (z == 0) | (downs > 1) | ((downs == 1) & ((n - z) % 2 == 1))),
    ):

        @pl.when(cond)
        def _(way=way, parity=parity):
            cum_copy(way, z, parity, up).wait_send()
            for q in range(CHUNKS):
                kv_copy(way, z, q, parity, up).wait_send()

    @pl.when(first_up)
    def _():
        halo_copy.wait_send()

    for k in range(1, n_tp):
        stat_copy(k).wait_send()

    for copy in pairs:
        copy.wait_send()
    for k, copy in outs:
        copy.wait_send()
    for copy in results:
        copy.wait()


def solution(mesh):
    n, n_tp = mesh.shape["sp"], mesh.shape["tp"]

    def local(
        inputs,
        norm_gain,
        w_conv_in,
        w_conv_gate,
        conv_kernel,
        ln_gain,
        w_query,
        w_key,
        w_value,
        cum_gate,
        w_conv_out,
        w_attn_out,
    ):
        rows, feat = inputs.shape
        width, full = w_key.shape
        heads = cum_gate.shape[0]
        n_taps = conv_kernel.shape[0]
        each = rows // n_tp
        nx = n_tp // 2
        pad = 32
        cut = full // OUT_CUTS
        half_n = n // 2
        dma = pltpu.SemaphoreType.DMA
        vmem = pltpu.VMEM
        scratch = [
            vmem((each, full), BF16),
            vmem((heads, rows), F32),
            dma((OUT_CUTS + 1,)),
            vmem((n_tp, rows, feat), BF16),
            vmem((n_tp, rows, feat), BF16),
            vmem((full // 128, 128), BF16),
            vmem((full // 128, 128), F32),
            vmem((n_taps, width), BF16),
            vmem((1, width), BF16),
            vmem((2 * width, full), BF16),
            vmem((3 * width, full), BF16),
            vmem((2 * width, full), BF16),
            vmem((n, rows, 2 * width), BF16),
            vmem((n, heads, rows), F32),
            vmem((rows, 2 * width), F32),
            vmem((rows, 128), F32),
            vmem((heads * rows, width), BF16),
            vmem((heads * rows, width), F32),
            vmem((heads * rows, width), F32),
            vmem((heads * rows, width), F32),
            vmem((pad + rows + 8, width), F32),
            vmem((pad, width), BF16),
            vmem((pad, width), BF16),
            vmem((width, rows), F32),
            vmem((n_tp, 2, rows), F32),
            vmem((nx, 2, each, 2 * width), BF16),
            vmem((OUT_CUTS, nx, each, cut), BF16),
            vmem((OUT_CUTS, nx, each, cut), BF16),
            vmem((OUT_CUTS, nx, each, cut), BF16),
            vmem((OUT_CUTS, nx - 1, each, cut), BF16),
            dma((12,)),
            dma((21,)),
            dma((n_tp, 4)),
            dma((2, 2, CHUNKS)),
            dma((n, CHUNKS)),
            dma((2, 2)),
            dma((n,)),
            dma((2,)),
            pltpu.SemaphoreType.REGULAR,
            dma((n_tp,)),
            dma((n_tp,)),
            dma((OUT_CUTS,)),
            dma((OUT_CUTS,)),
            dma((OUT_CUTS, nx - 1)),
            dma((OUT_CUTS, nx - 1)),
        ]
        return pl.pallas_call(
            functools.partial(layer, n, n_tp),
            out_shape=(
                jax.ShapeDtypeStruct((each, full), BF16),
                jax.ShapeDtypeStruct((heads, rows), F32),
            ),
            in_specs=[pl.BlockSpec(memory_space=pl.ANY)] * 12,
            out_specs=(pl.BlockSpec(memory_space=pl.ANY), pl.BlockSpec(memory_space=pl.ANY)),
            scratch_shapes=scratch,
            compiler_params=pltpu.CompilerParams(collective_id=0, has_side_effects=True),
        )(
            inputs,
            norm_gain.reshape(full // 128, 128),
            w_conv_in,
            w_conv_gate,
            conv_kernel,
            ln_gain.reshape(1, width),
            w_query,
            w_key,
            w_value,
            cum_gate,
            w_conv_out,
            w_attn_out,
        )

    in_specs = (
        P(("grp", "sp"), "tp"),
        P(),
        P("tp", None),
        P("tp", None),
        P(None, "tp"),
        P("tp"),
        P("tp", None),
        P("tp", None),
        P("tp", None),
        P("tp", ("grp", "sp")),
        P("tp", None),
        P("tp", None),
    )
    out_specs = (P(("grp", "sp", "tp"), None), P("tp", ("grp", "sp")))
    return jax.shard_map(local, mesh=mesh, in_specs=in_specs, out_specs=out_specs, check_vma=False)
```

```python
import functools

import jax
import jax.numpy as jnp
from jax import lax
from jax.experimental import pallas as pl
from jax.experimental.pallas import tpu as pltpu
from jax.sharding import PartitionSpec as P

MESH = pl.DeviceIdType.MESH
F32 = jnp.float32
BF16 = jnp.bfloat16
CHUNKS = 4
OUT_CUTS = 2
NT = (((1,), (1,)), ((), ()))
NN = (((1,), (0,)), ((), ()))


def dot(a, b, dims):
    return lax.dot_general(a, b, dims, preferred_element_type=F32)


def layer(
    n,
    n_tp,
    x_hbm,
    gain_hbm,
    wci_hbm,
    wcg_hbm,
    taps_hbm,
    lng_hbm,
    wq_hbm,
    wk_hbm,
    wv_hbm,
    cum_hbm,
    wco_hbm,
    wao_hbm,
    mixed_hbm,
    log_hbm,
    mixed_ref,
    log_ref,
    out_sem,
    xg,
    xs,
    gain,
    gain32,
    taps,
    lng,
    wkv,
    w3,
    wo,
    kv,
    cum,
    kvacc,
    sq,
    qs,
    m_ref,
    l_ref,
    acc,
    ext,
    glu_tail,
    halo,
    ctr,
    stats,
    comb,
    pair_out,
    pair_in,
    xout,
    xin,
    ld_sem,
    in_send,
    in_recv,
    kv_send,
    kv_recv,
    cum_send,
    cum_recv,
    halo_sem,
    far_ready,
    st_send,
    st_recv,
    pair_send,
    pair_recv,
    x_send,
    x_recv,
):
    z = lax.axis_index("sp")
    t = lax.axis_index("tp")
    rows, feat = x_hbm.shape
    width = wk_hbm.shape[0]
    heads = cum_hbm.shape[0]
    hd = width // heads
    n_taps = taps_hbm.shape[0]
    half_n = n // 2
    nx = n_tp // 2
    x = t // 2
    c = t % 2

    def at(dx, core):
        return 2 * ((x + dx + nx) % nx) + core

    right, left, far, mate = at(1, c), at(-1, c), at(2, c), at(0, 1 - c)
    up, down = (z + 1) % n, (z + n - 1) % n

    def rdma(src, dst, send, recv, **device):
        return pltpu.make_async_remote_copy(
            src_ref=src, dst_ref=dst, send_sem=send, recv_sem=recv, device_id=device, device_id_type=MESH
        )

    loads = [
        (x_hbm, xg.at[t]),
        (wk_hbm, wkv.at[pl.ds(0, width)]),
        (wv_hbm, wkv.at[pl.ds(width, width)]),
        (gain_hbm, gain),
        (cum_hbm, cum.at[z]),
        (wci_hbm, w3.at[pl.ds(0, width)]),
        (wcg_hbm, w3.at[pl.ds(width, width)]),
        (wq_hbm, w3.at[pl.ds(2 * width, width)]),
        (taps_hbm, taps),
        (lng_hbm, lng),
        (wco_hbm, wo.at[pl.ds(0, width)]),
        (wao_hbm, wo.at[pl.ds(width, width)]),
    ]
    loads = [pltpu.make_async_copy(a, b, ld_sem.at[i]) for i, (a, b) in enumerate(loads)]
    for copy in loads:
        copy.start()

    barrier = pltpu.get_barrier_semaphore()
    for k in range(1, n_tp):
        pl.semaphore_signal(barrier, inc=1, device_id={"tp": (t + k) % n_tp}, device_id_type=MESH)
    last = n - 1
    n_low = last - half_n

    def lowest(p):
        over = jnp.where(p <= half_n + 5, 2, jnp.where(p <= half_n + 11, 1, 0))
        return jnp.maximum(p - half_n - over, 0)

    low, low_up, low_down = lowest(z), lowest(z + 1), lowest(z - 1)
    express = n // 4 + 1
    first_tells = 3
    is_low = z < n_low
    relays_down = low_down > 0

    @pl.when(z > 0)
    def _():
        pl.semaphore_signal(barrier, inc=1, device_id={"sp": down}, device_id_type=MESH)

    @pl.when((low > 0) & (z < last))
    def _():
        pl.semaphore_signal(barrier, inc=1, device_id={"sp": up}, device_id_type=MESH)

    @pl.when(z == express)
    def _():
        pl.semaphore_signal(barrier, inc=1, device_id={"sp": 0}, device_id_type=MESH)

    @pl.when(is_low)
    def _():
        pl.semaphore_signal(barrier, inc=1, device_id={"sp": last}, device_id_type=MESH)

    pl.semaphore_wait(
        barrier,
        n_tp
        - 1
        + jnp.where(z < last, 1, 0)
        + jnp.where(relays_down, 1, 0)
        + jnp.where(z == 0, 1, 0)
        + jnp.where(z == last, n_low, 0),
    )

    def tell(j):
        pl.semaphore_signal(far_ready, inc=1, device_id={"sp": j}, device_id_type=MESH)

    @pl.when(z == last)
    def _():
        for j in range(min(first_tells, n_low)):
            tell(j)

    quarter = rows // 4
    pending = []

    def part(slot, h, m=1):
        return xg.at[slot, pl.ds(h * quarter, m * quarter)]

    def send_in(slot, h, to, m=1):
        k = len(pending)
        copy = rdma(part(slot, h, m), part(slot, h, m), in_send.at[k], in_recv.at[slot, h], tp=to)
        copy.start()
        pending.append(copy)

    def got(slot, h, m=1):
        rdma(part(slot, h, m), part(slot, h, m), in_send.at[0], in_recv.at[slot, h], tp=mate).wait_recv()

    loads[0].wait()
    for h in range(4):
        send_in(t, h, right)
        send_in(t, (h + 2) % 4, left)
    send_in(t, 0, mate, 4)
    for copy in loads[1:4]:
        copy.wait()
    gain32[...] = gain[...].astype(F32)
    kvacc[...] = jnp.zeros_like(kvacc)
    sq[...] = jnp.zeros_like(sq)

    def process(slot):
        xf = xg[slot].astype(F32)
        lanes = pl.ds(pl.multiple_of(slot * feat, feat), feat)
        s2 = xf * xf
        sq[...] += s2[:, :128] + s2[:, 128:]
        scale = [gain32[pl.ds(slot * (feat // 128) + i, 1)] for i in range(feat // 128)]
        sc = (xf * jnp.concatenate(scale, axis=1)).astype(BF16)
        xs[slot] = sc
        kvacc[...] += dot(sc, wkv[:, lanes], NT)

    process(t)
    got(mate, 0, 4)
    process(mate)
    for h in range(2):
        got(left, h)
        send_in(left, h, right)
        got(right, 2 + h)
        send_in(right, 2 + h, left)
    send_in(left, 0, mate, 2)
    send_in(right, 2, mate, 2)
    for h in range(2):
        got(left, 2 + h)
        got(right, h)
    send_in(left, 2, mate, 2)
    send_in(right, 0, mate, 2)
    process(left)
    process(right)
    for slot in (at(-1, 1 - c), at(1, 1 - c)):
        got(slot, 0, 2)
        got(slot, 2, 2)
        process(slot)
    for h in (0, 2, 1, 3):
        got(far, h)
        send_in(far, h, mate)
    process(far)
    for h in (0, 2, 1, 3):
        got(at(2, 1 - c), h)
    process(at(2, 1 - c))

    rms = lax.rsqrt(jnp.sum(sq[...], axis=1, keepdims=True) / (feat * n_tp) + 1e-06)
    kv[z] = (kvacc[...] * rms).astype(BF16)
    loads[4].wait()

    chunk = rows // CHUNKS

    def kv_copy(way, blk, q, k, to):
        ref = kv.at[blk, pl.ds(q * chunk, chunk)]
        return rdma(ref, ref, kv_send.at[way, k % 2, q], kv_recv.at[blk, q], sp=to)

    def cum_copy(way, blk, k, to):
        return rdma(cum.at[blk], cum.at[blk], cum_send.at[way, k % 2], cum_recv.at[blk], sp=to)

    first_up = z < last

    @pl.when(z == last)
    def _():
        for j in range(first_tells, min(first_tells + 3, n_low)):
            tell(j)

    @pl.when(first_up)
    def _():
        cum_copy(0, z, 0, up).start()
        for q in range(CHUNKS):
            kv_copy(0, z, q, 0, up).start()

    for copy in loads[5:8]:
        copy.wait()
    r3 = dot(xs[0], w3[:, :feat], NT)
    for p in range(1, n_tp):
        r3 += dot(xs[p], w3[:, p * feat : (p + 1) * feat], NT)
    r3 = r3 * rms
    glu = (r3[:, :width] * jax.nn.sigmoid(r3[:, width : 2 * width])).astype(BF16)
    pad = glu_tail.shape[0]
    glu_tail[...] = glu[rows - pad :]
    ext[pl.ds(pad, rows)] = glu.astype(F32)
    ext[pl.ds(pad + rows, 8)] = jnp.zeros((8, width), F32)
    query = (r3[:, 2 * width :]).astype(BF16) * jnp.asarray(hd ** (-0.5), BF16)
    lane = lax.broadcasted_iota(jnp.int32, (rows, width), 1)
    for h in range(heads):
        mine = (lane >= h * hd) & (lane < (h + 1) * hd)
        qs[pl.ds(h * rows, rows)] = jnp.where(mine, query.astype(F32), 0.0).astype(BF16)
    halo_copy = rdma(glu_tail, halo, halo_sem.at[0], halo_sem.at[1], sp=up)

    @pl.when(first_up)
    def _():
        halo_copy.start()

    ones = jnp.ones((rows, width), BF16)

    def attend(h, blocks, diagonal=False):
        here = pl.ds(h * rows, rows)
        q = qs[here]
        scores = []
        for blk in blocks:
            s = dot(q, kv[blk, :, :width], NT)
            s = s + (cum[z, h : h + 1, 0:1] - cum[blk, h : h + 1, :])
            if diagonal:
                q_pos = lax.broadcasted_iota(jnp.int32, s.shape, 0)
                k_pos = lax.broadcasted_iota(jnp.int32, s.shape, 1)
                s = jnp.where(k_pos <= q_pos, s, -1e30)
            scores.append(s)
        best = scores[0]
        for s in scores[1:]:
            best = jnp.maximum(best, s)
        m_new = jnp.broadcast_to(jnp.max(best, axis=1, keepdims=True), (rows, width))
        if not diagonal:
            m_old = m_ref[here]
            m_new = jnp.maximum(m_old, m_new)
        m_ref[here] = m_new
        wide = jnp.concatenate([m_new] * (rows // width), axis=1)
        out = None
        for blk, s in zip(blocks, scores):
            p = jnp.exp(s - wide).astype(BF16)
            o = dot(p, jnp.concatenate([kv[blk, :, width:], ones], axis=1), NN)
            out = o if out is None else out + o
        if diagonal:
            acc[here] = out[:, :width]
            l_ref[here] = out[:, width:]
        else:
            fade = jnp.exp(m_old - m_new)
            acc[here] = acc[here] * fade + out[:, :width]
            l_ref[here] = l_ref[here] * fade + out[:, width:]

    for h in range(heads):
        attend(h, [z], diagonal=True)

    def convolve():
        loads[8].wait()

        @pl.when(z > 0)
        def _():
            halo_copy.wait_recv()
            ext[pl.ds(0, pad)] = halo[...].astype(F32)

        @pl.when(z == 0)
        def _():
            ext[pl.ds(0, pad)] = jnp.zeros((pad, width), F32)

        weight = taps[...].astype(F32)
        shift = pad - (n_taps - 1)
        long = rows + 8
        total = jnp.zeros((rows, width), F32)
        for r in range(8):
            sub = None
            for j in range(n_taps):
                if (shift + j) % 8 == r:
                    base = shift + j - r
                    if r == 0:
                        term = ext[pl.ds(base, rows)] * weight[j : j + 1]
                    else:
                        term = ext[pl.ds(base, long)] * weight[j : j + 1]
                    sub = term if sub is None else sub + term
            if r == 0:
                total = total + sub
            else:
                total = total + pltpu.roll(sub, long - r, 0)[:rows]
        turned = total.T
        ctr[...] = turned
        stats[t, 0:1] = jnp.sum(turned, axis=0, keepdims=True)
        stats[t, 1:2] = jnp.sum(turned * turned, axis=0, keepdims=True)

    def stat_copy(k):
        return rdma(stats.at[t], stats.at[t], st_send.at[k], st_recv.at[t], tp=(t + k) % n_tp)

    def send_stats():
        for k in range(1, n_tp):
            stat_copy(k).start()

    def finish_conv():
        for k in range(1, n_tp):
            src = (t + k) % n_tp
            rdma(stats.at[src], stats.at[src], st_send.at[0], st_recv.at[src], tp=src).wait_recv()
        loads[9].wait()
        tot = stats[0]
        for p in range(1, n_tp):
            tot = tot + stats[p]
        mean = tot[0:1] / (width * n_tp)
        var = tot[1:2] / (width * n_tp) - mean * mean
        y = ((ctr[...] - mean) * lax.rsqrt(var + 1e-05)).T
        y = y * lng[...].astype(F32)
        y = (y * jax.nn.sigmoid(y)).astype(BF16)
        each = rows // n_tp
        for d in range(n_tp):
            comb[d // 2, d % 2, :, :width] = y[d * each : (d + 1) * each]

    conv_at = 2
    stats_at = min(5, half_n + 1)

    lag = jnp.where(low > 0, 1 + (2 * (last - z) + 2) // 5, 0)

    def flow_up(s):
        blk = z - s
        comes = (s >= 1) & (blk >= low)
        goes = comes & (z < last) & (blk >= low_up) & jnp.logical_not((blk == 0) & (z == express - 1))
        return comes, goes

    def flow_down(d):
        blk = z + d - n
        comes = (d >= 1) & (blk >= 0) & (blk < low)
        goes = comes & (blk < low_down)
        return comes, goes

    def send_far():
        @pl.when(z == 0)
        def _():
            cum_copy(1, z, 1, express).start()
            for q in range(CHUNKS):
                kv_copy(1, z, q, 1, express).start()

        pl.semaphore_wait(far_ready, 1)
        cum_copy(1, z, 0, last).start()
        for q in range(CHUNKS):
            kv_copy(1, z, q, 0, last).start()

    def step(s, carry):
        d = s - lag
        cw_in, cw_on = flow_up(s)
        cc_in, cc_on = flow_down(d)
        j_cw, j_cc = (z + n - s) % n, (z + n + d) % n
        b_cw, b_cc = (z + n - s + 1) % n, (z + n + d - 1) % n
        has_cw, _ = flow_up(s - 1)
        has_cc, _ = flow_down(d - 1)
        two = has_cw & has_cc
        one = has_cw ^ has_cc
        every = CHUNKS // heads

        @pl.when(is_low & (z < express) & (s == jnp.maximum(z, 1)))
        def _():
            send_far()

        for q in range(CHUNKS):
            for way, arrives, goes, blk, to, k, again in (
                (1, cc_in, cc_on, j_cc, down, d, d - 2 >= n - z),
                (0, cw_in, cw_on, j_cw, up, s, s >= 2),
            ):

                @pl.when(arrives)
                def _(way=way, blk=blk, to=to):
                    if q == 0:
                        cum_copy(way, blk, 0, to).wait_recv()
                    kv_copy(way, blk, q, 0, to).wait_recv()

                @pl.when(goes & again)
                def _(way=way, blk=blk, to=to, k=k):
                    if q == 0:
                        cum_copy(way, blk, k, to).wait_send()
                    kv_copy(way, blk, q, k, to).wait_send()

                @pl.when(goes)
                def _(way=way, blk=blk, to=to, k=k):
                    if q == 0:
                        cum_copy(way, blk, k, to).start()
                    kv_copy(way, blk, q, k, to).start()

            if q % every == every - 1:

                @pl.when(two)
                def _():
                    attend(q // every, [b_cw, b_cc])

                @pl.when(one)
                def _():
                    attend(q // every, [jnp.where(has_cw, b_cw, b_cc)])

        @pl.when((z == last) & (s <= n_low))
        def _():
            first = first_tells + 3 + s + s // 2
            for j, really in ((first - 1, s % 2 < 2), (first, s % 2 == 1)):

                @pl.when(really & (j < n_low))
                def _(j=j):
                    tell(j)

        @pl.when(s == conv_at)
        def _():
            convolve()
            send_stats()

        @pl.when(s == stats_at)
        def _():
            finish_conv()

        return carry

    steps = jnp.maximum(
        jnp.maximum(z - low + 1, stats_at), jnp.where(low > 0, n - z + low + lag, 0)
    )
    lax.fori_loop(1, steps + 1, step, 0)

    tops, sums = m_ref[...], l_ref[...]
    logs = tops + jnp.log(sums)
    attn = acc[...] / sums
    log_row = logs[:rows]
    attn_row = attn[:rows]
    for h in range(1, heads):
        attn_row = jnp.where(lane >= h * hd, attn[h * rows : (h + 1) * rows], attn_row)
        log_row = jnp.where(lane >= h, logs[h * rows : (h + 1) * rows], log_row)
    each = rows // n_tp
    attn_row = attn_row.astype(BF16)
    for d in range(n_tp):
        comb[d // 2, d % 2, :, width:] = attn_row[d * each : (d + 1) * each]

    for copy in loads[10:12]:
        copy.wait()
    cut = wo.shape[1] // OUT_CUTS

    def product(core, i):
        lhs = comb[:, core].reshape(nx * each, 2 * width)
        return dot(lhs, wo[:, i * cut : (i + 1) * cut], NN).reshape(nx, each, cut)

    pairs = []
    for i in range(OUT_CUTS):
        pair_out[i] = product(1 - c, i).astype(BF16)
        copy = rdma(pair_out.at[i], pair_in.at[i], pair_send.at[i], pair_recv.at[i], tp=mate)
        copy.start()
        pairs.append(copy)
    outs = []
    for i in range(OUT_CUTS):
        own = product(c, i)
        pairs[i].wait_recv()
        xout[i] = (own + pair_in[i].astype(F32)).astype(BF16)
        for dx in (2, 1, 3):
            dst = at(dx - nx, c)
            copy = rdma(
                xout.at[i, (x + dx) % nx], xin.at[i, dx - 1], x_send.at[i, dx - 1], x_recv.at[i, dx - 1], tp=dst
            )
            copy.start()
            outs.append((i, copy))
    @pl.when(is_low & (z >= express))
    def _():
        send_far()

    log_ref[...] = log_row.T[:heads] + (cum[z] - cum[z][:, 0:1])
    results = [pltpu.make_async_copy(log_ref, log_hbm, out_sem.at[OUT_CUTS])]
    results[0].start()
    for i in range(OUT_CUTS):
        total = xout[i, x].astype(F32)
        for k, copy in outs:
            if k == i:
                copy.wait_recv()
        for dx in range(nx - 1):
            total = total + xin[i, dx].astype(F32)
        columns = pl.ds(i * cut, cut)
        mixed_ref[:, columns] = total.astype(BF16)
        results.append(pltpu.make_async_copy(mixed_ref.at[:, columns], mixed_hbm.at[:, columns], out_sem.at[i]))
        results[-1].start()

    for copy in pending:
        copy.wait_send()
    ups = z - low_up - jnp.where(z == express - 1, 1, 0) + 1
    downs = low_down
    for way, parity, cond in (
        (0, 0, first_up),
        (0, 1, first_up & (ups > 1)),
        (1, 0, is_low | (downs > 1) | ((downs == 1) & ((n - z) % 2 == 0))),
        (1, 1, (z == 0) | (downs > 1) | ((downs == 1) & ((n - z) % 2 == 1))),
    ):

        @pl.when(cond)
        def _(way=way, parity=parity):
            cum_copy(way, z, parity, up).wait_send()
            for q in range(CHUNKS):
                kv_copy(way, z, q, parity, up).wait_send()

    @pl.when(first_up)
    def _():
        halo_copy.wait_send()

    for k in range(1, n_tp):
        stat_copy(k).wait_send()

    for copy in pairs:
        copy.wait_send()
    for k, copy in outs:
        copy.wait_send()
    for copy in results:
        copy.wait()


def solution(mesh):
    n, n_tp = mesh.shape["sp"], mesh.shape["tp"]

    def local(
        inputs,
        norm_gain,
        w_conv_in,
        w_conv_gate,
        conv_kernel,
        ln_gain,
        w_query,
        w_key,
        w_value,
        cum_gate,
        w_conv_out,
        w_attn_out,
    ):
        rows, feat = inputs.shape
        width, full = w_key.shape
        heads = cum_gate.shape[0]
        n_taps = conv_kernel.shape[0]
        each = rows // n_tp
        nx = n_tp // 2
        pad = 32
        cut = full // OUT_CUTS
        half_n = n // 2
        dma = pltpu.SemaphoreType.DMA
        vmem = pltpu.VMEM
        scratch = [
            vmem((each, full), BF16),
            vmem((heads, rows), F32),
            dma((OUT_CUTS + 1,)),
            vmem((n_tp, rows, feat), BF16),
            vmem((n_tp, rows, feat), BF16),
            vmem((full // 128, 128), BF16),
            vmem((full // 128, 128), F32),
            vmem((n_taps, width), BF16),
            vmem((1, width), BF16),
            vmem((2 * width, full), BF16),
            vmem((3 * width, full), BF16),
            vmem((2 * width, full), BF16),
            vmem((n, rows, 2 * width), BF16),
            vmem((n, heads, rows), F32),
            vmem((rows, 2 * width), F32),
            vmem((rows, 128), F32),
            vmem((heads * rows, width), BF16),
            vmem((heads * rows, width), F32),
            vmem((heads * rows, width), F32),
            vmem((heads * rows, width), F32),
            vmem((pad + rows + 8, width), F32),
            vmem((pad, width), BF16),
            vmem((pad, width), BF16),
            vmem((width, rows), F32),
            vmem((n_tp, 2, rows), F32),
            vmem((nx, 2, each, 2 * width), BF16),
            vmem((OUT_CUTS, nx, each, cut), BF16),
            vmem((OUT_CUTS, nx, each, cut), BF16),
            vmem((OUT_CUTS, nx, each, cut), BF16),
            vmem((OUT_CUTS, nx - 1, each, cut), BF16),
            dma((12,)),
            dma((21,)),
            dma((n_tp, 4)),
            dma((2, 2, CHUNKS)),
            dma((n, CHUNKS)),
            dma((2, 2)),
            dma((n,)),
            dma((2,)),
            pltpu.SemaphoreType.REGULAR,
            dma((n_tp,)),
            dma((n_tp,)),
            dma((OUT_CUTS,)),
            dma((OUT_CUTS,)),
            dma((OUT_CUTS, nx - 1)),
            dma((OUT_CUTS, nx - 1)),
        ]
        return pl.pallas_call(
            functools.partial(layer, n, n_tp),
            out_shape=(
                jax.ShapeDtypeStruct((each, full), BF16),
                jax.ShapeDtypeStruct((heads, rows), F32),
            ),
            in_specs=[pl.BlockSpec(memory_space=pl.ANY)] * 12,
            out_specs=(pl.BlockSpec(memory_space=pl.ANY), pl.BlockSpec(memory_space=pl.ANY)),
            scratch_shapes=scratch,
            compiler_params=pltpu.CompilerParams(collective_id=0, has_side_effects=True),
        )(
            inputs,
            norm_gain.reshape(full // 128, 128),
            w_conv_in,
            w_conv_gate,
            conv_kernel,
            ln_gain.reshape(1, width),
            w_query,
            w_key,
            w_value,
            cum_gate,
            w_conv_out,
            w_attn_out,
        )

    in_specs = (
        P(("grp", "sp"), "tp"),
        P(),
        P("tp", None),
        P("tp", None),
        P(None, "tp"),
        P("tp"),
        P("tp", None),
        P("tp", None),
        P("tp", None),
        P("tp", ("grp", "sp")),
        P("tp", None),
        P("tp", None),
    )
    out_specs = (P(("grp", "sp", "tp"), None), P("tp", ("grp", "sp")))
    return jax.shard_map(local, mesh=mesh, in_specs=in_specs, out_specs=out_specs, check_vma=False)
```

```python
import functools

import jax
import jax.numpy as jnp
from jax import lax
from jax.experimental import pallas as pl
from jax.experimental.pallas import tpu as pltpu
from jax.sharding import PartitionSpec as P

MESH = pl.DeviceIdType.MESH
F32 = jnp.float32
BF16 = jnp.bfloat16
CHUNKS = 4
OUT_CUTS = 2
NT = (((1,), (1,)), ((), ()))
NN = (((1,), (0,)), ((), ()))


def dot(a, b, dims):
    return lax.dot_general(a, b, dims, preferred_element_type=F32)


def layer(
    n,
    n_tp,
    x_hbm,
    gain_hbm,
    wci_hbm,
    wcg_hbm,
    taps_hbm,
    lng_hbm,
    wq_hbm,
    wk_hbm,
    wv_hbm,
    cum_hbm,
    wco_hbm,
    wao_hbm,
    mixed_hbm,
    log_hbm,
    mixed_ref,
    log_ref,
    out_sem,
    xg,
    xs,
    gain,
    gain32,
    taps,
    lng,
    wkv,
    w3,
    wc_all,
    wa_all,
    kv,
    cum,
    kvacc,
    sq,
    qs,
    m_ref,
    l_ref,
    acc,
    ext,
    glu_tail,
    halo,
    ctr,
    stats,
    conv_src,
    conv_in,
    attn_src,
    attn_in,
    conv_part,
    ld_sem,
    in_send,
    in_recv,
    kv_send,
    kv_recv,
    cum_send,
    cum_recv,
    halo_sem,
    far_ready,
    st_send,
    st_recv,
    w_send,
    w_recv,
    conv_send,
    conv_recv,
    attn_send,
    attn_recv,
):
    z = lax.axis_index("sp")
    t = lax.axis_index("tp")
    rows, feat = x_hbm.shape
    width = wk_hbm.shape[0]
    heads = cum_hbm.shape[0]
    hd = width // heads
    n_taps = taps_hbm.shape[0]
    half_n = n // 2
    nx = n_tp // 2
    x = t // 2
    c = t % 2

    def at(dx, core):
        return 2 * ((x + dx + nx) % nx) + core

    right, left, far, mate = at(1, c), at(-1, c), at(2, c), at(0, 1 - c)
    up, down = (z + 1) % n, (z + n - 1) % n

    def rdma(src, dst, send, recv, **device):
        return pltpu.make_async_remote_copy(
            src_ref=src, dst_ref=dst, send_sem=send, recv_sem=recv, device_id=device, device_id_type=MESH
        )

    loads = [
        (x_hbm, xg.at[t]),
        (wk_hbm, wkv.at[pl.ds(0, width)]),
        (wv_hbm, wkv.at[pl.ds(width, width)]),
        (gain_hbm, gain),
        (cum_hbm, cum.at[z]),
        (wci_hbm, w3.at[pl.ds(0, width)]),
        (wcg_hbm, w3.at[pl.ds(width, width)]),
        (wq_hbm, w3.at[pl.ds(2 * width, width)]),
        (taps_hbm, taps),
        (lng_hbm, lng),
        (wco_hbm, wc_all.at[pl.ds(pl.multiple_of(t * width, width), width)]),
        (wao_hbm, wa_all.at[pl.ds(pl.multiple_of(t * width, width), width)]),
    ]
    loads = [pltpu.make_async_copy(a, b, ld_sem.at[i]) for i, (a, b) in enumerate(loads)]
    for copy in loads:
        copy.start()

    barrier = pltpu.get_barrier_semaphore()
    for k in range(1, n_tp):
        pl.semaphore_signal(barrier, inc=1, device_id={"tp": (t + k) % n_tp}, device_id_type=MESH)
    last = n - 1
    n_low = last - half_n

    def lowest(p):
        over = jnp.where(p <= half_n + 5, 2, jnp.where(p <= half_n + 11, 1, 0))
        return jnp.maximum(p - half_n - over, 0)

    low, low_up, low_down = lowest(z), lowest(z + 1), lowest(z - 1)
    express = n // 4 + 1
    first_tells = 3
    is_low = z < n_low
    relays_down = low_down > 0

    @pl.when(z > 0)
    def _():
        pl.semaphore_signal(barrier, inc=1, device_id={"sp": down}, device_id_type=MESH)

    @pl.when((low > 0) & (z < last))
    def _():
        pl.semaphore_signal(barrier, inc=1, device_id={"sp": up}, device_id_type=MESH)

    @pl.when(z == express)
    def _():
        pl.semaphore_signal(barrier, inc=1, device_id={"sp": 0}, device_id_type=MESH)

    @pl.when(is_low)
    def _():
        pl.semaphore_signal(barrier, inc=1, device_id={"sp": last}, device_id_type=MESH)

    pl.semaphore_wait(
        barrier,
        n_tp
        - 1
        + jnp.where(z < last, 1, 0)
        + jnp.where(relays_down, 1, 0)
        + jnp.where(z == 0, 1, 0)
        + jnp.where(z == last, n_low, 0),
    )

    def tell(j):
        pl.semaphore_signal(far_ready, inc=1, device_id={"sp": j}, device_id_type=MESH)

    @pl.when(z == last)
    def _():
        for j in range(min(first_tells, n_low)):
            tell(j)

    quarter = rows // 4
    pending = []

    def part(slot, h, m=1):
        return xg.at[slot, pl.ds(h * quarter, m * quarter)]

    def send_in(slot, h, to, m=1):
        k = len(pending)
        copy = rdma(part(slot, h, m), part(slot, h, m), in_send.at[k], in_recv.at[slot, h], tp=to)
        copy.start()
        pending.append(copy)

    def got(slot, h, m=1):
        rdma(part(slot, h, m), part(slot, h, m), in_send.at[0], in_recv.at[slot, h], tp=mate).wait_recv()

    loads[0].wait()
    for h in range(4):
        send_in(t, h, right)
        send_in(t, (h + 2) % 4, left)
    send_in(t, 0, mate, 4)
    for copy in loads[1:4]:
        copy.wait()
    gain32[...] = gain[...].astype(F32)
    kvacc[...] = jnp.zeros_like(kvacc)
    sq[...] = jnp.zeros_like(sq)

    def process(slot):
        xf = xg[slot].astype(F32)
        lanes = pl.ds(pl.multiple_of(slot * feat, feat), feat)
        s2 = xf * xf
        sq[...] += s2[:, :128] + s2[:, 128:]
        scale = [gain32[pl.ds(slot * (feat // 128) + i, 1)] for i in range(feat // 128)]
        sc = (xf * jnp.concatenate(scale, axis=1)).astype(BF16)
        xs[slot] = sc
        kvacc[...] += dot(sc, wkv[:, lanes], NT)

    process(t)
    got(mate, 0, 4)
    process(mate)
    for h in range(2):
        got(left, h)
        send_in(left, h, right)
        got(right, 2 + h)
        send_in(right, 2 + h, left)
    send_in(left, 0, mate, 2)
    send_in(right, 2, mate, 2)
    for h in range(2):
        got(left, 2 + h)
        got(right, h)
    send_in(left, 2, mate, 2)
    send_in(right, 0, mate, 2)
    process(left)
    process(right)
    for slot in (at(-1, 1 - c), at(1, 1 - c)):
        got(slot, 0, 2)
        got(slot, 2, 2)
        process(slot)
    for h in (0, 2, 1, 3):
        got(far, h)
        send_in(far, h, mate)
    process(far)
    for h in (0, 2, 1, 3):
        got(at(2, 1 - c), h)
    process(at(2, 1 - c))

    rms = lax.rsqrt(jnp.sum(sq[...], axis=1, keepdims=True) / (feat * n_tp) + 1e-06)
    kv[z] = (kvacc[...] * rms).astype(BF16)
    loads[4].wait()

    chunk = rows // CHUNKS

    def kv_copy(way, blk, q, k, to):
        ref = kv.at[blk, pl.ds(q * chunk, chunk)]
        return rdma(ref, ref, kv_send.at[way, k % 2, q], kv_recv.at[blk, q], sp=to)

    def cum_copy(way, blk, k, to):
        return rdma(cum.at[blk], cum.at[blk], cum_send.at[way, k % 2], cum_recv.at[blk], sp=to)

    first_up = z < last

    @pl.when(z == last)
    def _():
        for j in range(first_tells, min(first_tells + 3, n_low)):
            tell(j)

    @pl.when(first_up)
    def _():
        cum_copy(0, z, 0, up).start()
        for q in range(CHUNKS):
            kv_copy(0, z, q, 0, up).start()

    def w_part(slot, h):
        whole = wc_all if h == 0 else wa_all
        return whole.at[pl.ds(pl.multiple_of(slot * width, width), width)]

    w_routes = [(t, 0, right), (t, 1, left), (t, 1, right), (t, 0, left), (t, 0, mate), (t, 1, mate)]
    w_routes += [(left, 0, right), (left, 0, mate), (right, 1, left), (right, 1, mate)]
    w_routes += [(left, 1, mate), (right, 0, mate), (far, 0, mate), (far, 1, mate)]
    w_copies = [
        rdma(w_part(slot, h), w_part(slot, h), w_send.at[k], w_recv.at[slot, h], tp=to)
        for k, (slot, h, to) in enumerate(w_routes)
    ]

    def got_w(slot, h):
        rdma(w_part(slot, h), w_part(slot, h), w_send.at[0], w_recv.at[slot, h], tp=mate).wait_recv()

    for copy in loads[10:12]:
        copy.wait()
    for copy in w_copies[:6]:
        copy.start()

    for copy in loads[5:8]:
        copy.wait()
    r3 = dot(xs[0], w3[:, :feat], NT)
    for p in range(1, n_tp):
        r3 += dot(xs[p], w3[:, p * feat : (p + 1) * feat], NT)
    r3 = r3 * rms
    glu = (r3[:, :width] * jax.nn.sigmoid(r3[:, width : 2 * width])).astype(BF16)
    pad = glu_tail.shape[0]
    glu_tail[...] = glu[rows - pad :]
    ext[pl.ds(pad, rows)] = glu.astype(F32)
    ext[pl.ds(pad + rows, 8)] = jnp.zeros((8, width), F32)
    query = (r3[:, 2 * width :]).astype(BF16) * jnp.asarray(hd ** (-0.5), BF16)
    lane = lax.broadcasted_iota(jnp.int32, (rows, width), 1)
    for h in range(heads):
        mine = (lane >= h * hd) & (lane < (h + 1) * hd)
        qs[pl.ds(h * rows, rows)] = jnp.where(mine, query.astype(F32), 0.0).astype(BF16)
    halo_copy = rdma(glu_tail, halo, halo_sem.at[0], halo_sem.at[1], sp=up)

    @pl.when(first_up)
    def _():
        halo_copy.start()

    ones = jnp.ones((rows, width), BF16)

    def attend(h, blocks, diagonal=False):
        here = pl.ds(h * rows, rows)
        q = qs[here]
        scores = []
        for blk in blocks:
            s = dot(q, kv[blk, :, :width], NT)
            s = s + (cum[z, h : h + 1, 0:1] - cum[blk, h : h + 1, :])
            if diagonal:
                q_pos = lax.broadcasted_iota(jnp.int32, s.shape, 0)
                k_pos = lax.broadcasted_iota(jnp.int32, s.shape, 1)
                s = jnp.where(k_pos <= q_pos, s, -1e30)
            scores.append(s)
        best = scores[0]
        for s in scores[1:]:
            best = jnp.maximum(best, s)
        m_new = jnp.broadcast_to(jnp.max(best, axis=1, keepdims=True), (rows, width))
        if not diagonal:
            m_old = m_ref[here]
            m_new = jnp.maximum(m_old, m_new)
        m_ref[here] = m_new
        wide = jnp.concatenate([m_new] * (rows // width), axis=1)
        out = None
        for blk, s in zip(blocks, scores):
            p = jnp.exp(s - wide).astype(BF16)
            o = dot(p, jnp.concatenate([kv[blk, :, width:], ones], axis=1), NN)
            out = o if out is None else out + o
        if diagonal:
            acc[here] = out[:, :width]
            l_ref[here] = out[:, width:]
        else:
            fade = jnp.exp(m_old - m_new)
            acc[here] = acc[here] * fade + out[:, :width]
            l_ref[here] = l_ref[here] * fade + out[:, width:]

    for h in range(heads):
        attend(h, [z], diagonal=True)

    def convolve():
        loads[8].wait()

        @pl.when(z > 0)
        def _():
            halo_copy.wait_recv()
            ext[pl.ds(0, pad)] = halo[...].astype(F32)

        @pl.when(z == 0)
        def _():
            ext[pl.ds(0, pad)] = jnp.zeros((pad, width), F32)

        weight = taps[...].astype(F32)
        shift = pad - (n_taps - 1)
        long = rows + 8
        total = jnp.zeros((rows, width), F32)
        for r in range(8):
            sub = None
            for j in range(n_taps):
                if (shift + j) % 8 == r:
                    base = shift + j - r
                    if r == 0:
                        term = ext[pl.ds(base, rows)] * weight[j : j + 1]
                    else:
                        term = ext[pl.ds(base, long)] * weight[j : j + 1]
                    sub = term if sub is None else sub + term
            if r == 0:
                total = total + sub
            else:
                total = total + pltpu.roll(sub, long - r, 0)[:rows]
        turned = total.T
        ctr[...] = turned
        stats[t, 0:1] = jnp.sum(turned, axis=0, keepdims=True)
        stats[t, 1:2] = jnp.sum(turned * turned, axis=0, keepdims=True)

    def stat_copy(k):
        return rdma(stats.at[t], stats.at[t], st_send.at[k], st_recv.at[t], tp=(t + k) % n_tp)

    def send_stats():
        for k in range(1, n_tp):
            stat_copy(k).start()

    def finish_conv():
        for k in range(1, n_tp):
            src = (t + k) % n_tp
            rdma(stats.at[src], stats.at[src], st_send.at[0], st_recv.at[src], tp=src).wait_recv()
        loads[9].wait()
        tot = stats[0]
        for p in range(1, n_tp):
            tot = tot + stats[p]
        mean = tot[0:1] / (width * n_tp)
        var = tot[1:2] / (width * n_tp) - mean * mean
        y = ((ctr[...] - mean) * lax.rsqrt(var + 1e-05)).T
        y = y * lng[...].astype(F32)
        y = (y * jax.nn.sigmoid(y)).astype(BF16)
        spread(y, conv_src, conv_in, conv_send, conv_recv)

    each = rows // n_tp

    def row_copy(k, src, dst, send, recv):
        d = (t + k) % n_tp
        return rdma(src.at[d], dst.at[t], send.at[k], recv.at[t], tp=d)

    def spread(values, src, dst, send, recv):
        for d in range(n_tp):
            src[d] = values[d * each : (d + 1) * each]
        for k in range(1, n_tp):
            row_copy(k, src, dst, send, recv).start()
        dst[t] = src[t]

    def collect(src, dst, send, recv):
        for k in range(1, n_tp):
            d = (t + k) % n_tp
            rdma(dst.at[d], dst.at[d], send.at[0], recv.at[d], tp=d).wait_recv()
        return jnp.concatenate([dst[d] for d in range(n_tp)], axis=1)

    conv_at = 2
    w_at = (6, 10, 14)
    stats_at = min(5, half_n + 1)

    lag = jnp.where(low > 0, 1 + (2 * (last - z) + 2) // 5, 0)

    def flow_up(s):
        blk = z - s
        comes = (s >= 1) & (blk >= low)
        goes = comes & (z < last) & (blk >= low_up) & jnp.logical_not((blk == 0) & (z == express - 1))
        return comes, goes

    def flow_down(d):
        blk = z + d - n
        comes = (d >= 1) & (blk >= 0) & (blk < low)
        goes = comes & (blk < low_down)
        return comes, goes

    def send_far():
        @pl.when(z == 0)
        def _():
            cum_copy(1, z, 1, express).start()
            for q in range(CHUNKS):
                kv_copy(1, z, q, 1, express).start()

        pl.semaphore_wait(far_ready, 1)
        cum_copy(1, z, 0, last).start()
        for q in range(CHUNKS):
            kv_copy(1, z, q, 0, last).start()

    def step(s, carry):
        d = s - lag
        cw_in, cw_on = flow_up(s)
        cc_in, cc_on = flow_down(d)
        j_cw, j_cc = (z + n - s) % n, (z + n + d) % n
        b_cw, b_cc = (z + n - s + 1) % n, (z + n + d - 1) % n
        has_cw, _ = flow_up(s - 1)
        has_cc, _ = flow_down(d - 1)
        two = has_cw & has_cc
        one = has_cw ^ has_cc
        every = CHUNKS // heads

        @pl.when(is_low & (z < express) & (s == jnp.maximum(z, 1)))
        def _():
            send_far()

        for q in range(CHUNKS):
            for way, arrives, goes, blk, to, k, again in (
                (1, cc_in, cc_on, j_cc, down, d, d - 2 >= n - z),
                (0, cw_in, cw_on, j_cw, up, s, s >= 2),
            ):

                @pl.when(arrives)
                def _(way=way, blk=blk, to=to):
                    if q == 0:
                        cum_copy(way, blk, 0, to).wait_recv()
                    kv_copy(way, blk, q, 0, to).wait_recv()

                @pl.when(goes & again)
                def _(way=way, blk=blk, to=to, k=k):
                    if q == 0:
                        cum_copy(way, blk, k, to).wait_send()
                    kv_copy(way, blk, q, k, to).wait_send()

                @pl.when(goes)
                def _(way=way, blk=blk, to=to, k=k):
                    if q == 0:
                        cum_copy(way, blk, k, to).start()
                    kv_copy(way, blk, q, k, to).start()

            if q % every == every - 1:

                @pl.when(two)
                def _():
                    attend(q // every, [b_cw, b_cc])

                @pl.when(one)
                def _():
                    attend(q // every, [jnp.where(has_cw, b_cw, b_cc)])

        @pl.when((z == last) & (s <= n_low))
        def _():
            first = first_tells + 3 + s + s // 2
            for j, really in ((first - 1, s % 2 < 2), (first, s % 2 == 1)):

                @pl.when(really & (j < n_low))
                def _(j=j):
                    tell(j)

        @pl.when(s == conv_at)
        def _():
            convolve()
            send_stats()

        @pl.when(s == stats_at)
        def _():
            finish_conv()

        @pl.when(s == w_at[0])
        def _():
            got_w(left, 0)
            w_copies[6].start()
            w_copies[7].start()
            got_w(right, 1)
            w_copies[8].start()
            w_copies[9].start()

        @pl.when(s == w_at[1])
        def _():
            got_w(left, 1)
            w_copies[10].start()
            got_w(right, 0)
            w_copies[11].start()

        @pl.when(s == w_at[2])
        def _():
            got_w(far, 0)
            w_copies[12].start()
            got_w(far, 1)
            w_copies[13].start()

        return carry

    steps = jnp.maximum(
        jnp.maximum(z - low + 1, max(stats_at, w_at[2])), jnp.where(low > 0, n - z + low + lag, 0)
    )
    lax.fori_loop(1, steps + 1, step, 0)

    tops, sums = m_ref[...], l_ref[...]
    logs = tops + jnp.log(sums)
    attn = acc[...] / sums
    log_row = logs[:rows]
    attn_row = attn[:rows]
    for h in range(1, heads):
        attn_row = jnp.where(lane >= h * hd, attn[h * rows : (h + 1) * rows], attn_row)
        log_row = jnp.where(lane >= h, logs[h * rows : (h + 1) * rows], log_row)
    spread(attn_row.astype(BF16), attn_src, attn_in, attn_send, attn_recv)

    @pl.when(is_low & (z >= express))
    def _():
        send_far()

    log_ref[...] = log_row.T[:heads] + (cum[z] - cum[z][:, 0:1])
    results = [pltpu.make_async_copy(log_ref, log_hbm, out_sem.at[OUT_CUTS])]
    results[0].start()
    for slot in (mate, at(-1, 1 - c), at(1, 1 - c), at(2, 1 - c)):
        got_w(slot, 0)
        got_w(slot, 1)
    cut = wc_all.shape[1] // OUT_CUTS
    lhs = collect(conv_src, conv_in, conv_send, conv_recv)
    for i in range(OUT_CUTS):
        columns = pl.ds(i * cut, cut)
        conv_part[:, columns] = dot(lhs, wc_all[:, columns], NN)
    lhs = collect(attn_src, attn_in, attn_send, attn_recv)
    for i in range(OUT_CUTS):
        columns = pl.ds(i * cut, cut)
        mixed_ref[:, columns] = (conv_part[:, columns] + dot(lhs, wa_all[:, columns], NN)).astype(BF16)
        results.append(pltpu.make_async_copy(mixed_ref.at[:, columns], mixed_hbm.at[:, columns], out_sem.at[i]))
        results[-1].start()

    for copy in pending:
        copy.wait_send()
    ups = z - low_up - jnp.where(z == express - 1, 1, 0) + 1
    downs = low_down
    for way, parity, cond in (
        (0, 0, first_up),
        (0, 1, first_up & (ups > 1)),
        (1, 0, is_low | (downs > 1) | ((downs == 1) & ((n - z) % 2 == 0))),
        (1, 1, (z == 0) | (downs > 1) | ((downs == 1) & ((n - z) % 2 == 1))),
    ):

        @pl.when(cond)
        def _(way=way, parity=parity):
            cum_copy(way, z, parity, up).wait_send()
            for q in range(CHUNKS):
                kv_copy(way, z, q, parity, up).wait_send()

    @pl.when(first_up)
    def _():
        halo_copy.wait_send()

    for k in range(1, n_tp):
        stat_copy(k).wait_send()

    for copy in w_copies:
        copy.wait_send()
    for k in range(1, n_tp):
        row_copy(k, conv_src, conv_in, conv_send, conv_recv).wait_send()
        row_copy(k, attn_src, attn_in, attn_send, attn_recv).wait_send()
    for copy in results:
        copy.wait()


def solution(mesh):
    n, n_tp = mesh.shape["sp"], mesh.shape["tp"]

    def local(
        inputs,
        norm_gain,
        w_conv_in,
        w_conv_gate,
        conv_kernel,
        ln_gain,
        w_query,
        w_key,
        w_value,
        cum_gate,
        w_conv_out,
        w_attn_out,
    ):
        rows, feat = inputs.shape
        width, full = w_key.shape
        heads = cum_gate.shape[0]
        n_taps = conv_kernel.shape[0]
        each = rows // n_tp
        pad = 32
        half_n = n // 2
        dma = pltpu.SemaphoreType.DMA
        vmem = pltpu.VMEM
        scratch = [
            vmem((each, full), BF16),
            vmem((heads, rows), F32),
            dma((OUT_CUTS + 1,)),
            vmem((n_tp, rows, feat), BF16),
            vmem((n_tp, rows, feat), BF16),
            vmem((full // 128, 128), BF16),
            vmem((full // 128, 128), F32),
            vmem((n_taps, width), BF16),
            vmem((1, width), BF16),
            vmem((2 * width, full), BF16),
            vmem((3 * width, full), BF16),
            vmem((n_tp * width, full), BF16),
            vmem((n_tp * width, full), BF16),
            vmem((n, rows, 2 * width), BF16),
            vmem((n, heads, rows), F32),
            vmem((rows, 2 * width), F32),
            vmem((rows, 128), F32),
            vmem((heads * rows, width), BF16),
            vmem((heads * rows, width), F32),
            vmem((heads * rows, width), F32),
            vmem((heads * rows, width), F32),
            vmem((pad + rows + 8, width), F32),
            vmem((pad, width), BF16),
            vmem((pad, width), BF16),
            vmem((width, rows), F32),
            vmem((n_tp, 2, rows), F32),
            vmem((n_tp, each, width), BF16),
            vmem((n_tp, each, width), BF16),
            vmem((n_tp, each, width), BF16),
            vmem((n_tp, each, width), BF16),
            vmem((each, full), F32),
            dma((12,)),
            dma((21,)),
            dma((n_tp, 4)),
            dma((2, 2, CHUNKS)),
            dma((n, CHUNKS)),
            dma((2, 2)),
            dma((n,)),
            dma((2,)),
            pltpu.SemaphoreType.REGULAR,
            dma((n_tp,)),
            dma((n_tp,)),
            dma((14,)),
            dma((n_tp, 2)),
            dma((n_tp,)),
            dma((n_tp,)),
            dma((n_tp,)),
            dma((n_tp,)),
        ]
        return pl.pallas_call(
            functools.partial(layer, n, n_tp),
            out_shape=(
                jax.ShapeDtypeStruct((each, full), BF16),
                jax.ShapeDtypeStruct((heads, rows), F32),
            ),
            in_specs=[pl.BlockSpec(memory_space=pl.ANY)] * 12,
            out_specs=(pl.BlockSpec(memory_space=pl.ANY), pl.BlockSpec(memory_space=pl.ANY)),
            scratch_shapes=scratch,
            compiler_params=pltpu.CompilerParams(collective_id=0, has_side_effects=True),
        )(
            inputs,
            norm_gain.reshape(full // 128, 128),
            w_conv_in,
            w_conv_gate,
            conv_kernel,
            ln_gain.reshape(1, width),
            w_query,
            w_key,
            w_value,
            cum_gate,
            w_conv_out,
            w_attn_out,
        )

    in_specs = (
        P(("grp", "sp"), "tp"),
        P(),
        P("tp", None),
        P("tp", None),
        P(None, "tp"),
        P("tp"),
        P("tp", None),
        P("tp", None),
        P("tp", None),
        P("tp", ("grp", "sp")),
        P("tp", None),
        P("tp", None),
    )
    out_specs = (P(("grp", "sp", "tp"), None), P("tp", ("grp", "sp")))
    return jax.shard_map(local, mesh=mesh, in_specs=in_specs, out_specs=out_specs, check_vma=False)
```

```python
import functools

import jax
import jax.numpy as jnp
from jax import lax
from jax.experimental import pallas as pl
from jax.experimental.pallas import tpu as pltpu
from jax.sharding import PartitionSpec as P

MESH = pl.DeviceIdType.MESH
F32 = jnp.float32
BF16 = jnp.bfloat16
CHUNKS = 4
OUT_CUTS = 2
NT = (((1,), (1,)), ((), ()))
NN = (((1,), (0,)), ((), ()))


def dot(a, b, dims):
    return lax.dot_general(a, b, dims, preferred_element_type=F32)


def layer(
    n,
    n_tp,
    x_hbm,
    gain_hbm,
    wci_hbm,
    wcg_hbm,
    taps_hbm,
    lng_hbm,
    wq_hbm,
    wk_hbm,
    wv_hbm,
    cum_hbm,
    wco_hbm,
    wao_hbm,
    mixed_hbm,
    log_hbm,
    mixed_ref,
    log_ref,
    out_sem,
    xg,
    xs,
    gain,
    gain32,
    taps,
    lng,
    wkv,
    w3,
    wc_all,
    wa_all,
    kv,
    cum,
    kvacc,
    sq,
    qs,
    m_ref,
    l_ref,
    acc,
    ext,
    glu_tail,
    halo,
    ctr,
    stats,
    conv_src,
    conv_in,
    attn_src,
    attn_in,
    conv_part,
    ld_sem,
    in_send,
    in_recv,
    kv_send,
    kv_recv,
    cum_send,
    cum_recv,
    halo_sem,
    far_ready,
    st_send,
    st_recv,
    pair_out,
    pair_in,
    xout,
    xin,
    pair_send,
    pair_recv,
    x_send,
    x_recv,
    w_send,
    w_recv,
    conv_send,
    conv_recv,
    attn_send,
    attn_recv,
):
    z = lax.axis_index("sp")
    t = lax.axis_index("tp")
    rows, feat = x_hbm.shape
    width = wk_hbm.shape[0]
    heads = cum_hbm.shape[0]
    hd = width // heads
    n_taps = taps_hbm.shape[0]
    half_n = n // 2
    nx = n_tp // 2
    x = t // 2
    c = t % 2

    def at(dx, core):
        return 2 * ((x + dx + nx) % nx) + core

    right, left, far, mate = at(1, c), at(-1, c), at(2, c), at(0, 1 - c)
    up, down = (z + 1) % n, (z + n - 1) % n

    def rdma(src, dst, send, recv, **device):
        return pltpu.make_async_remote_copy(
            src_ref=src, dst_ref=dst, send_sem=send, recv_sem=recv, device_id=device, device_id_type=MESH
        )

    loads = [
        (x_hbm, xg.at[t]),
        (wk_hbm, wkv.at[pl.ds(0, width)]),
        (wv_hbm, wkv.at[pl.ds(width, width)]),
        (gain_hbm, gain),
        (cum_hbm, cum.at[z]),
        (wci_hbm, w3.at[pl.ds(0, width)]),
        (wcg_hbm, w3.at[pl.ds(width, width)]),
        (wq_hbm, w3.at[pl.ds(2 * width, width)]),
        (taps_hbm, taps),
        (lng_hbm, lng),
        (wco_hbm, wc_all.at[pl.ds(pl.multiple_of(t * width, width), width)]),
        (wao_hbm, wa_all.at[pl.ds(pl.multiple_of(t * width, width), width)]),
    ]
    loads = [pltpu.make_async_copy(a, b, ld_sem.at[i]) for i, (a, b) in enumerate(loads)]
    for copy in loads:
        copy.start()

    barrier = pltpu.get_barrier_semaphore()
    for k in range(1, n_tp):
        pl.semaphore_signal(barrier, inc=1, device_id={"tp": (t + k) % n_tp}, device_id_type=MESH)
    last = n - 1
    n_low = last - half_n

    def lowest(p):
        over = jnp.where(p <= half_n + 5, 2, jnp.where(p <= half_n + 11, 1, 0))
        return jnp.maximum(p - half_n - over, 0)

    low, low_up, low_down = lowest(z), lowest(z + 1), lowest(z - 1)
    express = n // 4 + 1
    first_tells = 3
    is_low = z < n_low
    relays_down = low_down > 0

    @pl.when(z > 0)
    def _():
        pl.semaphore_signal(barrier, inc=1, device_id={"sp": down}, device_id_type=MESH)

    @pl.when((low > 0) & (z < last))
    def _():
        pl.semaphore_signal(barrier, inc=1, device_id={"sp": up}, device_id_type=MESH)

    @pl.when(z == express)
    def _():
        pl.semaphore_signal(barrier, inc=1, device_id={"sp": 0}, device_id_type=MESH)

    @pl.when(is_low)
    def _():
        pl.semaphore_signal(barrier, inc=1, device_id={"sp": last}, device_id_type=MESH)

    pl.semaphore_wait(
        barrier,
        n_tp
        - 1
        + jnp.where(z < last, 1, 0)
        + jnp.where(relays_down, 1, 0)
        + jnp.where(z == 0, 1, 0)
        + jnp.where(z == last, n_low, 0),
    )

    def tell(j):
        pl.semaphore_signal(far_ready, inc=1, device_id={"sp": j}, device_id_type=MESH)

    @pl.when(z == last)
    def _():
        for j in range(min(first_tells, n_low)):
            tell(j)

    quarter = rows // 4
    pending = []

    def part(slot, h, m=1):
        return xg.at[slot, pl.ds(h * quarter, m * quarter)]

    def send_in(slot, h, to, m=1):
        k = len(pending)
        copy = rdma(part(slot, h, m), part(slot, h, m), in_send.at[k], in_recv.at[slot, h], tp=to)
        copy.start()
        pending.append(copy)

    def got(slot, h, m=1):
        rdma(part(slot, h, m), part(slot, h, m), in_send.at[0], in_recv.at[slot, h], tp=mate).wait_recv()

    loads[0].wait()
    for h in range(4):
        send_in(t, h, right)
        send_in(t, (h + 2) % 4, left)
    send_in(t, 0, mate, 4)
    for copy in loads[1:4]:
        copy.wait()
    gain32[...] = gain[...].astype(F32)
    kvacc[...] = jnp.zeros_like(kvacc)
    sq[...] = jnp.zeros_like(sq)

    def process(slot):
        xf = xg[slot].astype(F32)
        lanes = pl.ds(pl.multiple_of(slot * feat, feat), feat)
        s2 = xf * xf
        sq[...] += s2[:, :128] + s2[:, 128:]
        scale = [gain32[pl.ds(slot * (feat // 128) + i, 1)] for i in range(feat // 128)]
        sc = (xf * jnp.concatenate(scale, axis=1)).astype(BF16)
        xs[slot] = sc
        kvacc[...] += dot(sc, wkv[:, lanes], NT)

    process(t)
    got(mate, 0, 4)
    process(mate)
    for h in range(2):
        got(left, h)
        send_in(left, h, right)
        got(right, 2 + h)
        send_in(right, 2 + h, left)
    send_in(left, 0, mate, 2)
    send_in(right, 2, mate, 2)
    for h in range(2):
        got(left, 2 + h)
        got(right, h)
    send_in(left, 2, mate, 2)
    send_in(right, 0, mate, 2)
    process(left)
    process(right)
    for slot in (at(-1, 1 - c), at(1, 1 - c)):
        got(slot, 0, 2)
        got(slot, 2, 2)
        process(slot)
    for h in (0, 2, 1, 3):
        got(far, h)
        send_in(far, h, mate)
    process(far)
    for h in (0, 2, 1, 3):
        got(at(2, 1 - c), h)
    process(at(2, 1 - c))

    rms = lax.rsqrt(jnp.sum(sq[...], axis=1, keepdims=True) / (feat * n_tp) + 1e-06)
    kv[z] = (kvacc[...] * rms).astype(BF16)
    loads[4].wait()

    chunk = rows // CHUNKS

    def kv_copy(way, blk, q, k, to):
        ref = kv.at[blk, pl.ds(q * chunk, chunk)]
        return rdma(ref, ref, kv_send.at[way, k % 2, q], kv_recv.at[blk, q], sp=to)

    def cum_copy(way, blk, k, to):
        return rdma(cum.at[blk], cum.at[blk], cum_send.at[way, k % 2], cum_recv.at[blk], sp=to)

    first_up = z < last

    @pl.when(z == last)
    def _():
        for j in range(first_tells, min(first_tells + 3, n_low)):
            tell(j)

    @pl.when(first_up)
    def _():
        cum_copy(0, z, 0, up).start()
        for q in range(CHUNKS):
            kv_copy(0, z, q, 0, up).start()

    def w_part(slot, h):
        whole = wc_all if h == 0 else wa_all
        return whole.at[pl.ds(pl.multiple_of(slot * width, width), width)]

    w_routes = [(t, 0, right), (t, 1, left), (t, 1, right), (t, 0, left), (t, 0, mate), (t, 1, mate)]
    w_routes += [(left, 0, right), (left, 0, mate), (right, 1, left), (right, 1, mate)]
    w_routes += [(left, 1, mate), (right, 0, mate), (far, 0, mate), (far, 1, mate)]
    w_copies = [
        rdma(w_part(slot, h), w_part(slot, h), w_send.at[k], w_recv.at[slot, h], tp=to)
        for k, (slot, h, to) in enumerate(w_routes)
    ]

    def got_w(slot, h):
        rdma(w_part(slot, h), w_part(slot, h), w_send.at[0], w_recv.at[slot, h], tp=mate).wait_recv()

    for copy in loads[10:12]:
        copy.wait()
    @pl.when(z > 0)
    def _():
        for copy in w_copies[:6]:
            copy.start()

    for copy in loads[5:8]:
        copy.wait()
    r3 = dot(xs[0], w3[:, :feat], NT)
    for p in range(1, n_tp):
        r3 += dot(xs[p], w3[:, p * feat : (p + 1) * feat], NT)
    r3 = r3 * rms
    glu = (r3[:, :width] * jax.nn.sigmoid(r3[:, width : 2 * width])).astype(BF16)
    pad = glu_tail.shape[0]
    glu_tail[...] = glu[rows - pad :]
    ext[pl.ds(pad, rows)] = glu.astype(F32)
    ext[pl.ds(pad + rows, 8)] = jnp.zeros((8, width), F32)
    query = (r3[:, 2 * width :]).astype(BF16) * jnp.asarray(hd ** (-0.5), BF16)
    lane = lax.broadcasted_iota(jnp.int32, (rows, width), 1)
    for h in range(heads):
        mine = (lane >= h * hd) & (lane < (h + 1) * hd)
        qs[pl.ds(h * rows, rows)] = jnp.where(mine, query.astype(F32), 0.0).astype(BF16)
    halo_copy = rdma(glu_tail, halo, halo_sem.at[0], halo_sem.at[1], sp=up)

    @pl.when(first_up)
    def _():
        halo_copy.start()

    ones = jnp.ones((rows, width), BF16)

    def attend(h, blocks, diagonal=False):
        here = pl.ds(h * rows, rows)
        q = qs[here]
        scores = []
        for blk in blocks:
            s = dot(q, kv[blk, :, :width], NT)
            s = s + (cum[z, h : h + 1, 0:1] - cum[blk, h : h + 1, :])
            if diagonal:
                q_pos = lax.broadcasted_iota(jnp.int32, s.shape, 0)
                k_pos = lax.broadcasted_iota(jnp.int32, s.shape, 1)
                s = jnp.where(k_pos <= q_pos, s, -1e30)
            scores.append(s)
        best = scores[0]
        for s in scores[1:]:
            best = jnp.maximum(best, s)
        m_new = jnp.broadcast_to(jnp.max(best, axis=1, keepdims=True), (rows, width))
        if not diagonal:
            m_old = m_ref[here]
            m_new = jnp.maximum(m_old, m_new)
        m_ref[here] = m_new
        wide = jnp.concatenate([m_new] * (rows // width), axis=1)
        out = None
        for blk, s in zip(blocks, scores):
            p = jnp.exp(s - wide).astype(BF16)
            o = dot(p, jnp.concatenate([kv[blk, :, width:], ones], axis=1), NN)
            out = o if out is None else out + o
        if diagonal:
            acc[here] = out[:, :width]
            l_ref[here] = out[:, width:]
        else:
            fade = jnp.exp(m_old - m_new)
            acc[here] = acc[here] * fade + out[:, :width]
            l_ref[here] = l_ref[here] * fade + out[:, width:]

    for h in range(heads):
        attend(h, [z], diagonal=True)

    def convolve():
        loads[8].wait()

        @pl.when(z > 0)
        def _():
            halo_copy.wait_recv()
            ext[pl.ds(0, pad)] = halo[...].astype(F32)

        @pl.when(z == 0)
        def _():
            ext[pl.ds(0, pad)] = jnp.zeros((pad, width), F32)

        weight = taps[...].astype(F32)
        shift = pad - (n_taps - 1)
        long = rows + 8
        total = jnp.zeros((rows, width), F32)
        for r in range(8):
            sub = None
            for j in range(n_taps):
                if (shift + j) % 8 == r:
                    base = shift + j - r
                    if r == 0:
                        term = ext[pl.ds(base, rows)] * weight[j : j + 1]
                    else:
                        term = ext[pl.ds(base, long)] * weight[j : j + 1]
                    sub = term if sub is None else sub + term
            if r == 0:
                total = total + sub
            else:
                total = total + pltpu.roll(sub, long - r, 0)[:rows]
        turned = total.T
        ctr[...] = turned
        stats[t, 0:1] = jnp.sum(turned, axis=0, keepdims=True)
        stats[t, 1:2] = jnp.sum(turned * turned, axis=0, keepdims=True)

    def stat_copy(k):
        return rdma(stats.at[t], stats.at[t], st_send.at[k], st_recv.at[t], tp=(t + k) % n_tp)

    def send_stats():
        for k in range(1, n_tp):
            stat_copy(k).start()

    def finish_conv():
        for k in range(1, n_tp):
            src = (t + k) % n_tp
            rdma(stats.at[src], stats.at[src], st_send.at[0], st_recv.at[src], tp=src).wait_recv()
        loads[9].wait()
        tot = stats[0]
        for p in range(1, n_tp):
            tot = tot + stats[p]
        mean = tot[0:1] / (width * n_tp)
        var = tot[1:2] / (width * n_tp) - mean * mean
        y = ((ctr[...] - mean) * lax.rsqrt(var + 1e-05)).T
        y = y * lng[...].astype(F32)
        y = (y * jax.nn.sigmoid(y)).astype(BF16)
        split(y, conv_src)

        @pl.when(z > 0)
        def _():
            spread(conv_src, conv_in, conv_send, conv_recv)

    each = rows // n_tp

    def row_copy(k, src, dst, send, recv):
        d = (t + k) % n_tp
        return rdma(src.at[d], dst.at[t], send.at[k], recv.at[t], tp=d)

    def split(values, src):
        for d in range(n_tp):
            src[d] = values[d * each : (d + 1) * each]

    def spread(src, dst, send, recv):
        for k in range(1, n_tp):
            row_copy(k, src, dst, send, recv).start()
        dst[t] = src[t]

    def collect(src, dst, send, recv):
        for k in range(1, n_tp):
            d = (t + k) % n_tp
            rdma(dst.at[d], dst.at[d], send.at[0], recv.at[d], tp=d).wait_recv()
        return jnp.concatenate([dst[d] for d in range(n_tp)], axis=1)

    conv_at = 2
    w_at = (6, 10, 14)
    stats_at = 12

    lag = jnp.where(low > 0, 1 + (2 * (last - z) + 2) // 5, 0)

    def flow_up(s):
        blk = z - s
        comes = (s >= 1) & (blk >= low)
        goes = comes & (z < last) & (blk >= low_up) & jnp.logical_not((blk == 0) & (z == express - 1))
        return comes, goes

    def flow_down(d):
        blk = z + d - n
        comes = (d >= 1) & (blk >= 0) & (blk < low)
        goes = comes & (blk < low_down)
        return comes, goes

    def send_far():
        @pl.when(z == 0)
        def _():
            cum_copy(1, z, 1, express).start()
            for q in range(CHUNKS):
                kv_copy(1, z, q, 1, express).start()

        pl.semaphore_wait(far_ready, 1)
        cum_copy(1, z, 0, last).start()
        for q in range(CHUNKS):
            kv_copy(1, z, q, 0, last).start()

    def step(s, carry):
        d = s - lag
        cw_in, cw_on = flow_up(s)
        cc_in, cc_on = flow_down(d)
        j_cw, j_cc = (z + n - s) % n, (z + n + d) % n
        b_cw, b_cc = (z + n - s + 1) % n, (z + n + d - 1) % n
        has_cw, _ = flow_up(s - 1)
        has_cc, _ = flow_down(d - 1)
        two = has_cw & has_cc
        one = has_cw ^ has_cc
        every = CHUNKS // heads

        @pl.when(is_low & (z < express) & (s == jnp.maximum(z, 1)))
        def _():
            send_far()

        for q in range(CHUNKS):
            for way, arrives, goes, blk, to, k, again in (
                (1, cc_in, cc_on, j_cc, down, d, d - 2 >= n - z),
                (0, cw_in, cw_on, j_cw, up, s, s >= 2),
            ):

                @pl.when(arrives)
                def _(way=way, blk=blk, to=to):
                    if q == 0:
                        cum_copy(way, blk, 0, to).wait_recv()
                    kv_copy(way, blk, q, 0, to).wait_recv()

                @pl.when(goes & again)
                def _(way=way, blk=blk, to=to, k=k):
                    if q == 0:
                        cum_copy(way, blk, k, to).wait_send()
                    kv_copy(way, blk, q, k, to).wait_send()

                @pl.when(goes)
                def _(way=way, blk=blk, to=to, k=k):
                    if q == 0:
                        cum_copy(way, blk, k, to).start()
                    kv_copy(way, blk, q, k, to).start()

            if q % every == every - 1:

                @pl.when(two)
                def _():
                    attend(q // every, [b_cw, b_cc])

                @pl.when(one)
                def _():
                    attend(q // every, [jnp.where(has_cw, b_cw, b_cc)])

        @pl.when((z == last) & (s <= n_low))
        def _():
            first = first_tells + 3 + s + s // 2
            for j, really in ((first - 1, s % 2 < 2), (first, s % 2 == 1)):

                @pl.when(really & (j < n_low))
                def _(j=j):
                    tell(j)

        @pl.when(s == conv_at)
        def _():
            convolve()
            send_stats()

        @pl.when(s == stats_at)
        def _():
            finish_conv()

        @pl.when((z > 0) & (s == w_at[0]))
        def _():
            got_w(left, 0)
            w_copies[6].start()
            w_copies[7].start()
            got_w(right, 1)
            w_copies[8].start()
            w_copies[9].start()

        @pl.when((z > 0) & (s == w_at[1]))
        def _():
            got_w(left, 1)
            w_copies[10].start()
            got_w(right, 0)
            w_copies[11].start()

        @pl.when((z > 0) & (s == w_at[2]))
        def _():
            got_w(far, 0)
            w_copies[12].start()
            got_w(far, 1)
            w_copies[13].start()

        return carry

    steps = jnp.maximum(
        jnp.maximum(z - low + 1, max(stats_at, w_at[2])), jnp.where(low > 0, n - z + low + lag, 0)
    )
    lax.fori_loop(1, steps + 1, step, 0)

    tops, sums = m_ref[...], l_ref[...]
    logs = tops + jnp.log(sums)
    attn = acc[...] / sums
    log_row = logs[:rows]
    attn_row = attn[:rows]
    for h in range(1, heads):
        attn_row = jnp.where(lane >= h * hd, attn[h * rows : (h + 1) * rows], attn_row)
        log_row = jnp.where(lane >= h, logs[h * rows : (h + 1) * rows], log_row)
    split(attn_row.astype(BF16), attn_src)
    cut = wc_all.shape[1] // OUT_CUTS
    nx = n_tp // 2
    own_rows = pl.ds(pl.multiple_of(t * width, width), width)

    def product(core, i):
        columns = slice(i * cut, (i + 1) * cut)
        conv = jnp.concatenate([conv_src[2 * k + core] for k in range(nx)], axis=0)
        attn = jnp.concatenate([attn_src[2 * k + core] for k in range(nx)], axis=0)
        total = dot(conv, wc_all[own_rows, columns], NN) + dot(attn, wa_all[own_rows, columns], NN)
        return total.reshape(nx, each, cut)

    @pl.when(z > 0)
    def _():
        spread(attn_src, attn_in, attn_send, attn_recv)

    @pl.when(is_low & (z >= express))
    def _():
        send_far()

    log_ref[...] = log_row.T[:heads] + (cum[z] - cum[z][:, 0:1])
    results = [pltpu.make_async_copy(log_ref, log_hbm, out_sem.at[OUT_CUTS])]
    results[0].start()
    @pl.when(z > 0)
    def _():
        for slot in (mate, at(-1, 1 - c), at(1, 1 - c), at(2, 1 - c)):
            got_w(slot, 0)
            got_w(slot, 1)
        lhs = collect(conv_src, conv_in, conv_send, conv_recv)
        for i in range(OUT_CUTS):
            columns = pl.ds(i * cut, cut)
            conv_part[:, columns] = dot(lhs, wc_all[:, columns], NN)
        lhs = collect(attn_src, attn_in, attn_send, attn_recv)
        for i in range(OUT_CUTS):
            columns = pl.ds(i * cut, cut)
            mixed_ref[:, columns] = (conv_part[:, columns] + dot(lhs, wa_all[:, columns], NN)).astype(BF16)

    @pl.when(z == 0)
    def _():
        pairs = []
        for i in range(OUT_CUTS):
            pair_out[i] = product(1 - c, i).astype(BF16)
            copy = rdma(pair_out.at[i], pair_in.at[i], pair_send.at[i], pair_recv.at[i], tp=mate)
            copy.start()
            pairs.append(copy)
        outs = []
        for i in range(OUT_CUTS):
            own = product(c, i)
            pairs[i].wait_recv()
            xout[i] = (own + pair_in[i].astype(F32)).astype(BF16)
            for dx in (2, 1, 3):
                copy = rdma(
                    xout.at[i, (x + dx) % nx], xin.at[i, dx - 1], x_send.at[i, dx - 1], x_recv.at[i, dx - 1], tp=at(dx - nx, c)
                )
                copy.start()
                outs.append((i, copy))
        for i in range(OUT_CUTS):
            total = xout[i, x].astype(F32)
            for k, copy in outs:
                if k == i:
                    copy.wait_recv()
            for dx in range(nx - 1):
                total = total + xin[i, dx].astype(F32)
            mixed_ref[:, i * cut : (i + 1) * cut] = total.astype(BF16)
        for copy in pairs:
            copy.wait_send()
        for k, copy in outs:
            copy.wait_send()

    results.append(pltpu.make_async_copy(mixed_ref, mixed_hbm, out_sem.at[0]))
    results[-1].start()

    for copy in pending:
        copy.wait_send()
    ups = z - low_up - jnp.where(z == express - 1, 1, 0) + 1
    downs = low_down
    for way, parity, cond in (
        (0, 0, first_up),
        (0, 1, first_up & (ups > 1)),
        (1, 0, is_low | (downs > 1) | ((downs == 1) & ((n - z) % 2 == 0))),
        (1, 1, (z == 0) | (downs > 1) | ((downs == 1) & ((n - z) % 2 == 1))),
    ):

        @pl.when(cond)
        def _(way=way, parity=parity):
            cum_copy(way, z, parity, up).wait_send()
            for q in range(CHUNKS):
                kv_copy(way, z, q, parity, up).wait_send()

    @pl.when(first_up)
    def _():
        halo_copy.wait_send()

    for k in range(1, n_tp):
        stat_copy(k).wait_send()

    @pl.when(z > 0)
    def _():
        for copy in w_copies:
            copy.wait_send()
        for k in range(1, n_tp):
            row_copy(k, conv_src, conv_in, conv_send, conv_recv).wait_send()
            row_copy(k, attn_src, attn_in, attn_send, attn_recv).wait_send()

    for copy in results:
        copy.wait()


def solution(mesh):
    n, n_tp = mesh.shape["sp"], mesh.shape["tp"]

    def local(
        inputs,
        norm_gain,
        w_conv_in,
        w_conv_gate,
        conv_kernel,
        ln_gain,
        w_query,
        w_key,
        w_value,
        cum_gate,
        w_conv_out,
        w_attn_out,
    ):
        rows, feat = inputs.shape
        width, full = w_key.shape
        heads = cum_gate.shape[0]
        n_taps = conv_kernel.shape[0]
        each = rows // n_tp
        pad = 32
        half_n = n // 2
        dma = pltpu.SemaphoreType.DMA
        vmem = pltpu.VMEM
        scratch = [
            vmem((each, full), BF16),
            vmem((heads, rows), F32),
            dma((OUT_CUTS + 1,)),
            vmem((n_tp, rows, feat), BF16),
            vmem((n_tp, rows, feat), BF16),
            vmem((full // 128, 128), BF16),
            vmem((full // 128, 128), F32),
            vmem((n_taps, width), BF16),
            vmem((1, width), BF16),
            vmem((2 * width, full), BF16),
            vmem((3 * width, full), BF16),
            vmem((n_tp * width, full), BF16),
            vmem((n_tp * width, full), BF16),
            vmem((n, rows, 2 * width), BF16),
            vmem((n, heads, rows), F32),
            vmem((rows, 2 * width), F32),
            vmem((rows, 128), F32),
            vmem((heads * rows, width), BF16),
            vmem((heads * rows, width), F32),
            vmem((heads * rows, width), F32),
            vmem((heads * rows, width), F32),
            vmem((pad + rows + 8, width), F32),
            vmem((pad, width), BF16),
            vmem((pad, width), BF16),
            vmem((width, rows), F32),
            vmem((n_tp, 2, rows), F32),
            vmem((n_tp, each, width), BF16),
            vmem((n_tp, each, width), BF16),
            vmem((n_tp, each, width), BF16),
            vmem((n_tp, each, width), BF16),
            vmem((each, full), F32),
            dma((12,)),
            dma((21,)),
            dma((n_tp, 4)),
            dma((2, 2, CHUNKS)),
            dma((n, CHUNKS)),
            dma((2, 2)),
            dma((n,)),
            dma((2,)),
            pltpu.SemaphoreType.REGULAR,
            dma((n_tp,)),
            dma((n_tp,)),
            vmem((OUT_CUTS, n_tp // 2, each, full // OUT_CUTS), BF16),
            vmem((OUT_CUTS, n_tp // 2, each, full // OUT_CUTS), BF16),
            vmem((OUT_CUTS, n_tp // 2, each, full // OUT_CUTS), BF16),
            vmem((OUT_CUTS, n_tp // 2 - 1, each, full // OUT_CUTS), BF16),
            dma((OUT_CUTS,)),
            dma((OUT_CUTS,)),
            dma((OUT_CUTS, n_tp // 2 - 1)),
            dma((OUT_CUTS, n_tp // 2 - 1)),
            dma((14,)),
            dma((n_tp, 2)),
            dma((n_tp,)),
            dma((n_tp,)),
            dma((n_tp,)),
            dma((n_tp,)),
        ]
        return pl.pallas_call(
            functools.partial(layer, n, n_tp),
            out_shape=(
                jax.ShapeDtypeStruct((each, full), BF16),
                jax.ShapeDtypeStruct((heads, rows), F32),
            ),
            in_specs=[pl.BlockSpec(memory_space=pl.ANY)] * 12,
            out_specs=(pl.BlockSpec(memory_space=pl.ANY), pl.BlockSpec(memory_space=pl.ANY)),
            scratch_shapes=scratch,
            compiler_params=pltpu.CompilerParams(collective_id=0, has_side_effects=True),
        )(
            inputs,
            norm_gain.reshape(full // 128, 128),
            w_conv_in,
            w_conv_gate,
            conv_kernel,
            ln_gain.reshape(1, width),
            w_query,
            w_key,
            w_value,
            cum_gate,
            w_conv_out,
            w_attn_out,
        )

    in_specs = (
        P(("grp", "sp"), "tp"),
        P(),
        P("tp", None),
        P("tp", None),
        P(None, "tp"),
        P("tp"),
        P("tp", None),
        P("tp", None),
        P("tp", None),
        P("tp", ("grp", "sp")),
        P("tp", None),
        P("tp", None),
    )
    out_specs = (P(("grp", "sp", "tp"), None), P("tp", ("grp", "sp")))
    return jax.shard_map(local, mesh=mesh, in_specs=in_specs, out_specs=out_specs, check_vma=False)
```

```python
import functools

import jax
import jax.numpy as jnp
from jax import lax
from jax.experimental import pallas as pl
from jax.experimental.pallas import tpu as pltpu
from jax.sharding import PartitionSpec as P

MESH = pl.DeviceIdType.MESH
F32 = jnp.float32
BF16 = jnp.bfloat16
CHUNKS = 4
OUT_CUTS = 2
NT = (((1,), (1,)), ((), ()))
NN = (((1,), (0,)), ((), ()))


def dot(a, b, dims):
    return lax.dot_general(a, b, dims, preferred_element_type=F32)


def layer(
    n,
    n_tp,
    x_hbm,
    gain_hbm,
    wci_hbm,
    wcg_hbm,
    taps_hbm,
    lng_hbm,
    wq_hbm,
    wk_hbm,
    wv_hbm,
    cum_hbm,
    wco_hbm,
    wao_hbm,
    mixed_hbm,
    log_hbm,
    mixed_ref,
    log_ref,
    out_sem,
    xg,
    xs,
    gain,
    gain32,
    taps,
    lng,
    wkv,
    w3,
    wc_all,
    wa_all,
    kv,
    cum,
    kvacc,
    sq,
    qs,
    m_ref,
    l_ref,
    acc,
    ext,
    glu_tail,
    halo,
    ctr,
    stats,
    conv_src,
    conv_in,
    attn_src,
    attn_in,
    conv_part,
    ld_sem,
    in_send,
    in_recv,
    kv_send,
    kv_recv,
    cum_send,
    cum_recv,
    halo_sem,
    far_ready,
    st_send,
    st_recv,
    pair_out,
    pair_in,
    xout,
    xin,
    pair_send,
    pair_recv,
    x_send,
    x_recv,
    w_send,
    w_recv,
    conv_send,
    conv_recv,
    attn_send,
    attn_recv,
):
    z = lax.axis_index("sp")
    t = lax.axis_index("tp")
    rows, feat = x_hbm.shape
    width = wk_hbm.shape[0]
    heads = cum_hbm.shape[0]
    hd = width // heads
    n_taps = taps_hbm.shape[0]
    half_n = n // 2
    nx = n_tp // 2
    x = t // 2
    c = t % 2

    def at(dx, core):
        return 2 * ((x + dx + nx) % nx) + core

    right, left, far, mate = at(1, c), at(-1, c), at(2, c), at(0, 1 - c)
    up, down = (z + 1) % n, (z + n - 1) % n

    def rdma(src, dst, send, recv, **device):
        return pltpu.make_async_remote_copy(
            src_ref=src, dst_ref=dst, send_sem=send, recv_sem=recv, device_id=device, device_id_type=MESH
        )

    loads = [
        (x_hbm, xg.at[t]),
        (wk_hbm, wkv.at[pl.ds(0, width)]),
        (wv_hbm, wkv.at[pl.ds(width, width)]),
        (gain_hbm, gain),
        (cum_hbm, cum.at[z]),
        (wci_hbm, w3.at[pl.ds(0, width)]),
        (wcg_hbm, w3.at[pl.ds(width, width)]),
        (wq_hbm, w3.at[pl.ds(2 * width, width)]),
        (taps_hbm, taps),
        (lng_hbm, lng),
        (wco_hbm, wc_all.at[pl.ds(pl.multiple_of(t * width, width), width)]),
        (wao_hbm, wa_all.at[pl.ds(pl.multiple_of(t * width, width), width)]),
    ]
    loads = [pltpu.make_async_copy(a, b, ld_sem.at[i]) for i, (a, b) in enumerate(loads)]
    for copy in loads:
        copy.start()

    barrier = pltpu.get_barrier_semaphore()
    for k in range(1, n_tp):
        pl.semaphore_signal(barrier, inc=1, device_id={"tp": (t + k) % n_tp}, device_id_type=MESH)
    last = n - 1
    n_low = last - half_n

    def lowest(p):
        over = jnp.where(p <= half_n + 5, 2, jnp.where(p <= half_n + 11, 1, 0))
        return jnp.maximum(p - half_n - over, 0)

    low, low_up, low_down = lowest(z), lowest(z + 1), lowest(z - 1)
    express = n // 4 + 1
    first_tells = 4
    is_low = z < n_low
    relays_down = low_down > 0

    @pl.when(z > 0)
    def _():
        pl.semaphore_signal(barrier, inc=1, device_id={"sp": down}, device_id_type=MESH)

    @pl.when((low > 0) & (z < last))
    def _():
        pl.semaphore_signal(barrier, inc=1, device_id={"sp": up}, device_id_type=MESH)

    @pl.when(z == express)
    def _():
        pl.semaphore_signal(barrier, inc=1, device_id={"sp": 0}, device_id_type=MESH)

    @pl.when(is_low)
    def _():
        pl.semaphore_signal(barrier, inc=1, device_id={"sp": last}, device_id_type=MESH)

    pl.semaphore_wait(
        barrier,
        n_tp
        - 1
        + jnp.where(z < last, 1, 0)
        + jnp.where(relays_down, 1, 0)
        + jnp.where(z == 0, 1, 0)
        + jnp.where(z == last, n_low, 0),
    )

    def tell(j):
        pl.semaphore_signal(far_ready, inc=1, device_id={"sp": j}, device_id_type=MESH)

    @pl.when(z == last)
    def _():
        for j in range(min(first_tells, n_low)):
            tell(j)

    quarter = rows // 4
    pending = []

    def part(slot, h, m=1):
        return xg.at[slot, pl.ds(h * quarter, m * quarter)]

    def send_in(slot, h, to, m=1):
        k = len(pending)
        copy = rdma(part(slot, h, m), part(slot, h, m), in_send.at[k], in_recv.at[slot, h], tp=to)
        copy.start()
        pending.append(copy)

    def got(slot, h, m=1):
        rdma(part(slot, h, m), part(slot, h, m), in_send.at[0], in_recv.at[slot, h], tp=mate).wait_recv()

    loads[0].wait()
    for h in range(4):
        send_in(t, h, right)
        send_in(t, (h + 2) % 4, left)
    send_in(t, 0, mate, 4)
    for copy in loads[1:4]:
        copy.wait()
    gain32[...] = gain[...].astype(F32)
    kvacc[...] = jnp.zeros_like(kvacc)
    sq[...] = jnp.zeros_like(sq)

    def process(slot):
        xf = xg[slot].astype(F32)
        lanes = pl.ds(pl.multiple_of(slot * feat, feat), feat)
        s2 = xf * xf
        sq[...] += s2[:, :128] + s2[:, 128:]
        scale = [gain32[pl.ds(slot * (feat // 128) + i, 1)] for i in range(feat // 128)]
        sc = (xf * jnp.concatenate(scale, axis=1)).astype(BF16)
        xs[slot] = sc
        kvacc[...] += dot(sc, wkv[:, lanes], NT)

    process(t)
    got(mate, 0, 4)
    process(mate)
    for h in range(2):
        got(left, h)
        send_in(left, h, right)
        got(right, 2 + h)
        send_in(right, 2 + h, left)
    send_in(left, 0, mate, 2)
    send_in(right, 2, mate, 2)
    for h in range(2):
        got(left, 2 + h)
        got(right, h)
    send_in(left, 2, mate, 2)
    send_in(right, 0, mate, 2)
    process(left)
    process(right)
    for slot in (at(-1, 1 - c), at(1, 1 - c)):
        got(slot, 0, 2)
        got(slot, 2, 2)
        process(slot)
    for h in (0, 2, 1, 3):
        got(far, h)
        send_in(far, h, mate)
    process(far)
    for h in (0, 2, 1, 3):
        got(at(2, 1 - c), h)
    process(at(2, 1 - c))

    rms = lax.rsqrt(jnp.sum(sq[...], axis=1, keepdims=True) / (feat * n_tp) + 1e-06)
    kv[z] = (kvacc[...] * rms).astype(BF16)
    loads[4].wait()

    chunk = rows // CHUNKS

    def kv_copy(way, blk, q, k, to):
        ref = kv.at[blk, pl.ds(q * chunk, chunk)]
        return rdma(ref, ref, kv_send.at[way, k % 2, q], kv_recv.at[blk, q], sp=to)

    def cum_copy(way, blk, k, to):
        return rdma(cum.at[blk], cum.at[blk], cum_send.at[way, k % 2], cum_recv.at[blk], sp=to)

    first_up = z < last

    @pl.when(z == last)
    def _():
        for j in range(first_tells, min(first_tells + 2, n_low)):
            tell(j)

    @pl.when(first_up)
    def _():
        cum_copy(0, z, 0, up).start()
        for q in range(CHUNKS):
            kv_copy(0, z, q, 0, up).start()

    def w_part(slot, h):
        whole = wc_all if h == 0 else wa_all
        return whole.at[pl.ds(pl.multiple_of(slot * width, width), width)]

    w_routes = [(t, 0, right), (t, 1, left), (t, 1, right), (t, 0, left), (t, 0, mate), (t, 1, mate)]
    w_routes += [(left, 0, right), (left, 0, mate), (right, 1, left), (right, 1, mate)]
    w_routes += [(left, 1, mate), (right, 0, mate), (far, 0, mate), (far, 1, mate)]
    w_copies = [
        rdma(w_part(slot, h), w_part(slot, h), w_send.at[k], w_recv.at[slot, h], tp=to)
        for k, (slot, h, to) in enumerate(w_routes)
    ]

    def got_w(slot, h):
        rdma(w_part(slot, h), w_part(slot, h), w_send.at[0], w_recv.at[slot, h], tp=mate).wait_recv()

    for copy in loads[10:12]:
        copy.wait()
    @pl.when(z > 0)
    def _():
        for copy in w_copies[:6]:
            copy.start()

    for copy in loads[5:8]:
        copy.wait()
    r3 = dot(xs[0], w3[:, :feat], NT)
    for p in range(1, n_tp):
        r3 += dot(xs[p], w3[:, p * feat : (p + 1) * feat], NT)
    r3 = r3 * rms
    glu = (r3[:, :width] * jax.nn.sigmoid(r3[:, width : 2 * width])).astype(BF16)
    pad = glu_tail.shape[0]
    glu_tail[...] = glu[rows - pad :]
    ext[pl.ds(pad, rows)] = glu.astype(F32)
    ext[pl.ds(pad + rows, 8)] = jnp.zeros((8, width), F32)
    query = (r3[:, 2 * width :]).astype(BF16) * jnp.asarray(hd ** (-0.5), BF16)
    lane = lax.broadcasted_iota(jnp.int32, (rows, width), 1)
    for h in range(heads):
        mine = (lane >= h * hd) & (lane < (h + 1) * hd)
        qs[pl.ds(h * rows, rows)] = jnp.where(mine, query.astype(F32), 0.0).astype(BF16)
    halo_copy = rdma(glu_tail, halo, halo_sem.at[0], halo_sem.at[1], sp=up)

    @pl.when(first_up)
    def _():
        halo_copy.start()

    ones = jnp.ones((rows, width), BF16)

    def attend(h, blocks, diagonal=False):
        here = pl.ds(h * rows, rows)
        q = qs[here]
        scores = []
        for blk in blocks:
            s = dot(q, kv[blk, :, :width], NT)
            s = s + (cum[z, h : h + 1, 0:1] - cum[blk, h : h + 1, :])
            if diagonal:
                q_pos = lax.broadcasted_iota(jnp.int32, s.shape, 0)
                k_pos = lax.broadcasted_iota(jnp.int32, s.shape, 1)
                s = jnp.where(k_pos <= q_pos, s, -1e30)
            scores.append(s)
        best = scores[0]
        for s in scores[1:]:
            best = jnp.maximum(best, s)
        m_new = jnp.broadcast_to(jnp.max(best, axis=1, keepdims=True), (rows, width))
        if not diagonal:
            m_old = m_ref[here]
            m_new = jnp.maximum(m_old, m_new)
        m_ref[here] = m_new
        wide = jnp.concatenate([m_new] * (rows // width), axis=1)
        out = None
        for blk, s in zip(blocks, scores):
            p = jnp.exp(s - wide).astype(BF16)
            o = dot(p, jnp.concatenate([kv[blk, :, width:], ones], axis=1), NN)
            out = o if out is None else out + o
        if diagonal:
            acc[here] = out[:, :width]
            l_ref[here] = out[:, width:]
        else:
            fade = jnp.exp(m_old - m_new)
            acc[here] = acc[here] * fade + out[:, :width]
            l_ref[here] = l_ref[here] * fade + out[:, width:]

    for h in range(heads):
        attend(h, [z], diagonal=True)

    def convolve():
        loads[8].wait()

        @pl.when(z > 0)
        def _():
            halo_copy.wait_recv()
            ext[pl.ds(0, pad)] = halo[...].astype(F32)

        @pl.when(z == 0)
        def _():
            ext[pl.ds(0, pad)] = jnp.zeros((pad, width), F32)

        weight = taps[...].astype(F32)
        shift = pad - (n_taps - 1)
        long = rows + 8
        total = jnp.zeros((rows, width), F32)
        for r in range(8):
            sub = None
            for j in range(n_taps):
                if (shift + j) % 8 == r:
                    base = shift + j - r
                    if r == 0:
                        term = ext[pl.ds(base, rows)] * weight[j : j + 1]
                    else:
                        term = ext[pl.ds(base, long)] * weight[j : j + 1]
                    sub = term if sub is None else sub + term
            if r == 0:
                total = total + sub
            else:
                total = total + pltpu.roll(sub, long - r, 0)[:rows]
        turned = total.T
        ctr[...] = turned
        stats[t, 0:1] = jnp.sum(turned, axis=0, keepdims=True)
        stats[t, 1:2] = jnp.sum(turned * turned, axis=0, keepdims=True)

    def stat_copy(k):
        return rdma(stats.at[t], stats.at[t], st_send.at[k], st_recv.at[t], tp=(t + k) % n_tp)

    def send_stats():
        for k in range(1, n_tp):
            stat_copy(k).start()

    def finish_conv():
        for k in range(1, n_tp):
            src = (t + k) % n_tp
            rdma(stats.at[src], stats.at[src], st_send.at[0], st_recv.at[src], tp=src).wait_recv()
        loads[9].wait()
        tot = stats[0]
        for p in range(1, n_tp):
            tot = tot + stats[p]
        mean = tot[0:1] / (width * n_tp)
        var = tot[1:2] / (width * n_tp) - mean * mean
        y = ((ctr[...] - mean) * lax.rsqrt(var + 1e-05)).T
        y = y * lng[...].astype(F32)
        y = (y * jax.nn.sigmoid(y)).astype(BF16)
        split(y, conv_src)

        @pl.when(z > 0)
        def _():
            spread(conv_src, conv_in, conv_send, conv_recv)

    each = rows // n_tp

    def row_copy(k, src, dst, send, recv):
        d = (t + k) % n_tp
        return rdma(src.at[d], dst.at[t], send.at[k], recv.at[t], tp=d)

    def split(values, src):
        for d in range(n_tp):
            src[d] = values[d * each : (d + 1) * each]

    def spread(src, dst, send, recv):
        for k in range(1, n_tp):
            row_copy(k, src, dst, send, recv).start()
        dst[t] = src[t]

    def collect(src, dst, send, recv):
        for k in range(1, n_tp):
            d = (t + k) % n_tp
            rdma(dst.at[d], dst.at[d], send.at[0], recv.at[d], tp=d).wait_recv()
        return jnp.concatenate([dst[d] for d in range(n_tp)], axis=1)

    conv_at = 2
    w_at = (6, 10, 14)
    stats_at = 12

    lag = jnp.where(low > 0, 1 + (2 * (last - z) + 2) // 5, 0)

    def flow_up(s):
        blk = z - s
        comes = (s >= 1) & (blk >= low)
        goes = comes & (z < last) & (blk >= low_up) & jnp.logical_not((blk == 0) & (z == express - 1))
        return comes, goes

    def flow_down(d):
        blk = z + d - n
        comes = (d >= 1) & (blk >= 0) & (blk < low)
        goes = comes & (blk < low_down)
        return comes, goes

    def send_far():
        @pl.when(z == 0)
        def _():
            cum_copy(1, z, 1, express).start()
            for q in range(CHUNKS):
                kv_copy(1, z, q, 1, express).start()

        pl.semaphore_wait(far_ready, 1)
        cum_copy(1, z, 0, last).start()
        for q in range(CHUNKS):
            kv_copy(1, z, q, 0, last).start()

    def step(s, carry):
        d = s - lag
        cw_in, cw_on = flow_up(s)
        cc_in, cc_on = flow_down(d)
        j_cw, j_cc = (z + n - s) % n, (z + n + d) % n
        b_cw, b_cc = (z + n - s + 1) % n, (z + n + d - 1) % n
        has_cw, _ = flow_up(s - 1)
        has_cc, _ = flow_down(d - 1)
        two = has_cw & has_cc
        one = has_cw ^ has_cc
        every = CHUNKS // heads

        @pl.when(is_low & (z < express) & (s == jnp.maximum(z, 1)))
        def _():
            send_far()

        for q in range(CHUNKS):
            for way, arrives, goes, blk, to, k, again in (
                (1, cc_in, cc_on, j_cc, down, d, d - 2 >= n - z),
                (0, cw_in, cw_on, j_cw, up, s, s >= 2),
            ):

                @pl.when(arrives)
                def _(way=way, blk=blk, to=to):
                    if q == 0:
                        cum_copy(way, blk, 0, to).wait_recv()
                    kv_copy(way, blk, q, 0, to).wait_recv()

                @pl.when(goes & again)
                def _(way=way, blk=blk, to=to, k=k):
                    if q == 0:
                        cum_copy(way, blk, k, to).wait_send()
                    kv_copy(way, blk, q, k, to).wait_send()

                @pl.when(goes)
                def _(way=way, blk=blk, to=to, k=k):
                    if q == 0:
                        cum_copy(way, blk, k, to).start()
                    kv_copy(way, blk, q, k, to).start()

            if q % every == every - 1:

                @pl.when(two)
                def _():
                    attend(q // every, [b_cw, b_cc])

                @pl.when(one)
                def _():
                    attend(q // every, [jnp.where(has_cw, b_cw, b_cc)])

        @pl.when((z == last) & (s <= n_low))
        def _():
            first = first_tells + 2 + s + s // 2
            for j, really in ((first - 1, s % 2 < 2), (first, s % 2 == 1)):

                @pl.when(really & (j < n_low))
                def _(j=j):
                    tell(j)

        @pl.when(s == conv_at)
        def _():
            convolve()
            send_stats()

        @pl.when(s == stats_at)
        def _():
            finish_conv()

        @pl.when((z > 0) & (s == w_at[0]))
        def _():
            got_w(left, 0)
            w_copies[6].start()
            w_copies[7].start()
            got_w(right, 1)
            w_copies[8].start()
            w_copies[9].start()

        @pl.when((z > 0) & (s == w_at[1]))
        def _():
            got_w(left, 1)
            w_copies[10].start()
            got_w(right, 0)
            w_copies[11].start()

        @pl.when((z > 0) & (s == w_at[2]))
        def _():
            got_w(far, 0)
            w_copies[12].start()
            got_w(far, 1)
            w_copies[13].start()

        return carry

    steps = jnp.maximum(
        jnp.maximum(z - low + 1, max(stats_at, w_at[2])), jnp.where(low > 0, n - z + low + lag, 0)
    )
    lax.fori_loop(1, steps + 1, step, 0)

    tops, sums = m_ref[...], l_ref[...]
    logs = tops + jnp.log(sums)
    attn = acc[...] / sums
    log_row = logs[:rows]
    attn_row = attn[:rows]
    for h in range(1, heads):
        attn_row = jnp.where(lane >= h * hd, attn[h * rows : (h + 1) * rows], attn_row)
        log_row = jnp.where(lane >= h, logs[h * rows : (h + 1) * rows], log_row)
    split(attn_row.astype(BF16), attn_src)
    cut = wc_all.shape[1] // OUT_CUTS
    nx = n_tp // 2
    own_rows = pl.ds(pl.multiple_of(t * width, width), width)

    def product(core, i):
        columns = slice(i * cut, (i + 1) * cut)
        conv = jnp.concatenate([conv_src[2 * k + core] for k in range(nx)], axis=0)
        attn = jnp.concatenate([attn_src[2 * k + core] for k in range(nx)], axis=0)
        total = dot(conv, wc_all[own_rows, columns], NN) + dot(attn, wa_all[own_rows, columns], NN)
        return total.reshape(nx, each, cut)

    @pl.when(z > 0)
    def _():
        spread(attn_src, attn_in, attn_send, attn_recv)

    @pl.when(is_low & (z >= express))
    def _():
        send_far()

    log_ref[...] = log_row.T[:heads] + (cum[z] - cum[z][:, 0:1])
    results = [pltpu.make_async_copy(log_ref, log_hbm, out_sem.at[OUT_CUTS])]
    results[0].start()
    @pl.when(z > 0)
    def _():
        for slot in (mate, at(-1, 1 - c), at(1, 1 - c), at(2, 1 - c)):
            got_w(slot, 0)
            got_w(slot, 1)
        lhs = collect(conv_src, conv_in, conv_send, conv_recv)
        for i in range(OUT_CUTS):
            columns = pl.ds(i * cut, cut)
            conv_part[:, columns] = dot(lhs, wc_all[:, columns], NN)
        lhs = collect(attn_src, attn_in, attn_send, attn_recv)
        for i in range(OUT_CUTS):
            columns = pl.ds(i * cut, cut)
            mixed_ref[:, columns] = (conv_part[:, columns] + dot(lhs, wa_all[:, columns], NN)).astype(BF16)

    @pl.when(z == 0)
    def _():
        pairs = []
        for i in range(OUT_CUTS):
            pair_out[i] = product(1 - c, i).astype(BF16)
            copy = rdma(pair_out.at[i], pair_in.at[i], pair_send.at[i], pair_recv.at[i], tp=mate)
            copy.start()
            pairs.append(copy)
        outs = []
        for i in range(OUT_CUTS):
            own = product(c, i)
            pairs[i].wait_recv()
            xout[i] = (own + pair_in[i].astype(F32)).astype(BF16)
            for dx in (2, 1, 3):
                copy = rdma(
                    xout.at[i, (x + dx) % nx], xin.at[i, dx - 1], x_send.at[i, dx - 1], x_recv.at[i, dx - 1], tp=at(dx - nx, c)
                )
                copy.start()
                outs.append((i, copy))
        for i in range(OUT_CUTS):
            total = xout[i, x].astype(F32)
            for k, copy in outs:
                if k == i:
                    copy.wait_recv()
            for dx in range(nx - 1):
                total = total + xin[i, dx].astype(F32)
            mixed_ref[:, i * cut : (i + 1) * cut] = total.astype(BF16)
        for copy in pairs:
            copy.wait_send()
        for k, copy in outs:
            copy.wait_send()

    results.append(pltpu.make_async_copy(mixed_ref, mixed_hbm, out_sem.at[0]))
    results[-1].start()

    for copy in pending:
        copy.wait_send()
    ups = z - low_up - jnp.where(z == express - 1, 1, 0) + 1
    downs = low_down
    for way, parity, cond in (
        (0, 0, first_up),
        (0, 1, first_up & (ups > 1)),
        (1, 0, is_low | (downs > 1) | ((downs == 1) & ((n - z) % 2 == 0))),
        (1, 1, (z == 0) | (downs > 1) | ((downs == 1) & ((n - z) % 2 == 1))),
    ):

        @pl.when(cond)
        def _(way=way, parity=parity):
            cum_copy(way, z, parity, up).wait_send()
            for q in range(CHUNKS):
                kv_copy(way, z, q, parity, up).wait_send()

    @pl.when(first_up)
    def _():
        halo_copy.wait_send()

    for k in range(1, n_tp):
        stat_copy(k).wait_send()

    @pl.when(z > 0)
    def _():
        for copy in w_copies:
            copy.wait_send()
        for k in range(1, n_tp):
            row_copy(k, conv_src, conv_in, conv_send, conv_recv).wait_send()
            row_copy(k, attn_src, attn_in, attn_send, attn_recv).wait_send()

    for copy in results:
        copy.wait()


def solution(mesh):
    n, n_tp = mesh.shape["sp"], mesh.shape["tp"]

    def local(
        inputs,
        norm_gain,
        w_conv_in,
        w_conv_gate,
        conv_kernel,
        ln_gain,
        w_query,
        w_key,
        w_value,
        cum_gate,
        w_conv_out,
        w_attn_out,
    ):
        rows, feat = inputs.shape
        width, full = w_key.shape
        heads = cum_gate.shape[0]
        n_taps = conv_kernel.shape[0]
        each = rows // n_tp
        pad = 32
        half_n = n // 2
        dma = pltpu.SemaphoreType.DMA
        vmem = pltpu.VMEM
        scratch = [
            vmem((each, full), BF16),
            vmem((heads, rows), F32),
            dma((OUT_CUTS + 1,)),
            vmem((n_tp, rows, feat), BF16),
            vmem((n_tp, rows, feat), BF16),
            vmem((full // 128, 128), BF16),
            vmem((full // 128, 128), F32),
            vmem((n_taps, width), BF16),
            vmem((1, width), BF16),
            vmem((2 * width, full), BF16),
            vmem((3 * width, full), BF16),
            vmem((n_tp * width, full), BF16),
            vmem((n_tp * width, full), BF16),
            vmem((n, rows, 2 * width), BF16),
            vmem((n, heads, rows), F32),
            vmem((rows, 2 * width), F32),
            vmem((rows, 128), F32),
            vmem((heads * rows, width), BF16),
            vmem((heads * rows, width), F32),
            vmem((heads * rows, width), F32),
            vmem((heads * rows, width), F32),
            vmem((pad + rows + 8, width), F32),
            vmem((pad, width), BF16),
            vmem((pad, width), BF16),
            vmem((width, rows), F32),
            vmem((n_tp, 2, rows), F32),
            vmem((n_tp, each, width), BF16),
            vmem((n_tp, each, width), BF16),
            vmem((n_tp, each, width), BF16),
            vmem((n_tp, each, width), BF16),
            vmem((each, full), F32),
            dma((12,)),
            dma((21,)),
            dma((n_tp, 4)),
            dma((2, 2, CHUNKS)),
            dma((n, CHUNKS)),
            dma((2, 2)),
            dma((n,)),
            dma((2,)),
            pltpu.SemaphoreType.REGULAR,
            dma((n_tp,)),
            dma((n_tp,)),
            vmem((OUT_CUTS, n_tp // 2, each, full // OUT_CUTS), BF16),
            vmem((OUT_CUTS, n_tp // 2, each, full // OUT_CUTS), BF16),
            vmem((OUT_CUTS, n_tp // 2, each, full // OUT_CUTS), BF16),
            vmem((OUT_CUTS, n_tp // 2 - 1, each, full // OUT_CUTS), BF16),
            dma((OUT_CUTS,)),
            dma((OUT_CUTS,)),
            dma((OUT_CUTS, n_tp // 2 - 1)),
            dma((OUT_CUTS, n_tp // 2 - 1)),
            dma((14,)),
            dma((n_tp, 2)),
            dma((n_tp,)),
            dma((n_tp,)),
            dma((n_tp,)),
            dma((n_tp,)),
        ]
        return pl.pallas_call(
            functools.partial(layer, n, n_tp),
            out_shape=(
                jax.ShapeDtypeStruct((each, full), BF16),
                jax.ShapeDtypeStruct((heads, rows), F32),
            ),
            in_specs=[pl.BlockSpec(memory_space=pl.ANY)] * 12,
            out_specs=(pl.BlockSpec(memory_space=pl.ANY), pl.BlockSpec(memory_space=pl.ANY)),
            scratch_shapes=scratch,
            compiler_params=pltpu.CompilerParams(collective_id=0, has_side_effects=True),
        )(
            inputs,
            norm_gain.reshape(full // 128, 128),
            w_conv_in,
            w_conv_gate,
            conv_kernel,
            ln_gain.reshape(1, width),
            w_query,
            w_key,
            w_value,
            cum_gate,
            w_conv_out,
            w_attn_out,
        )

    in_specs = (
        P(("grp", "sp"), "tp"),
        P(),
        P("tp", None),
        P("tp", None),
        P(None, "tp"),
        P("tp"),
        P("tp", None),
        P("tp", None),
        P("tp", None),
        P("tp", ("grp", "sp")),
        P("tp", None),
        P("tp", None),
    )
    out_specs = (P(("grp", "sp", "tp"), None), P("tp", ("grp", "sp")))
    return jax.shard_map(local, mesh=mesh, in_specs=in_specs, out_specs=out_specs, check_vma=False)
```
